32 devices in a mesh: grp: 2 (over x), ep: 16 (over z, y, core).
Axes of the slice: x: 2, y: 2, z: 4, core: 2. Of those that a mesh axis runs over, the one named last changes fastest.
Arguments:
- tokens: bfloat16 [8192, 2048], P(('grp', 'ep')), parts along dimension 0, may hold values from -6 to 6
- norm_gain: float32 [2048], replicated, may hold values from 0.1 to 1.9
- expert_ids: int32 [8192, 2], P(('grp', 'ep')), parts along dimension 0, may hold values from 0 to 15, all different within a row; in each aligned block of 256 rows (0 to 255, 256 to 511, ...) at most 64 rows name the same one
- gate_weights: float32 [8192, 2], P(('grp', 'ep')), parts along dimension 0, may hold values from 0.1 to 1
- w_gate: bfloat16 [16, 2048, 1024], P('ep'), may hold values from -0.125 to 0.125
- w_up: bfloat16 [16, 2048, 1024], P('ep'), may hold values from -0.125 to 0.125
- w_down: bfloat16 [16, 1024, 2048], P('ep'), may hold values from -0.1875 to 0.1875
Outputs:
- mixed: bfloat16 [8192, 2048], P(('grp', 'ep')), parts along dimension 0
The draws below stay inside these ranges and needn't reach their ends.
There are 2 independent parts, one for each index of `grp`. The reference program is written for one: setup_inputs(seed, part) draws one part's arguments, and reference() takes and returns one part's arrays. A program takes and returns all parts, laid end to end along the dimension named above; an argument that names none is the same for every part. Nothing has to cross between parts.
Inputs may be any that keep to these rules, and one draw needn't show every extreme that they name: `expert_ids`: A token's 2 experts are distinct. Within the rows of one device (aligned blocks of 256 tokens) no expert is named more than 64 times, and in some block one expert is named exactly 64 times.
All inputs are finite; a program needn't handle non-finite values.
Results may differ from the reference program's by a relative error of at most 0.0071.
Values may be sent and summed in bfloat16 or wider, within the bound.
A program may use at most 64 MiB of HBM per device.

```python
import math
import jax
import jax.numpy as jnp
import numpy as np
from jax import lax

D = 2048
FF = 1024
TOP = 2
TOK_DEV = 256
EXPERTS = 16
CAP = 64
TOKENS = 4096
N_EP = 16


def steps_of(stream_key, extent, shards, smallest, high):
    def one(axis_at, shards_of):
        draws = jax.random.uniform(jax.random.fold_in(jax.random.fold_in(stream_key, 6), axis_at), (shards_of,), jnp.float32, smallest / len(shards), high / len(shards))
        return jnp.repeat(jnp.exp(draws), extent[axis_at] // shards_of).reshape((-1,) + (1,) * (len(extent) - axis_at - 1))

    level = one(*shards[0])
    for cut in shards[1:]:
        level = level * one(*cut)
    return level


def shared_out(own_key, own, number, rows, amount, top, bound, lean):
    ranking = jax.random.permutation(own_key, amount)
    heavy_load, common = shares(amount, rows * top, bound, lean, True), shares(amount, rows * top, bound, lean, False)
    places = jnp.arange(amount)

    def named(lengths, rotation):
        used = int((lengths > 0).sum())
        fixed = max(1, used // 4)
        shifted = fixed + (places - fixed + rotation * (used - fixed)) % max(1, amount - fixed)
        return jnp.zeros((amount,), jnp.int32).at[ranking[jnp.where(places < fixed, places, shifted)]].set(jnp.asarray(lengths, jnp.int32))

    lengths = jnp.where(number % 4 == 0, named(heavy_load, number // 4), named(common, number - number // 4 - 1))
    mixed = jax.random.permutation(jax.random.fold_in(own, 3), amount)
    giver, taker = mixed[0:amount // 2 * 2:2], mixed[1:amount // 2 * 2:2]
    margin = jnp.minimum(lengths[giver] - 1, bound - lengths[taker]) // 2
    margin = jnp.where((giver == ranking[0]) | (taker == ranking[0]) | (lengths[taker] == 0), 0, jnp.maximum(margin, 0))
    shifted = jax.random.randint(jax.random.fold_in(own, 4), (amount // 2,), 0, 1 << 20) % (margin + 1)
    lengths = lengths.at[giver].add(-shifted).at[taker].add(shifted)
    members = jnp.searchsorted(jnp.cumsum(lengths), jnp.arange(rows * top), side="right").astype(jnp.int32)
    listing = members.reshape(top, rows).T
    listing = listing[jax.random.permutation(jax.random.fold_in(own, 1), rows)]
    rotation = jax.random.randint(jax.random.fold_in(own, 2), (rows, 1), 0, top)
    return jnp.take_along_axis(listing, (jnp.arange(top)[None, :] + rotation) % top, axis=1)


def shares(count, total, most, skew, full):
    loads = [(1 << 20) // math.isqrt(rank ** skew) + 1 for rank in range(1, count + 1)]
    largest = most if full else min(most, max(-(-total // count), total * loads[0] // sum(loads)))
    least = 1 if total - largest >= count - 1 else 0
    holding, spare = [largest] + [least] * (count - 1), total - largest - least * (count - 1)
    while spare > 0:
        movable = [i for i in range(1, count) if holding[i] < largest] or [i for i in range(1, count) if holding[i] < most]
        mass, remaining = sum([loads[i] for i in movable]), spare
        for i in movable:
            extra = min(most - holding[i], max(1, remaining * loads[i] // mass), spare)
            holding[i] = holding[i] + extra
            spare = spare - extra
    return np.array(holding)


def centred(stream_key, shape, width, reach, split=(), kind=jnp.bfloat16):
    drawn = width * jax.random.normal(stream_key, shape, jnp.float32)
    if split:
        drawn = drawn * steps_of(stream_key, shape, split, -0.22, 0.18)
    return jnp.clip(drawn, -reach, reach).astype(kind)


def setup_inputs(seed: int = 0, part: int = 0) -> dict:
    key_list = jax.random.split(jax.random.key(seed), 8)
    part_splits = jax.random.split(jax.random.fold_in(key_list[7], part), 8)
    tokens = centred(part_splits[0], (TOKENS, D), 1.0, 6.0, ((0, 16),))
    norm_gain = jnp.clip(1.0 + 0.18 * jax.random.normal(key_list[1], (D,), jnp.float32), 0.1, 1.9)
    expert_ids_keys = jax.random.split(jax.random.fold_in(part_splits[2], 1), TOKENS // TOK_DEV)
    expert_ids_turns = jax.random.permutation(jax.random.fold_in(part_splits[2], 3), TOKENS // TOK_DEV)
    expert_ids = jax.vmap(lambda own, number: shared_out(jax.random.fold_in(part_splits[2], 2), own, number, TOK_DEV, EXPERTS, TOP, CAP, 2))(expert_ids_keys, expert_ids_turns).reshape((TOKENS, TOP))
    gate_weights = jnp.clip(0.1 + 0.9 * jax.random.uniform(part_splits[3], (TOKENS, TOP), jnp.float32) ** steps_of(part_splits[3], (TOKENS, TOP), ((0, 16),), -0.2, 0.2), 0.1, 1.0)
    w_gate = centred(key_list[4], (EXPERTS, D, FF), D ** -0.5, 0.125, ((0, 16),))
    w_up = centred(key_list[5], (EXPERTS, D, FF), D ** -0.5, 0.125, ((0, 16),))
    w_down = centred(key_list[6], (EXPERTS, FF, D), FF ** -0.5, 0.1875, ((0, 16),))
    return dict(tokens=tokens, norm_gain=norm_gain, expert_ids=expert_ids, gate_weights=gate_weights, w_gate=w_gate, w_up=w_up, w_down=w_down)


def reference(tokens, norm_gain, expert_ids, gate_weights, w_gate, w_up, w_down):
    values = tokens.astype(jnp.float32)
    normed = (values * lax.rsqrt(lax.optimization_barrier(jnp.mean(values * values, -1, keepdims=True)) + 1e-06) * norm_gain).astype(jnp.bfloat16)
    flat_ids = expert_ids.reshape(N_EP, TOK_DEV * TOP)
    onehot = (flat_ids[:, :, None] == jnp.arange(EXPERTS, dtype=jnp.int32)[None, None, :]).astype(jnp.int32)
    before = jnp.cumsum(onehot, axis=1) - onehot
    slots = lax.optimization_barrier(jnp.sum(onehot * before, axis=-1)).astype(jnp.int32)
    dest = (flat_ids * CAP + slots).astype(jnp.int32)
    copies = jnp.repeat(normed.reshape(N_EP, TOK_DEV, D), TOP, axis=1)
    buffers = jnp.zeros((N_EP, EXPERTS * CAP, D), jnp.bfloat16)
    sources = jnp.arange(N_EP, dtype=jnp.int32)[:, None]
    buffers = buffers.at[sources, dest].set(copies)
    buffers = buffers.reshape(N_EP, EXPERTS, CAP, D).transpose(1, 0, 2, 3).reshape(EXPERTS, N_EP * CAP, D)

    def run(operands):
        rows, gate_w, up_w, down_w = operands
        gate = jnp.dot(rows, gate_w, preferred_element_type=jnp.float32)
        upper = jnp.dot(rows, up_w, preferred_element_type=jnp.float32)
        hidden = (jax.nn.silu(gate) * upper).astype(jnp.bfloat16)
        return jnp.dot(hidden, down_w, preferred_element_type=jnp.float32).astype(jnp.bfloat16)
    results = lax.map(run, (buffers, w_gate, w_up, w_down))
    results = results.reshape(EXPERTS, N_EP, CAP, D).transpose(1, 0, 2, 3).reshape(N_EP, EXPERTS * CAP, D)
    back = jnp.take_along_axis(results, dest[:, :, None], axis=1).astype(jnp.float32)
    back = back.reshape(N_EP, TOK_DEV, TOP, D)
    weights = gate_weights.reshape(N_EP, TOK_DEV, TOP)
    mixed = lax.optimization_barrier(jnp.sum(back * weights[:, :, :, None], axis=2))
    return mixed.reshape(TOKENS, D).astype(jnp.bfloat16)
```

```python
import functools
import jax
import jax.numpy as jnp
from jax import lax
from jax.experimental import pallas as pl
from jax.experimental.pallas import tpu as pltpu
from jax.sharding import PartitionSpec as P

SUB = 4
KD = 4
KR = 4


def kernel(n, cap, tok_ref, gain_ref, ids_ref, gw_ref, wg_ref, wu_ref, wd_ref, out_ref,
           wg, wu, wd, lines, places, outgoing, arrived, results, returned, hidden, chain,
           pick, high, low,
           wsem, lsend, lrecv, psend, precv, dsend, drecv, bsend, brecv, csend, crecv):
    zs = n // SUB
    me = lax.axis_index("ep")
    hi, lo = me // SUB, me % SUB
    tok, width = tok_ref.shape
    ff = wg.shape[1]
    rows = SUB * cap
    dcols, rcols = width // KD, width // KR
    own = 2

    def peer(plane, part):
        return {"ep": plane * SUB + part}

    barrier = pltpu.get_barrier_semaphore()

    def greet(to):
        pl.semaphore_signal(barrier, inc=1, device_id=to, device_id_type=pl.DeviceIdType.MESH)

    for dl in range(1, SUB):
        greet(peer(hi, (lo + dl) % SUB))

    @pl.when(hi > 0)
    def _():
        greet(peer((hi + zs - 1) % zs, lo))

    @pl.when(hi < zs - 1)
    def _():
        greet(peer((hi + 1) % zs, lo))

    w_copies = [
        pltpu.make_async_copy(wg_ref.at[0], wg, wsem.at[0]),
        pltpu.make_async_copy(wu_ref.at[0], wu, wsem.at[1]),
        pltpu.make_async_copy(wd_ref.at[0], wd, wsem.at[2]),
    ]
    for c in w_copies:
        c.start()

    def remote(src, dst, send, recv, to):
        return pltpu.make_async_remote_copy(
            src_ref=src, dst_ref=dst, send_sem=send, recv_sem=recv,
            device_id=to, device_id_type=pl.DeviceIdType.MESH)

    def dcol(k):
        return pl.ds(pl.multiple_of(k * dcols, dcols), dcols)

    def rcol(k):
        return pl.ds(pl.multiple_of(k * rcols, rcols), rcols)

    def slot_rows(j, dl):
        return pl.ds(pl.multiple_of(j * rows + dl * cap, cap), cap)

    def block_rows(j):
        return pl.ds(pl.multiple_of(j * rows, rows), rows)

    def far_rows(j):
        return pl.ds(pl.multiple_of(j * rows + cap, cap), rows - cap)

    def onward(way):
        return (hi + 2 * way - 1 + zs) % zs

    def line_copy(block, k, way):
        part = lines.at[block, :, dcol(k)]
        return remote(part, part, lsend.at[way * zs + block], lrecv.at[block * KD + k],
                      peer(onward(way), lo))

    def place_copy(block, way):
        return remote(places.at[block], places.at[block], psend.at[way * zs + block],
                      precv.at[block], peer(onward(way), lo))

    def out_copy(j, dl, k):
        at = slot_rows(j, dl)
        return remote(outgoing.at[at, dcol(k)], arrived.at[at, dcol(k)],
                      dsend.at[j], drecv.at[j * KD + k], peer(hi, (lo + dl) % SUB))

    def out_arrival(j, k):
        at = arrived.at[far_rows(j), dcol(k)]
        return remote(at, at, dsend.at[j], drecv.at[j * KD + k], peer(hi, (lo + 1) % SUB))

    def back_copy(j, dl, k):
        at = slot_rows(j, dl)
        return remote(results.at[at, rcol(k)], returned.at[at, rcol(k)],
                      bsend.at[j], brecv.at[j * KR + k], peer(hi, (lo - dl + SUB) % SUB))

    def back_arrival(j, k):
        at = returned.at[far_rows(j), rcol(k)]
        return remote(at, at, bsend.at[j], brecv.at[j * KR + k], peer(hi, (lo + 1) % SUB))

    def chain_copy(way, j, k):
        part = chain.at[way * zs + j, :, rcol(k)]
        return remote(part, part, csend.at[way * zs + j], crecv.at[(way * zs + j) * KR + k],
                      peer(onward(way), lo))

    step = 32

    def norm(i, carry):
        at = pl.ds(pl.multiple_of(i * step, step), step)
        v = tok_ref[at, :].astype(jnp.float32)
        scale = lax.rsqrt(jnp.mean(v * v, -1, keepdims=True) + 1e-06)
        lines[hi, at, :] = (v * scale * gain_ref[...]).astype(jnp.bfloat16)
        return carry

    lax.fori_loop(0, tok // step, norm, 0)

    ends = jnp.where(hi == 0, 1, 0) + jnp.where(hi == zs - 1, 1, 0)
    pl.semaphore_wait(barrier, SUB + 1 - ends)

    def forward(way, act):
        @pl.when(jnp.where(way == 1, zs - 1 - hi, hi) > 0)
        def _():
            act(way)

    for way in (1, 0):
        forward(way, lambda w: line_copy(hi, 0, w).start())

    ids = ids_ref[...]
    id0, id1 = ids[:, 0:1], ids[:, 1:2]
    lane = lax.broadcasted_iota(jnp.int32, (tok, 128), 1)
    chosen = jnp.where((id0 == lane) | (id1 == lane), 1.0, 0.0)
    t_row = lax.broadcasted_iota(jnp.int32, (tok, tok), 0)
    t_col = lax.broadcasted_iota(jnp.int32, (tok, tok), 1)
    earlier = jnp.where(t_col < t_row, 1.0, 0.0).astype(jnp.bfloat16)
    before = jnp.dot(earlier, chosen.astype(jnp.bfloat16), preferred_element_type=jnp.float32)
    slot0 = jnp.sum(jnp.where(id0 == lane, before, 0.0), axis=1, keepdims=True)
    slot1 = jnp.sum(jnp.where(id1 == lane, before, 0.0), axis=1, keepdims=True)
    dest0 = id0.astype(jnp.float32) * cap + slot0
    dest1 = id1.astype(jnp.float32) * cap + slot1
    gw = gw_ref[...]
    g0, g1 = gw[:, 0:1], gw[:, 1:2]
    both = jnp.where(lane == 0, dest0, jnp.where(
        lane == 1, dest1, jnp.where(lane == 2, g0, jnp.where(lane == 3, g1, 0.0))))
    turned = jnp.transpose(both)
    where = lax.broadcasted_iota(jnp.int32, (8, tok), 0)
    places[hi] = jnp.where(
        where == 0, turned[0:1, :], jnp.where(
            where == 1, turned[1:2, :], jnp.where(where == 2, turned[2:3, :], turned[3:4, :])))

    def send_own(way):
        place_copy(hi, way).start()
        for k in range(1, KD):
            line_copy(hi, k, way).start()

    for way in (1, 0):
        forward(way, send_own)

    def row_index():
        r = lax.broadcasted_iota(jnp.int32, (rows, tok), 0)
        return ((hi * SUB + (lo + r // cap) % SUB) * cap + r % cap).astype(jnp.float32)

    def choose(j, at):
        index = row_index()
        w = places[j]
        pick[at] = jnp.where((index == w[0:1, :]) | (index == w[1:2, :]), 1.0, 0.0).astype(
            jnp.bfloat16)

    def pack(j, k, at):
        got = jnp.dot(pick[at], lines[j, :, dcol(k)],
                      preferred_element_type=jnp.float32).astype(jnp.bfloat16)
        outgoing[far_rows(j), dcol(k)] = got[cap:, :]
        for dl in range(1, SUB):
            out_copy(j, dl, k).start()
        arrived[slot_rows(j, 0), dcol(k)] = got[:cap, :]

    ftile = min(ff, 256)

    def experts(j):
        at = block_rows(j)

        def landed(k, carry):
            out_arrival(j, k).wait_recv()
            return carry

        lax.fori_loop(0, KD, landed, 0)

        def up(f, carry):
            cols = pl.ds(pl.multiple_of(f * ftile, ftile), ftile)
            x = arrived[at, :]
            g = jnp.dot(x, wg[:, cols], preferred_element_type=jnp.float32)
            u = jnp.dot(x, wu[:, cols], preferred_element_type=jnp.float32)
            hidden[:, cols] = (g / (1.0 + jnp.exp(-g)) * u).astype(jnp.bfloat16)
            return carry

        lax.fori_loop(0, ff // ftile, up, 0)

        def down(k, carry):
            got = jnp.dot(hidden[...], wd[:, rcol(k)],
                          preferred_element_type=jnp.float32).astype(jnp.bfloat16)
            results[far_rows(j), rcol(k)] = got[cap:, :]
            for dl in range(1, SUB):
                back_copy(j, dl, k).start()
            returned[slot_rows(j, 0), rcol(k)] = got[:cap, :]
            return carry

        lax.fori_loop(0, KR, down, 0)

    def weigh(j, at):
        index = row_index()
        w = places[j]
        weight = jnp.transpose(jnp.where(index == w[0:1, :], w[2:3, :], 0.0)
                               + jnp.where(index == w[1:2, :], w[3:4, :], 0.0))
        top = weight.astype(jnp.bfloat16)
        high[at] = top
        low[at] = (weight - top.astype(jnp.float32)).astype(jnp.bfloat16)

    def mix(j, k, at):
        block = returned[block_rows(j), rcol(k)]
        return (jnp.dot(high[at], block, preferred_element_type=jnp.float32)
                + jnp.dot(low[at], block, preferred_element_type=jnp.float32))

    choose(hi, own)

    def pack_own(k, carry):
        pack(hi, k, own)
        return carry

    lax.fori_loop(0, KD, pack_own, 0)
    for c in w_copies:
        c.wait()

    experts(hi)
    weigh(hi, own)

    first = hi // ((zs + 1) // 2)
    ways = (first, 1 - first)

    def arriving(s, act):
        for way in ways:
            block = hi + (1 - 2 * way) * s

            @pl.when((block >= 0) & (block < zs))
            def _():
                act((block + zs) % zs, way)

    def stage(s):
        def begin(block, way):
            place_copy(block, way).wait_recv()
            forward(way, lambda w: place_copy(block, w).start())
            choose(block, way)

        arriving(s, begin)

        def chunk(k, carry):
            def take(block, way):
                line_copy(block, k, way).wait_recv()
                forward(way, lambda w: line_copy(block, k, w).start())
                pack(block, k, way)

            arriving(s, take)
            return carry

        lax.fori_loop(0, KD, chunk, 0)
        arriving(s, lambda block, way: experts(block))

    def leaving(t, act):
        for way in (1, 0):
            j = way * t + (1 - way) * (zs - 1 - t)

            @pl.when(j > hi if way else j < hi)
            def _():
                act(j, way)

    def give(t):
        leaving(t, lambda j, way: weigh(j, way))

        def chunk(k, carry):
            def add(j, way):
                back_arrival(j, k).wait_recv()
                value = mix(j, k, way)
                at = way * zs + j

                @pl.when(hi > 0 if way else hi < zs - 1)
                def _():
                    chain_copy(way, j, k).wait_recv()
                    chain[at, :, rcol(k)] = (
                        value + chain[at, :, rcol(k)].astype(jnp.float32)).astype(jnp.bfloat16)

                @pl.when(hi == 0 if way else hi == zs - 1)
                def _():
                    chain[at, :, rcol(k)] = value.astype(jnp.bfloat16)

                chain_copy(way, j, k).start()

            leaving(t, add)
            return carry

        lax.fori_loop(0, KR, chunk, 0)

    def turn(s, carry):
        stage(s)
        give(s)
        return carry

    lax.fori_loop(1, zs, turn, 0)

    def final(k, carry):
        back_arrival(hi, k).wait_recv()
        value = mix(hi, k, own)

        @pl.when(hi == 0)
        def _():
            chain_copy(0, hi, k).wait_recv()
            out_ref[:, rcol(k)] = (
                value + chain[hi, :, rcol(k)].astype(jnp.float32)).astype(out_ref.dtype)

        @pl.when(hi == zs - 1)
        def _():
            chain_copy(1, hi, k).wait_recv()
            out_ref[:, rcol(k)] = (
                value + chain[zs + hi, :, rcol(k)].astype(jnp.float32)).astype(out_ref.dtype)

        @pl.when((hi > 0) & (hi < zs - 1))
        def _():
            chain_copy(0, hi, k).wait_recv()
            chain_copy(1, hi, k).wait_recv()
            out_ref[:, rcol(k)] = (
                value + chain[hi, :, rcol(k)].astype(jnp.float32)
                + chain[zs + hi, :, rcol(k)].astype(jnp.float32)).astype(out_ref.dtype)

        return carry

    lax.fori_loop(0, KR, final, 0)

    def finish(j, carry):
        at = far_rows(j)
        remote(outgoing.at[at, :], outgoing.at[at, :], dsend.at[j], drecv.at[0],
               peer(hi, (lo + 1) % SUB)).wait_send()
        remote(results.at[at, :], results.at[at, :], bsend.at[j], brecv.at[0],
               peer(hi, (lo + 1) % SUB)).wait_send()
        for way in (0, 1):
            to = peer(onward(way), lo)

            @pl.when((hi < zs - 1) & (j <= hi) if way else (hi > 0) & (j >= hi))
            def _():
                place_copy(j, way).wait_send()
                remote(lines.at[j], lines.at[j], lsend.at[way * zs + j], lrecv.at[0],
                       to).wait_send()

            @pl.when(j > hi if way else j < hi)
            def _():
                at = way * zs + j
                remote(chain.at[at], chain.at[at], csend.at[at], crecv.at[0], to).wait_send()

        return carry

    lax.fori_loop(0, zs, finish, 0)


def per_device(tokens, norm_gain, expert_ids, gate_weights, w_gate, w_up, w_down):
    n = lax.axis_size("ep")
    tok, width = tokens.shape
    top = expert_ids.shape[1]
    ff = w_gate.shape[2]
    cap = 2 * tok * top // n
    total = n * cap
    zs = n // SUB
    rows = SUB * cap
    bf16 = jnp.bfloat16
    dma = pltpu.SemaphoreType.DMA
    vmem = pl.BlockSpec(memory_space=pltpu.VMEM)
    hbm = pl.BlockSpec(memory_space=pl.ANY)
    return pl.pallas_call(
        functools.partial(kernel, n, cap),
        out_shape=jax.ShapeDtypeStruct((tok, width), bf16),
        in_specs=[vmem] * 4 + [hbm] * 3,
        out_specs=vmem,
        scratch_shapes=[
            pltpu.VMEM((width, ff), bf16),
            pltpu.VMEM((width, ff), bf16),
            pltpu.VMEM((ff, width), bf16),
            pltpu.VMEM((zs, tok, width), bf16),
            pltpu.VMEM((zs, 8, tok), jnp.float32),
            pltpu.VMEM((total, width), bf16),
            pltpu.VMEM((total, width), bf16),
            pltpu.VMEM((total, width), bf16),
            pltpu.VMEM((total, width), bf16),
            pltpu.VMEM((rows, ff), bf16),
            pltpu.VMEM((2 * zs, tok, width), bf16),
            pltpu.VMEM((3, rows, tok), bf16),
            pltpu.VMEM((3, tok, rows), bf16),
            pltpu.VMEM((3, tok, rows), bf16),
            dma((3,)),
            dma((2 * zs,)),
            dma((zs * KD,)),
            dma((2 * zs,)),
            dma((zs,)),
            dma((zs,)),
            dma((zs * KD,)),
            dma((zs,)),
            dma((zs * KR,)),
            dma((2 * zs,)),
            dma((2 * zs * KR,)),
        ],
        compiler_params=pltpu.CompilerParams(
            collective_id=0, has_side_effects=True, vmem_limit_bytes=62 * 1024 * 1024),
    )(tokens, norm_gain.reshape(1, width), expert_ids, gate_weights, w_gate, w_up, w_down)


def solution(mesh):
    return jax.shard_map(
        per_device,
        mesh=mesh,
        in_specs=(
            P(("grp", "ep"), None),
            P(),
            P(("grp", "ep"), None),
            P(("grp", "ep"), None),
            P("ep", None, None),
            P("ep", None, None),
            P("ep", None, None),
        ),
        out_specs=P(("grp", "ep"), None),
        check_vma=False,
    )
```

```python
import functools
import heapq
import jax
import jax.numpy as jnp
from jax import lax
from jax.experimental import pallas as pl
from jax.experimental.pallas import tpu as pltpu
from jax.sharding import PartitionSpec as P

SUB = 4
KD = 4
KR = 4
KINDS = "SZTUDMFX"
Z_BLOCK, Y_BLOCK, LAG = 23.0, 11.2, 2.0
COST = {"S": 0.1, "Z": 0.1, "T": 0.9, "U": 3.1, "D": 1.9, "M": 1.2, "F": 1.2}
RANK = {"S": 0, "Z": 0, "T": 1, "M": 2, "F": 3, "D": 4, "U": 5}
START, PACK = 6.0, 8.0
PRIO = {}
HOLD = {}


def tables(zs):
    need, when, todo = {}, {}, [[] for _ in range(zs)]
    order = [[] for _ in range(zs)]

    def task(h, name, b, k, deps, at=0.0):
        need[h, name, b, k], when[h, name, b, k] = deps, at
        todo[h].append((name, b, k))

    def rule(h, name, b, k):
        flip = h >= zs / 2
        if name in "SZ":
            name = "ZS"["SZ".index(name)] if flip else name
            return (zs - 1 - h if flip else h), name, k * 4 // KD
        return (zs - 1 - h, name, zs - 1 - b) if flip else (h, name, b)

    for h in range(zs):
        for b in range(zs):
            for k in range(KD):
                task(h, "T", b, k, int(b != h), PACK if b == h else 0.0)
            task(h, "U", b, 0, KD)
            for k in range(KR):
                task(h, "D", b, k, 1)
                if b == h:
                    task(h, "F", b, k, 1 + (h > 0) + (h < zs - 1))
                else:
                    task(h, "M", b, k, 1 + (h > 0 if b > h else h < zs - 1))
        for name, way in (("S", 1), ("Z", 0)):
            for k in range(KD if (h < zs - 1 if way else h > 0) else 0):
                task(h, name, h, k, 0, START)
    events, busy, link = [], [0.0] * zs, {}

    def supply(h, name, b, k, at):
        need[h, name, b, k] -= 1
        when[h, name, b, k] = max(when[h, name, b, k], at)
        heapq.heappush(events, (at, h))

    def wire(key, time, at):
        link[key] = max(at, link.get(key, 0.0)) + time
        return link[key] + LAG

    def onward(h, way, b, k, name, time, at):
        g = h + 2 * way - 1
        supply(g, "F" if name == "M" and g == b else name, b, k, wire((h, way), time, at))

    for h in range(zs):
        events += [(START, h), (PACK, h)]
    heapq.heapify(events)
    end = 0.0
    while events:
        t, h = heapq.heappop(events)
        if busy[h] > t + 1e-9:
            continue
        best, later = None, None
        for c in todo[h]:
            if need[(h,) + c] > 0:
                continue
            key = rule(h, *c)
            at = max(when[(h,) + c], HOLD.get(key, 0.0))
            if at <= t + 1e-9:
                p = (-1 if c[0] in "SZ" and c[2] == 0 else PRIO.get(key, RANK[c[0]]) + 0.01 * c[2], c)
                best = min(best, p) if best else p
            else:
                later = at if later is None else min(later, at)
        if best is None:
            if later is not None:
                heapq.heappush(events, (later, h))
            continue
        name, b, k = best[1]
        todo[h].remove(best[1])
        order[h].append(best[1])
        done = t + 0.1 + COST[name] / {"T": KD, "D": KR, "M": KR, "F": KR}.get(name, 1)
        if name in "SZ":
            onward(h, int(name == "S"), b, k, "T", Z_BLOCK / KD, t)
        elif name == "T":
            way = int(b < h)
            if b != h and (h < zs - 1 if way else h > 0):
                onward(h, way, b, k, "T", Z_BLOCK / KD, t + 0.1)
            supply(h, "U", b, 0, wire(h, Y_BLOCK / KD, done))
        elif name == "U":
            for r in range(KR):
                supply(h, "D", b, r, done)
        elif name == "D":
            supply(h, "F" if b == h else "M", b, k, wire(h, Y_BLOCK / KR, done))
        elif name == "M":
            onward(h, int(b > h), b, k, "M", Z_BLOCK / KR, done)
        end = max(end, done)
        busy[h] = done
        heapq.heappush(events, (done, h))
    assert not any(todo)
    codes = [[KINDS.index(n) * 1024 + b * 32 + k for n, b, k in o if n not in "SZ" or k > 0]
             for o in order]
    size = max(map(len, codes))
    return [c + [KINDS.index("X") * 1024] * (size - len(c)) for c in codes]


def kernel(n, cap, table, tok_ref, gain_ref, ids_ref, gw_ref, wg_ref, wu_ref, wd_ref, out_ref,
           wg, wu, wd, lines, places, outgoing, arrived, results, returned, hidden, chain,
           pick, high, low,
           wsem, lsend, lrecv, psend, precv, dsend, drecv, bsend, brecv, csend, crecv):
    zs = n // SUB
    me = lax.axis_index("ep")
    hi, lo = me // SUB, me % SUB
    tok, width = tok_ref.shape
    ff = wg.shape[1]
    rows = SUB * cap
    dcols, rcols = width // KD, width // KR

    def peer(plane, part):
        return {"ep": plane * SUB + part}

    barrier = pltpu.get_barrier_semaphore()

    def greet(to):
        pl.semaphore_signal(barrier, inc=1, device_id=to, device_id_type=pl.DeviceIdType.MESH)

    for dl in range(1, SUB):
        greet(peer(hi, (lo + dl) % SUB))

    @pl.when(hi > 0)
    def _():
        greet(peer((hi + zs - 1) % zs, lo))

    @pl.when(hi < zs - 1)
    def _():
        greet(peer((hi + 1) % zs, lo))

    w_copies = [
        pltpu.make_async_copy(wg_ref.at[0], wg, wsem.at[0]),
        pltpu.make_async_copy(wu_ref.at[0], wu, wsem.at[1]),
        pltpu.make_async_copy(wd_ref.at[0], wd, wsem.at[2]),
    ]
    for c in w_copies:
        c.start()

    def remote(src, dst, send, recv, to):
        return pltpu.make_async_remote_copy(
            src_ref=src, dst_ref=dst, send_sem=send, recv_sem=recv,
            device_id=to, device_id_type=pl.DeviceIdType.MESH)

    def dcol(k):
        return pl.ds(pl.multiple_of(k * dcols, dcols), dcols)

    def rcol(k):
        return pl.ds(pl.multiple_of(k * rcols, rcols), rcols)

    def slot_rows(j, dl):
        return pl.ds(pl.multiple_of(j * rows + dl * cap, cap), cap)

    def block_rows(j):
        return pl.ds(pl.multiple_of(j * rows, rows), rows)

    def far_rows(j):
        return pl.ds(pl.multiple_of(j * rows + cap, cap), rows - cap)

    def onward(way):
        return (hi + 2 * way - 1 + zs) % zs

    def line_copy(block, k, way):
        part = lines.at[block, :, dcol(k)]
        return remote(part, part, lsend.at[way * zs + block], lrecv.at[block * KD + k],
                      peer(onward(way), lo))

    def place_copy(block, way):
        return remote(places.at[block], places.at[block], psend.at[way * zs + block],
                      precv.at[block], peer(onward(way), lo))

    def out_copy(j, dl, k):
        at = slot_rows(j, dl)
        return remote(outgoing.at[at, dcol(k)], arrived.at[at, dcol(k)],
                      dsend.at[j], drecv.at[j * KD + k], peer(hi, (lo + dl) % SUB))

    def out_arrival(j, k):
        at = arrived.at[far_rows(j), dcol(k)]
        return remote(at, at, dsend.at[j], drecv.at[j * KD + k], peer(hi, (lo + 1) % SUB))

    def back_copy(j, dl, k):
        at = slot_rows(j, dl)
        return remote(results.at[at, rcol(k)], returned.at[at, rcol(k)],
                      bsend.at[j], brecv.at[j * KR + k], peer(hi, (lo - dl + SUB) % SUB))

    def back_arrival(j, k):
        at = returned.at[far_rows(j), rcol(k)]
        return remote(at, at, bsend.at[j], brecv.at[j * KR + k], peer(hi, (lo + 1) % SUB))

    def chain_copy(way, j, k):
        part = chain.at[way * zs + j, :, rcol(k)]
        return remote(part, part, csend.at[way * zs + j], crecv.at[(way * zs + j) * KR + k],
                      peer(onward(way), lo))

    steps = []
    for codes in zip(*table):
        code = jnp.int32(codes[0])
        for plane in range(1, zs):
            code = jnp.where(hi == plane, codes[plane], code)
        steps.append(code)

    step = 32

    def norm(i, carry):
        at = pl.ds(pl.multiple_of(i * step, step), step)
        v = tok_ref[at, :].astype(jnp.float32)
        scale = lax.rsqrt(jnp.mean(v * v, -1, keepdims=True) + 1e-06)
        lines[hi, at, :] = (v * scale * gain_ref[...]).astype(jnp.bfloat16)
        return carry

    lax.fori_loop(0, tok // step, norm, 0)

    ends = jnp.where(hi == 0, 1, 0) + jnp.where(hi == zs - 1, 1, 0)
    pl.semaphore_wait(barrier, SUB + 1 - ends)

    def forward(way, act):
        @pl.when(jnp.where(way == 1, zs - 1 - hi, hi) > 0)
        def _():
            act(way)

    for way in (1, 0):
        forward(way, lambda w: line_copy(hi, 0, w).start())

    ids = ids_ref[...]
    id0, id1 = ids[:, 0:1], ids[:, 1:2]
    lane = lax.broadcasted_iota(jnp.int32, (tok, 128), 1)
    chosen = jnp.where((id0 == lane) | (id1 == lane), 1.0, 0.0)
    t_row = lax.broadcasted_iota(jnp.int32, (tok, tok), 0)
    t_col = lax.broadcasted_iota(jnp.int32, (tok, tok), 1)
    earlier = jnp.where(t_col < t_row, 1.0, 0.0).astype(jnp.bfloat16)
    before = jnp.dot(earlier, chosen.astype(jnp.bfloat16), preferred_element_type=jnp.float32)
    slot0 = jnp.sum(jnp.where(id0 == lane, before, 0.0), axis=1, keepdims=True)
    slot1 = jnp.sum(jnp.where(id1 == lane, before, 0.0), axis=1, keepdims=True)
    dest0 = id0.astype(jnp.float32) * cap + slot0
    dest1 = id1.astype(jnp.float32) * cap + slot1
    gw = gw_ref[...]
    g0, g1 = gw[:, 0:1], gw[:, 1:2]
    both = jnp.where(lane == 0, dest0, jnp.where(
        lane == 1, dest1, jnp.where(lane == 2, g0, jnp.where(lane == 3, g1, 0.0))))
    turned = jnp.transpose(both)
    where = lax.broadcasted_iota(jnp.int32, (8, tok), 0)
    places[hi] = jnp.where(
        where == 0, turned[0:1, :], jnp.where(
            where == 1, turned[1:2, :], jnp.where(where == 2, turned[2:3, :], turned[3:4, :])))

    def send_own(way):
        place_copy(hi, way).start()

    for way in (1, 0):
        forward(way, send_own)

    def row_index():
        r = lax.broadcasted_iota(jnp.int32, (rows, tok), 0)
        return ((hi * SUB + (lo + r // cap) % SUB) * cap + r % cap).astype(jnp.float32)

    def choose(j, at):
        index = row_index()
        w = places[j]
        pick[at] = jnp.where((index == w[0:1, :]) | (index == w[1:2, :]), 1.0, 0.0).astype(
            jnp.bfloat16)

    def pack(j, k, at):
        got = jnp.dot(pick[at], lines[j, :, dcol(k)],
                      preferred_element_type=jnp.float32).astype(jnp.bfloat16)
        outgoing[far_rows(j), dcol(k)] = got[cap:, :]
        for dl in range(1, SUB):
            out_copy(j, dl, k).start()
        arrived[slot_rows(j, 0), dcol(k)] = got[:cap, :]

    ftile = min(ff, 256)

    def landed(j, k, carry):
        out_arrival(j, k).wait_recv()
        return carry

    def up(j, f, carry):
        cols = pl.ds(pl.multiple_of(f * ftile, ftile), ftile)
        x = arrived[block_rows(j), :]
        g = jnp.dot(x, wg[:, cols], preferred_element_type=jnp.float32)
        u = jnp.dot(x, wu[:, cols], preferred_element_type=jnp.float32)
        hidden[j, :, cols] = (g / (1.0 + jnp.exp(-g)) * u).astype(jnp.bfloat16)
        return carry

    def down(j, k):
        got = jnp.dot(hidden[j], wd[:, rcol(k)],
                      preferred_element_type=jnp.float32).astype(jnp.bfloat16)
        results[far_rows(j), rcol(k)] = got[cap:, :]
        for dl in range(1, SUB):
            back_copy(j, dl, k).start()
        returned[slot_rows(j, 0), rcol(k)] = got[:cap, :]

    def weigh(j, at):
        index = row_index()
        w = places[j]
        weight = jnp.transpose(jnp.where(index == w[0:1, :], w[2:3, :], 0.0)
                               + jnp.where(index == w[1:2, :], w[3:4, :], 0.0))
        top = weight.astype(jnp.bfloat16)
        high[at] = top
        low[at] = (weight - top.astype(jnp.float32)).astype(jnp.bfloat16)

    def mix(j, k, at):
        block = returned[block_rows(j), rcol(k)]
        return (jnp.dot(high[at], block, preferred_element_type=jnp.float32)
                + jnp.dot(low[at], block, preferred_element_type=jnp.float32))

    def take(j, k):
        way = jnp.where(j < hi, 1, 0)

        @pl.when((k == 0) & (j != hi))
        def _():
            place_copy(j, way).wait_recv()
            forward(way, lambda w: place_copy(j, w).start())

        @pl.when(k == 0)
        def _():
            choose(j, j)

        @pl.when(j != hi)
        def _():
            line_copy(j, k, way).wait_recv()
            forward(way, lambda w: line_copy(j, k, w).start())

        pack(j, k, j)

    def up_all(j):
        lax.fori_loop(0, KD, lambda k, c: landed(j, k, c), 0)

        @pl.when(j == hi)
        def _():
            for c in w_copies:
                c.wait()

        lax.fori_loop(0, ff // ftile, lambda f, c: up(j, f, c), 0)

    def add(j, k):
        way = jnp.where(j > hi, 1, 0)

        @pl.when(k == 0)
        def _():
            weigh(j, j)

        back_arrival(j, k).wait_recv()
        value = mix(j, k, j)
        at = way * zs + j
        beyond = way * hi + (1 - way) * (zs - 1 - hi)

        @pl.when(beyond > 0)
        def _():
            chain_copy(way, j, k).wait_recv()
            chain[at, :, rcol(k)] = (
                value + chain[at, :, rcol(k)].astype(jnp.float32)).astype(jnp.bfloat16)

        @pl.when(beyond == 0)
        def _():
            chain[at, :, rcol(k)] = value.astype(jnp.bfloat16)

        chain_copy(way, j, k).start()

    def final(k):
        @pl.when(k == 0)
        def _():
            weigh(hi, hi)

        back_arrival(hi, k).wait_recv()
        value = mix(hi, k, hi)

        def arrived_from(way):
            chain_copy(way, hi, k).wait_recv()
            return chain[way * zs + hi, :, rcol(k)].astype(jnp.float32)

        def put(total):
            out_ref[:, rcol(k)] = total.astype(out_ref.dtype)

        @pl.when(hi == 0)
        def _():
            put(value + arrived_from(0))

        @pl.when(hi == zs - 1)
        def _():
            put(value + arrived_from(1))

        @pl.when((hi > 0) & (hi < zs - 1))
        def _():
            put(value + arrived_from(0) + arrived_from(1))

    def run(i, carry):
        code = steps[0]
        for at in range(1, len(steps)):
            code = jnp.where(i == at, steps[at], code)
        kind, j, k = code // 1024, code // 32 % 32, code % 32

        def on(name, act):
            @pl.when(kind == KINDS.index(name))
            def _():
                act()

        on("S", lambda: forward(1, lambda w: line_copy(hi, k, w).start()))
        on("Z", lambda: forward(0, lambda w: line_copy(hi, k, w).start()))
        on("T", lambda: take(j, k))
        on("U", lambda: up_all(j))
        on("D", lambda: down(j, k))
        on("M", lambda: add(j, k))
        on("F", lambda: final(k))
        return carry

    lax.fori_loop(0, len(table[0]), run, 0)

    def finish(j, carry):
        at = far_rows(j)
        remote(outgoing.at[at, :], outgoing.at[at, :], dsend.at[j], drecv.at[0],
               peer(hi, (lo + 1) % SUB)).wait_send()
        remote(results.at[at, :], results.at[at, :], bsend.at[j], brecv.at[0],
               peer(hi, (lo + 1) % SUB)).wait_send()
        for way in (0, 1):
            to = peer(onward(way), lo)

            @pl.when((hi < zs - 1) & (j <= hi) if way else (hi > 0) & (j >= hi))
            def _():
                place_copy(j, way).wait_send()
                remote(lines.at[j], lines.at[j], lsend.at[way * zs + j], lrecv.at[0],
                       to).wait_send()

            @pl.when(j > hi if way else j < hi)
            def _():
                at = way * zs + j
                remote(chain.at[at], chain.at[at], csend.at[at], crecv.at[0], to).wait_send()

        return carry

    lax.fori_loop(0, zs, finish, 0)


def per_device(tokens, norm_gain, expert_ids, gate_weights, w_gate, w_up, w_down):
    n = lax.axis_size("ep")
    tok, width = tokens.shape
    top = expert_ids.shape[1]
    ff = w_gate.shape[2]
    cap = 2 * tok * top // n
    total = n * cap
    zs = n // SUB
    rows = SUB * cap
    table = tables(zs)
    bf16 = jnp.bfloat16
    dma = pltpu.SemaphoreType.DMA
    vmem = pl.BlockSpec(memory_space=pltpu.VMEM)
    hbm = pl.BlockSpec(memory_space=pl.ANY)
    return pl.pallas_call(
        functools.partial(kernel, n, cap, table),
        out_shape=jax.ShapeDtypeStruct((tok, width), bf16),
        in_specs=[vmem] * 4 + [hbm] * 3,
        out_specs=vmem,
        scratch_shapes=[
            pltpu.VMEM((width, ff), bf16),
            pltpu.VMEM((width, ff), bf16),
            pltpu.VMEM((ff, width), bf16),
            pltpu.VMEM((zs, tok, width), bf16),
            pltpu.VMEM((zs, 8, tok), jnp.float32),
            pltpu.VMEM((total, width), bf16),
            pltpu.VMEM((total, width), bf16),
            pltpu.VMEM((total, width), bf16),
            pltpu.VMEM((total, width), bf16),
            pltpu.VMEM((zs, rows, ff), bf16),
            pltpu.VMEM((2 * zs, tok, width), bf16),
            pltpu.VMEM((zs, rows, tok), bf16),
            pltpu.VMEM((zs, tok, rows), bf16),
            pltpu.VMEM((zs, tok, rows), bf16),
            dma((3,)),
            dma((2 * zs,)),
            dma((zs * KD,)),
            dma((2 * zs,)),
            dma((zs,)),
            dma((zs,)),
            dma((zs * KD,)),
            dma((zs,)),
            dma((zs * KR,)),
            dma((2 * zs,)),
            dma((2 * zs * KR,)),
        ],
        compiler_params=pltpu.CompilerParams(
            collective_id=0, has_side_effects=True, vmem_limit_bytes=62 * 1024 * 1024),
    )(tokens, norm_gain.reshape(1, width), expert_ids, gate_weights, w_gate, w_up, w_down)


def solution(mesh):
    return jax.shard_map(
        per_device,
        mesh=mesh,
        in_specs=(
            P(("grp", "ep"), None),
            P(),
            P(("grp", "ep"), None),
            P(("grp", "ep"), None),
            P("ep", None, None),
            P("ep", None, None),
            P("ep", None, None),
        ),
        out_specs=P(("grp", "ep"), None),
        check_vma=False,
    )
```

```python
import functools
import heapq
import jax
import jax.numpy as jnp
from jax import lax
from jax.experimental import pallas as pl
from jax.experimental.pallas import tpu as pltpu
from jax.sharding import PartitionSpec as P

SUB = 4
KD = 8
KR = 8
PIECES = 4
KINDS = "SZTUDMFWX"
COST = {"S": 0.0, "Z": 0.0, "T": 0.9, "U": 3.1, "D": 1.8, "M": 1.25, "F": 1.4}
RANK = {"S": 0, "Z": 0, "T": 1, "M": 2, "F": 3, "D": 4, "U": 5}
Z_BLOCK, Y_BLOCK, LAG, START, PACK, STEP = 22.6, 11.2, 2.2, 2.9, 3.6, 0.12
PRIO = {(0, 'D', 2): 4.8, (1, 'U', 3): 4.7, (0, 'U', 1): 0.6}
HOLD = {(1, 'Z', 1): 54, (1, 'Z', 2): 68, (1, 'Z', 3): 70, (0, 'D', 0): 88, (1, 'U', 1): 68, (1, 'T', 1): 7, (1, 'D', 0): 62}


def tables(zs):
    half = zs // 2
    need, when, ready = {}, {}, [[] for _ in range(half)]
    order = [[] for _ in range(half)]
    pieces = {"T": KD, "D": KR, "M": KR, "F": KR}

    def release(h, name, b, k):
        key = (h, name, k * 4 // KD) if name in "SZ" else (h, name, b)
        rank = -1.0 if name in "SZ" and k == 0 else PRIO.get(key, RANK[name])
        at = max(when[h, name, b, k], HOLD.get(key, 0.0))
        ready[h].append((rank + 0.01 * k, abs(b - h), name, b, k, at))

    def task(h, name, b, k, deps, at=0.0):
        need[h, name, b, k], when[h, name, b, k] = deps, at
        if deps == 0:
            release(h, name, b, k)

    for h in range(half):
        for b in range(zs):
            for k in range(KD):
                task(h, "T", b, k, int(b != h), PACK if b == h else 0.0)
            task(h, "U", b, 0, KD)
            for k in range(KR):
                task(h, "D", b, k, 1)
                if b == h:
                    task(h, "F", b, k, 1 + (h > 0) + (h < zs - 1))
                else:
                    task(h, "M", b, k, 1 + (h > 0 if b > h else h < zs - 1))
        for k in range(KD):
            task(h, "S", h, k, 0, START)
            if h > 0:
                task(h, "Z", h, k, 0, START)
    busy, link = [0.0] * half, {}
    events = [(at, h) for at in (START, PACK) for h in range(half)]

    def supply(h, name, b, k, at):
        if h >= half:
            h, b = zs - 1 - h, zs - 1 - b
        need[h, name, b, k] -= 1
        when[h, name, b, k] = max(when[h, name, b, k], at)
        if need[h, name, b, k] == 0:
            release(h, name, b, k)
        heapq.heappush(events, (at, h))

    def wire(key, time, at):
        link[key] = max(at, link.get(key, 0.0)) + time
        return link[key] + LAG

    def onward(h, way, b, k, name, time, at):
        g = h + 2 * way - 1
        supply(g, "F" if name == "M" and g == b else name, b, k, wire((h, way), time, at))

    heapq.heapify(events)
    while events:
        t, h = heapq.heappop(events)
        if busy[h] > t + 1e-9:
            continue
        now = [c for c in ready[h] if c[5] <= t + 1e-9]
        if not now:
            if ready[h]:
                heapq.heappush(events, (min(c[5] for c in ready[h]), h))
            continue
        best = min(now)
        ready[h].remove(best)
        name, b, k = best[2:5]
        order[h].append((name, b, k))
        done = t + STEP + COST[name] / pieces.get(name, 1)
        if name in "SZ":
            onward(h, int(name == "S"), b, k, "T", Z_BLOCK / KD, t + 0.05)
        elif name == "T":
            way = int(b < h)
            if b != h and (h < zs - 1 if way else h > 0):
                onward(h, way, b, k, "T", Z_BLOCK / KD, t + 0.1)
            supply(h, "U", b, 0, wire(h, Y_BLOCK / KD, done))
        elif name == "U":
            for r in range(KR):
                supply(h, "D", b, r, done)
        elif name == "D":
            supply(h, "F" if b == h else "M", b, k, wire(h, Y_BLOCK / KR, done))
        elif name == "M":
            onward(h, int(b > h), b, k, "M", Z_BLOCK / KR, done)
        busy[h] = done
        heapq.heappush(events, (done, h))
    assert sum(map(len, order)) == len(need)

    def code(name, b, k):
        return KINDS.index(name) * 1024 + b * 32 + k

    def mirror(name, b, k):
        return {"S": "Z", "Z": "S"}.get(name, name), zs - 1 - b, k

    order = [[c for c in o if c[0] not in "SZ" or c[2] > 0] for o in order]
    for o in order:
        o.insert([c[0] for c in o].index("U"), ("W", 0, 0))
    order += [[mirror(*c) for c in o] for o in reversed(order)]
    size = max(map(len, order))
    return [[code(*c) for c in o] + [code("X", 0, 0)] * (size - len(o)) for o in order]


def kernel(n, cap, table, tok_ref, gain_ref, ids_ref, gw_ref, wg_ref, wu_ref, wd_ref, out_ref,
           wg, wu, wd, lines, places, outgoing, arrived, results, returned, hidden, chain,
           pick, high, low, raw,
           tsem, wsem, lsend, lrecv, psend, precv, dsend, drecv, bsend, brecv, csend, crecv):
    zs = n // SUB
    me = lax.axis_index("ep")
    hi, lo = me // SUB, me % SUB
    tok, width = tok_ref.shape
    ff = wg.shape[1]
    rows = SUB * cap
    dcols, rcols = width // KD, width // KR

    def peer(plane, part):
        return {"ep": plane * SUB + part}

    pieces = [pl.ds(i * (tok // PIECES), tok // PIECES) for i in range(PIECES)]
    t_copies = [pltpu.make_async_copy(tok_ref.at[at, :], raw.at[at, :], tsem.at[i])
                for i, at in enumerate(pieces)]
    for c in t_copies:
        c.start()

    barrier = pltpu.get_barrier_semaphore()

    def greet(to):
        pl.semaphore_signal(barrier, inc=1, device_id=to, device_id_type=pl.DeviceIdType.MESH)

    for dl in range(1, SUB):
        greet(peer(hi, (lo + dl) % SUB))

    @pl.when(hi > 0)
    def _():
        greet(peer((hi + zs - 1) % zs, lo))

    @pl.when(hi < zs - 1)
    def _():
        greet(peer((hi + 1) % zs, lo))

    w_copies = [
        pltpu.make_async_copy(wg_ref.at[0], wg, wsem.at[0]),
        pltpu.make_async_copy(wu_ref.at[0], wu, wsem.at[1]),
        pltpu.make_async_copy(wd_ref.at[0], wd, wsem.at[2]),
    ]
    for c in w_copies:
        c.start()

    def remote(src, dst, send, recv, to):
        return pltpu.make_async_remote_copy(
            src_ref=src, dst_ref=dst, send_sem=send, recv_sem=recv,
            device_id=to, device_id_type=pl.DeviceIdType.MESH)

    def dcol(k):
        return pl.ds(pl.multiple_of(k * dcols, dcols), dcols)

    def rcol(k):
        return pl.ds(pl.multiple_of(k * rcols, rcols), rcols)

    def slot_rows(j, dl):
        return pl.ds(pl.multiple_of(j * rows + dl * cap, cap), cap)

    def block_rows(j):
        return pl.ds(pl.multiple_of(j * rows, rows), rows)

    def far_rows(j):
        return pl.ds(pl.multiple_of(j * rows + cap, cap), rows - cap)

    def onward(way):
        return (hi + 2 * way - 1 + zs) % zs

    def line_copy(block, k, way):
        part = lines.at[block, :, dcol(k)]
        return remote(part, part, lsend.at[way * zs + block], lrecv.at[block * KD + k],
                      peer(onward(way), lo))

    def place_copy(block, way):
        return remote(places.at[block], places.at[block], psend.at[way * zs + block],
                      precv.at[block], peer(onward(way), lo))

    def out_copy(j, dl, k):
        at = slot_rows(j, dl)
        return remote(outgoing.at[at, dcol(k)], arrived.at[at, dcol(k)],
                      dsend.at[j], drecv.at[j * KD + k], peer(hi, (lo + dl) % SUB))

    def out_arrival(j, k):
        at = arrived.at[far_rows(j), dcol(k)]
        return remote(at, at, dsend.at[j], drecv.at[j * KD + k], peer(hi, (lo + 1) % SUB))

    def back_copy(j, dl, k):
        at = slot_rows(j, dl)
        return remote(results.at[at, rcol(k)], returned.at[at, rcol(k)],
                      bsend.at[j], brecv.at[j * KR + k], peer(hi, (lo - dl + SUB) % SUB))

    def back_arrival(j, k):
        at = returned.at[far_rows(j), rcol(k)]
        return remote(at, at, bsend.at[j], brecv.at[j * KR + k], peer(hi, (lo + 1) % SUB))

    def chain_copy(way, j, k):
        part = chain.at[way * zs + j, :, rcol(k)]
        return remote(part, part, csend.at[way * zs + j], crecv.at[(way * zs + j) * KR + k],
                      peer(onward(way), lo))

    steps = []
    for codes in zip(*table):
        code = jnp.int32(codes[0])
        for plane in range(1, zs):
            code = jnp.where(hi == plane, codes[plane], code)
        steps.append(code)

    step = 32

    def norm(i, carry):
        at = pl.ds(pl.multiple_of(i * step, step), step)
        v = raw[at, :].astype(jnp.float32)
        scale = lax.rsqrt(jnp.mean(v * v, -1, keepdims=True) + 1e-06)
        lines[hi, at, :] = (v * scale * gain_ref[...]).astype(jnp.bfloat16)
        return carry

    per = tok // PIECES // step
    for i, c in enumerate(t_copies):
        c.wait()
        lax.fori_loop(i * per, (i + 1) * per, norm, 0)

    ends = jnp.where(hi == 0, 1, 0) + jnp.where(hi == zs - 1, 1, 0)
    pl.semaphore_wait(barrier, SUB + 1 - ends)

    def forward(way, act):
        @pl.when(jnp.where(way == 1, zs - 1 - hi, hi) > 0)
        def _():
            act(way)

    for way in (1, 0):
        forward(way, lambda w: line_copy(hi, 0, w).start())

    expert = lax.broadcasted_iota(jnp.int32, (n, tok), 0)
    id0, id1 = ids_ref[0:1, :], ids_ref[1:2, :]
    chosen = jnp.where((id0 == expert) | (id1 == expert), 1.0, 0.0).astype(jnp.bfloat16)
    t_row = lax.broadcasted_iota(jnp.int32, (tok, tok), 0)
    t_col = lax.broadcasted_iota(jnp.int32, (tok, tok), 1)
    earlier = jnp.where(t_row < t_col, 1.0, 0.0).astype(jnp.bfloat16)
    before = jnp.dot(chosen, earlier, preferred_element_type=jnp.float32)

    def dest(ids):
        slot = jnp.sum(jnp.where(ids == expert, before, 0.0), axis=0, keepdims=True)
        return ids.astype(jnp.float32) * cap + slot

    where = lax.broadcasted_iota(jnp.int32, (8, tok), 0)
    places[hi] = jnp.where(
        where == 0, dest(id0), jnp.where(
            where == 1, dest(id1), jnp.where(where == 2, gw_ref[0:1, :], gw_ref[1:2, :])))

    def send_own(way):
        place_copy(hi, way).start()

    for way in (1, 0):
        forward(way, send_own)

    def row_index():
        r = lax.broadcasted_iota(jnp.int32, (rows, tok), 0)
        return ((hi * SUB + (lo + r // cap) % SUB) * cap + r % cap).astype(jnp.float32)

    def choose(j, at):
        index = row_index()
        w = places[j]
        pick[at] = jnp.where((index == w[0:1, :]) | (index == w[1:2, :]), 1.0, 0.0).astype(
            jnp.bfloat16)

    def pack(j, k, at):
        got = jnp.dot(pick[at], lines[j, :, dcol(k)],
                      preferred_element_type=jnp.float32).astype(jnp.bfloat16)
        outgoing[far_rows(j), dcol(k)] = got[cap:, :]
        for dl in range(1, SUB):
            out_copy(j, dl, k).start()
        arrived[slot_rows(j, 0), dcol(k)] = got[:cap, :]

    ftile = min(ff, 256)

    def landed(j, k, carry):
        out_arrival(j, k).wait_recv()
        return carry

    def up(j, f, carry):
        cols = pl.ds(pl.multiple_of(f * ftile, ftile), ftile)
        x = arrived[block_rows(j), :]
        g = jnp.dot(x, wg[:, cols], preferred_element_type=jnp.float32)
        u = jnp.dot(x, wu[:, cols], preferred_element_type=jnp.float32)
        hidden[j, :, cols] = (g / (1.0 + jnp.exp(-g)) * u).astype(jnp.bfloat16)
        return carry

    def down(j, k):
        got = jnp.dot(hidden[j], wd[:, rcol(k)],
                      preferred_element_type=jnp.float32).astype(jnp.bfloat16)
        results[far_rows(j), rcol(k)] = got[cap:, :]
        for dl in range(1, SUB):
            back_copy(j, dl, k).start()
        returned[slot_rows(j, 0), rcol(k)] = got[:cap, :]

    def weigh(j, at):
        index = row_index()
        w = places[j]
        weight = jnp.transpose(jnp.where(index == w[0:1, :], w[2:3, :], 0.0)
                               + jnp.where(index == w[1:2, :], w[3:4, :], 0.0))
        top = weight.astype(jnp.bfloat16)
        high[at] = top
        low[at] = (weight - top.astype(jnp.float32)).astype(jnp.bfloat16)

    def mix(j, k, at):
        block = returned[block_rows(j), rcol(k)]
        return (jnp.dot(high[at], block, preferred_element_type=jnp.float32)
                + jnp.dot(low[at], block, preferred_element_type=jnp.float32))

    def take(j, k):
        way = jnp.where(j < hi, 1, 0)

        @pl.when((k == 0) & (j != hi))
        def _():
            place_copy(j, way).wait_recv()
            forward(way, lambda w: place_copy(j, w).start())

        @pl.when(k == 0)
        def _():
            choose(j, j)

        @pl.when(j != hi)
        def _():
            line_copy(j, k, way).wait_recv()
            forward(way, lambda w: line_copy(j, k, w).start())

        pack(j, k, j)

    def up_all(j):
        lax.fori_loop(0, KD, lambda k, c: landed(j, k, c), 0)

        lax.fori_loop(0, ff // ftile, lambda f, c: up(j, f, c), 0)

    def add(j, k):
        way = jnp.where(j > hi, 1, 0)

        @pl.when(k == 0)
        def _():
            weigh(j, j)

        back_arrival(j, k).wait_recv()
        value = mix(j, k, j)
        at = way * zs + j
        beyond = way * hi + (1 - way) * (zs - 1 - hi)

        @pl.when(beyond > 0)
        def _():
            chain_copy(way, j, k).wait_recv()
            chain[at, :, rcol(k)] = (
                value + chain[at, :, rcol(k)].astype(jnp.float32)).astype(jnp.bfloat16)

        @pl.when(beyond == 0)
        def _():
            chain[at, :, rcol(k)] = value.astype(jnp.bfloat16)

        chain_copy(way, j, k).start()

    def final(k):
        @pl.when(k == 0)
        def _():
            weigh(hi, hi)

        back_arrival(hi, k).wait_recv()
        value = mix(hi, k, hi)

        def arrived_from(way):
            chain_copy(way, hi, k).wait_recv()
            return chain[way * zs + hi, :, rcol(k)].astype(jnp.float32)

        def put(total):
            out_ref[:, rcol(k)] = total.astype(out_ref.dtype)

        @pl.when(hi == 0)
        def _():
            put(value + arrived_from(0))

        @pl.when(hi == zs - 1)
        def _():
            put(value + arrived_from(1))

        @pl.when((hi > 0) & (hi < zs - 1))
        def _():
            put(value + arrived_from(0) + arrived_from(1))

    def run(i, carry):
        code = steps[0]
        for at in range(1, len(steps)):
            code = jnp.where(i == at, steps[at], code)
        kind, j, k = code // 1024, code // 32 % 32, code % 32

        def on(name, act):
            @pl.when(kind == KINDS.index(name))
            def _():
                act()

        on("S", lambda: forward(1, lambda w: line_copy(hi, k, w).start()))
        on("Z", lambda: forward(0, lambda w: line_copy(hi, k, w).start()))
        on("T", lambda: take(j, k))
        on("U", lambda: up_all(j))
        on("W", lambda: [c.wait() for c in w_copies])
        on("D", lambda: down(j, k))
        on("M", lambda: add(j, k))
        on("F", lambda: final(k))
        return carry

    lax.fori_loop(0, len(table[0]), run, 0)

    def finish(j, carry):
        at = far_rows(j)
        remote(outgoing.at[at, :], outgoing.at[at, :], dsend.at[j], drecv.at[0],
               peer(hi, (lo + 1) % SUB)).wait_send()
        remote(results.at[at, :], results.at[at, :], bsend.at[j], brecv.at[0],
               peer(hi, (lo + 1) % SUB)).wait_send()
        for way in (0, 1):
            to = peer(onward(way), lo)

            @pl.when((hi < zs - 1) & (j <= hi) if way else (hi > 0) & (j >= hi))
            def _():
                place_copy(j, way).wait_send()
                remote(lines.at[j], lines.at[j], lsend.at[way * zs + j], lrecv.at[0],
                       to).wait_send()

            @pl.when(j > hi if way else j < hi)
            def _():
                at = way * zs + j
                remote(chain.at[at], chain.at[at], csend.at[at], crecv.at[0], to).wait_send()

        return carry

    lax.fori_loop(0, zs, finish, 0)


def per_device(tokens, norm_gain, expert_ids, gate_weights, w_gate, w_up, w_down):
    n = lax.axis_size("ep")
    tok, width = tokens.shape
    top = expert_ids.shape[1]
    ff = w_gate.shape[2]
    cap = 2 * tok * top // n
    total = n * cap
    zs = n // SUB
    rows = SUB * cap
    table = tables(zs)
    bf16 = jnp.bfloat16
    dma = pltpu.SemaphoreType.DMA
    vmem = pl.BlockSpec(memory_space=pltpu.VMEM)
    hbm = pl.BlockSpec(memory_space=pl.ANY)
    return pl.pallas_call(
        functools.partial(kernel, n, cap, table),
        out_shape=pltpu.VMEM((tok, width), bf16),
        in_specs=[hbm] + [vmem] * 3 + [hbm] * 3,
        out_specs=vmem,
        scratch_shapes=[
            pltpu.VMEM((width, ff), bf16),
            pltpu.VMEM((width, ff), bf16),
            pltpu.VMEM((ff, width), bf16),
            pltpu.VMEM((zs, tok, width), bf16),
            pltpu.VMEM((zs, 8, tok), jnp.float32),
            pltpu.VMEM((total, width), bf16),
            pltpu.VMEM((total, width), bf16),
            pltpu.VMEM((total, width), bf16),
            pltpu.VMEM((total, width), bf16),
            pltpu.VMEM((zs, rows, ff), bf16),
            pltpu.VMEM((2 * zs, tok, width), bf16),
            pltpu.VMEM((zs, rows, tok), bf16),
            pltpu.VMEM((zs, tok, rows), bf16),
            pltpu.VMEM((zs, tok, rows), bf16),
            pltpu.VMEM((tok, width), bf16),
            dma((PIECES,)),
            dma((3,)),
            dma((2 * zs,)),
            dma((zs * KD,)),
            dma((2 * zs,)),
            dma((zs,)),
            dma((zs,)),
            dma((zs * KD,)),
            dma((zs,)),
            dma((zs * KR,)),
            dma((2 * zs,)),
            dma((2 * zs * KR,)),
        ],
        compiler_params=pltpu.CompilerParams(
            collective_id=0, has_side_effects=True, vmem_limit_bytes=58 * 1024 * 1024),
    )(tokens, norm_gain.reshape(1, width), expert_ids.T, gate_weights.T, w_gate, w_up, w_down)


def solution(mesh):
    return jax.shard_map(
        per_device,
        mesh=mesh,
        in_specs=(
            P(("grp", "ep"), None),
            P(),
            P(("grp", "ep"), None),
            P(("grp", "ep"), None),
            P("ep", None, None),
            P("ep", None, None),
            P("ep", None, None),
        ),
        out_specs=P(("grp", "ep"), None),
        check_vma=False,
    )
```

```python
import bisect
import functools
import heapq
import jax
import jax.numpy as jnp
from jax import lax
from jax.experimental import pallas as pl
from jax.experimental.pallas import tpu as pltpu
from jax.sharding import PartitionSpec as P

SUB = 4
KD = 8
KR = 8
PIECES = 4
GROUP = 8
KINDS = "SZGTUVDEMFWNQX"
COST = {"T": 1.76, "U": 2.5, "V": 2.5, "D": 1.4, "E": 1.4, "M": 1.9, "F": 2.0}
RANK = {"S": 0, "Z": 0, "G": 0.5, "T": 1, "N": -1, "M": 2, "F": 3, "D": 4, "E": 4, "U": 5, "V": 5}
Z_BLOCK, Y_BLOCK, LAG, START, PACK, STEP, BACKLOG = 11.3, 5.6, 2.2, 2.9, 4.6, 0.16, 3.0
HANDOVER = 2
PRIO = {(0, 0, 'D', 1): 1.4,
 (0, 0, 'D', 2): 5.6,
 (0, 0, 'D', 3): 1.2,
 (0, 0, 'E', 3): 1.2,
 (0, 0, 'M', 1): 0.5,
 (0, 0, 'M', 2): 4.1,
 (0, 0, 'S', 0): 3.2,
 (0, 0, 'S', 1): 4.0,
 (0, 0, 'S', 3): 1.7,
 (0, 0, 'T', 1): 3.2,
 (0, 0, 'T', 2): 3.5,
 (0, 0, 'U', 1): 4.7,
 (0, 0, 'U', 3): 1.4,
 (0, 1, 'D', 0): 4.3,
 (0, 1, 'D', 2): 0.4,
 (0, 1, 'D', 3): 2.8,
 (0, 1, 'E', 2): 1.0,
 (0, 1, 'M', 2): 0.0,
 (0, 1, 'M', 3): 0.3,
 (0, 1, 'S', 0): 0.5,
 (0, 1, 'S', 1): 3.9,
 (0, 1, 'T', 1): 2.3,
 (0, 1, 'V', 2): 3.3,
 (1, 0, 'E', 2): 4.8,
 (1, 0, 'E', 3): 2.5,
 (1, 0, 'S', 1): 3.4,
 (1, 0, 'S', 2): 2.0,
 (1, 0, 'T', 1): 4.7,
 (1, 0, 'U', 1): 2.3,
 (1, 0, 'V', 1): 0.1,
 (1, 0, 'Z', 1): 0.3,
 (1, 0, 'Z', 2): 1.8,
 (1, 1, 'E', 0): 5.5,
 (1, 1, 'E', 1): 3.0,
 (1, 1, 'E', 3): 0.2,
 (1, 1, 'G', 3): 3.5,
 (1, 1, 'S', 0): 4.1,
 (1, 1, 'S', 1): 4.5,
 (1, 1, 'S', 2): 3.7,
 (1, 1, 'T', 1): 4.7,
 (1, 1, 'T', 2): 5.0,
 (1, 1, 'U', 3): 5.5,
 (1, 1, 'V', 2): 5.4,
 (1, 1, 'Z', 0): 5.3}
HOLD = {(0, 0, 'E', 2): 81,
 (0, 1, 'D', 0): 64,
 (0, 1, 'S', 3): 23,
 (0, 1, 'U', 2): 79,
 (0, 1, 'V', 0): 60,
 (1, 0, 'D', 3): 52,
 (1, 0, 'E', 0): 66,
 (1, 0, 'G', 2): 38,
 (1, 0, 'S', 0): 26,
 (1, 0, 'U', 0): 64,
 (1, 0, 'U', 1): 67,
 (1, 0, 'U', 3): 34,
 (1, 0, 'V', 1): 57,
 (1, 1, 'D', 1): 83,
 (1, 1, 'S', 3): 29,
 (1, 1, 'T', 1): 33,
 (1, 1, 'U', 2): 87,
 (1, 1, 'Z', 2): 64}


def plan(zs):
    half = zs // 2
    cores = [(h, c) for h in range(half) for c in (0, 1)]
    need, when, ready = {}, {}, {d: [] for d in cores}
    order = {d: [] for d in cores}
    pieces = {"T": KD, "D": KR, "E": KR, "M": KR, "F": KR}
    events, busy, links, turn = [], dict.fromkeys(cores, 0.0), {}, [0]

    def post(at, what, key):
        turn[0] += 1
        heapq.heappush(events, (at, turn[0], what, key))

    def way_of(h, name, b):
        if name == "S" or (name == "G" and b < h) or (name == "M" and b > h):
            return h, 1
        if name in "ZGM":
            return h, 0
        return (h, 2) if name in "DE" else None

    def release(d, name, b, k):
        key = d + ((name, k * 4 // KD) if name in "SZ" else (name, b))
        at = max(when[d, name, b, k], HOLD.get(key, 0.0))
        if name in "SZ" and k + d[1] == 0:
            key, at = (), START
        bisect.insort(ready[d], (PRIO.get(key, RANK[name]) + 0.01 * k, abs(b - d[0]), name, b, k,
                                 at, way_of(d[0], name, b)))

    def task(d, name, b, k, deps, at=0.0):
        need[d, name, b, k], when[d, name, b, k] = deps, at
        if deps == 0:
            release(d, name, b, k)

    for d in cores:
        h, c = d
        for b in range(zs):
            for k in range(KD):
                task(d, "T", b, k, int(b != h), PACK if b == h else 0.0)
                if b != h and (h < zs - 1 if b < h else h > 0):
                    task(d, "G", b, k, 1)
            for name, other in (("U", "D"), ("V", "E")):
                task(d, name, b, 0, KD)
                for k in range(KR):
                    task(d, other, b, k, 1)
            for k in range(KR):
                if b == h:
                    task(d, "F", b, k, 2 + (h > 0) + (h < zs - 1))
                else:
                    task(d, "M", b, k, 2 + (h > 0 if b > h else h < zs - 1))
        if c == 0:
            task(d, "N", h + 1, 0, 1)
        for k in range(KD):
            for name in "SZ" if h > 0 else "S":
                task(d, name, h, k, c + (k > 0), START)
        post(START, "core", d)
        post(PACK, "core", d)

    def supply(d, name, b, k, at):
        if d[0] >= half:
            d, b = (zs - 1 - d[0], d[1]), zs - 1 - b
        key = (d, name, b, k)
        need[key] -= 1
        when[key] = max(when[key], at)
        if need[key] == 0:
            release(*key)
        post(at, "core", d)

    def settle(key, t):
        lk = links[key]
        live = [q for q in lk["queues"] if q]
        for q in live:
            q[0][0] -= (t - lk["at"]) / len(live)
        lk["at"] = t
        for q in live:
            while q and q[0][0] <= 1e-6:
                for e in q.pop(0)[1]:
                    supply(*e, t + LAG)
        lk["stamp"] += 1
        live = [q for q in lk["queues"] if q]
        if live:
            post(t + min(q[0][0] for q in live) * len(live), "link", (key, lk["stamp"]))

    def wire(key, c, time, t, targets):
        lk = links.setdefault(key, {"at": 0.0, "queues": ([], []), "stamp": 0})
        if any(lk["queues"]):
            settle(key, t)
        lk["at"] = t
        lk["queues"][c].append([time, targets])
        settle(key, t)

    def backlog(key, c, t):
        lk = links.get(key)
        if lk is None:
            return 0.0
        return sum(x[0] for x in lk["queues"][c]) * sum(map(bool, lk["queues"]))

    def onward(h, c, way, b, k, name, time, t):
        g = h + 2 * way - 1
        wire((h, way), c, time, t, [((g, c), "F" if name == "M" and g == b else name, b, k)])

    def pick(d, t):
        later, full = None, {}
        for i, x in enumerate(ready[d]):
            at, gate = x[5:]
            if at <= t + 1e-9 and gate is not None:
                if gate not in full:
                    full[gate] = backlog(gate, d[1], t) - BACKLOG
                at = t + full[gate] if full[gate] > 1e-6 else at
            if at <= t + 1e-9:
                return ready[d].pop(i)[2:5]
            later = at if later is None else min(later, at)
        if later is not None:
            post(max(later, t + 0.1), "core", d)
        return None

    while events:
        t, _, what, key = heapq.heappop(events)
        if what == "link":
            if links[key[0]]["stamp"] == key[1]:
                settle(key[0], t)
            continue
        d = key
        if busy[d] > t + 1e-9:
            continue
        choice = pick(d, t)
        if choice is None:
            continue
        h, c = d
        name, b, k = choice
        order[d].append(choice)
        done = t + STEP + COST.get(name, 0.0) / pieces.get(name, 1)
        done += 0.25 if k == 0 and name in "TM" else 0.0
        if name in "SZ":
            onward(h, c, int(name == "S"), b, k, "T", Z_BLOCK / KD, t)
            if k + 1 < KD:
                supply(d, name, b, k + 1, done)
        elif name == "G":
            onward(h, c, int(b < h), b, k, "T", Z_BLOCK / KD, t)
        elif name == "T":
            if (d, "G", b, k) in need:
                supply(d, "G", b, k, done)
            if c == 0 and b == h + 1 and k == KD * HANDOVER // 8:
                supply(d, "N", b, 0, done)
            wire((h, 2), c, Y_BLOCK / KD, t, [(d, "U", b, 0), ((h, 1 - c), "V", b, 0)])
        elif name == "N":
            for r in range(KD):
                for s in "SZ" if h > 0 else "S":
                    supply((h, 1), s, h, r, done + 0.3)
        elif name in "UV":
            for r in range(KR):
                supply(d, "D" if name == "U" else "E", b, r, done)
        elif name in "DE":
            wire((h, 2), c, Y_BLOCK / KR / 2, t + STEP,
                 [((h, c if name == "D" else 1 - c), "F" if b == h else "M", b, k)])
        elif name == "M":
            onward(h, c, int(b > h), b, k, "M", Z_BLOCK / KR, t + STEP)
        busy[d] = done
        post(done, "core", d)
    assert sum(map(len, order.values())) == len(need)
    return order


def tables(zs):
    order = plan(zs)

    def code(name, b, k):
        return (KINDS.index(name) * zs + b) * max(KD, KR) + k

    def listed(h, c):
        todo = list(order[min(h, zs - 1 - h), c])
        if h >= zs // 2:
            todo = [({"S": "Z", "Z": "S"}.get(name, name), zs - 1 - b, k) for name, b, k in todo]
        if c == 0:
            todo = [x for x in todo if x[0] not in "SZ" or x[2] > 0]
        names = [x[0] for x in todo]
        first = min(names.index("U"), names.index("V"))
        todo.insert(first, ("W", 0, 0))
        if c == 1:
            turn = min(i for i, x in enumerate(todo) if x[0] in "SZ")
            todo.insert(turn, ("Q", 0, 0))
        return todo

    lists = [listed(h, c) for h in range(zs) for c in (0, 1)]
    size = max(map(len, lists))
    size += -size % 3
    return [[code(*x) for x in o] + [code("X", 0, 0)] * (size - len(o)) for o in lists]


def kernel(n, cap, table, tok_ref, gain_ref, ids_ref, gw_ref, wg_ref, wu_ref, wd_ref, out_ref,
           wg, wu, wd, lines, places, outgoing, arrived, results, returned, hidden, chain,
           pick, high, low, raw,
           tsem, wsem, lsend, lrecv, psend, precv, dsend, drecv, bsend, brecv, csend, crecv, turn):
    zs = n // SUB
    me = lax.axis_index("ep")
    hi, lo = me // SUB, me % SUB
    core = lo % 2
    tok, width = tok_ref.shape
    ff = wg.shape[1]
    rows = SUB * cap
    dcols, rcols = width // KD, width // KR

    def peer(plane, part):
        return {"ep": plane * SUB + part}

    pieces = [pl.ds(i * (tok // PIECES), tok // PIECES) for i in range(PIECES)]
    t_copies = [pltpu.make_async_copy(tok_ref.at[at, :], raw.at[at, :], tsem.at[i])
                for i, at in enumerate(pieces)]
    for c in t_copies:
        c.start()

    barrier = pltpu.get_barrier_semaphore()

    def greet(to):
        pl.semaphore_signal(barrier, inc=1, device_id=to, device_id_type=pl.DeviceIdType.MESH)

    for dl in range(1, SUB):
        greet(peer(hi, (lo + dl) % SUB))

    @pl.when(hi > 0)
    def _():
        greet(peer((hi + zs - 1) % zs, lo))

    @pl.when(hi < zs - 1)
    def _():
        greet(peer((hi + 1) % zs, lo))

    w_copies = [
        pltpu.make_async_copy(wg_ref.at[0], wg, wsem.at[0]),
        pltpu.make_async_copy(wu_ref.at[0], wu, wsem.at[1]),
        pltpu.make_async_copy(wd_ref.at[0], wd, wsem.at[2]),
    ]
    for c in w_copies:
        c.start()

    def remote(src, dst, send, recv, to):
        return pltpu.make_async_remote_copy(
            src_ref=src, dst_ref=dst, send_sem=send, recv_sem=recv,
            device_id=to, device_id_type=pl.DeviceIdType.MESH)

    def dcol(k):
        return pl.ds(pl.multiple_of(k * dcols, dcols), dcols)

    def rcol(k):
        return pl.ds(pl.multiple_of(k * rcols, rcols), rcols)

    def slot_rows(j, dl):
        return pl.ds(pl.multiple_of(j * rows + (dl // 2 + dl % 2 * 2) * cap, cap), cap)

    def side_rows(j, side):
        return pl.ds(pl.multiple_of(j * rows + side * 2 * cap, 2 * cap), 2 * cap)

    def block_rows(j):
        return pl.ds(pl.multiple_of(j * rows, rows), rows)

    def far_rows(j):
        return pl.ds(pl.multiple_of(j * rows + cap, cap), rows - cap)

    def onward(way):
        return (hi + 2 * way - 1 + zs) % zs

    def line_copy(block, k, way):
        part = lines.at[block, :, dcol(k)]
        return remote(part, part, lsend.at[way * zs + block], lrecv.at[block * KD + k],
                      peer(onward(way), lo))

    def place_copy(block, way):
        return remote(places.at[block], places.at[block], psend.at[way * zs + block],
                      precv.at[block], peer(onward(way), lo))

    def out_copy(j, dl, k):
        at = slot_rows(j, dl)
        return remote(outgoing.at[at, dcol(k)], arrived.at[at, dcol(k)],
                      dsend.at[j], drecv.at[(j * 2 + dl % 2) * KD + k], peer(hi, (lo + dl) % SUB))

    def out_arrival(j, side, k):
        at = arrived.at[side_rows(j, 1) if side else slot_rows(j, 2), dcol(k)]
        return remote(at, at, dsend.at[j], drecv.at[(j * 2 + side) * KD + k],
                      peer(hi, (lo + 1) % SUB))

    def back_copy(j, dl, k):
        at = slot_rows(j, dl)
        return remote(results.at[at, rcol(k)], returned.at[at, rcol(k)],
                      bsend.at[j], brecv.at[j * KR + k], peer(hi, (lo - dl + SUB) % SUB))

    def back_arrival(j, k):
        at = returned.at[far_rows(j), rcol(k)]
        return remote(at, at, bsend.at[j], brecv.at[j * KR + k], peer(hi, (lo + 1) % SUB))

    def chain_copy(way, j, k):
        part = chain.at[way * zs + j, :, rcol(k)]
        return remote(part, part, csend.at[way * zs + j], crecv.at[(way * zs + j) * KR + k],
                      peer(onward(way), lo))

    bits = (len(KINDS) * zs * max(KD, KR) - 1).bit_length()
    many = 30 // bits
    idle = KINDS.index("X") * zs * max(KD, KR)
    where_am_i = hi * 2 + core
    words = []
    for i in range(0, len(table[0]), many):
        packed = [sum(x << bits * r for r, x in enumerate(row[i:i + many])) for row in table]
        word = jnp.int32(packed[0])
        for at in range(1, 2 * zs):
            word = jnp.where(where_am_i == at, packed[at], word)
        words.append(word)
    words += [jnp.int32(sum(idle << bits * r for r in range(many)))] * (-len(words) % GROUP)

    step = 32

    def norm(i, carry):
        at = pl.ds(pl.multiple_of(i * step, step), step)
        v = raw[at, :].astype(jnp.float32)
        scale = lax.rsqrt(jnp.mean(v * v, -1, keepdims=True) + 1e-06)
        lines[hi, at, :] = (v * scale * gain_ref[...]).astype(jnp.bfloat16)
        return carry

    per = tok // PIECES // step
    for i, c in enumerate(t_copies):
        c.wait()
        lax.fori_loop(i * per, (i + 1) * per, norm, 0)

    ends = jnp.where(hi == 0, 1, 0) + jnp.where(hi == zs - 1, 1, 0)
    pl.semaphore_wait(barrier, SUB + 1 - ends)

    def forward(way, act):
        @pl.when(jnp.where(way == 1, zs - 1 - hi, hi) > 0)
        def _():
            act(way)

    def send_own(way, k):
        forward(way, lambda w: line_copy(hi, k, w).start())

    def send_places(way):
        forward(way, lambda w: place_copy(hi, w).start())

    @pl.when(core == 0)
    def _():
        for way in (1, 0):
            send_own(way, 0)

    expert = lax.broadcasted_iota(jnp.int32, (n, tok), 0)
    id0, id1 = ids_ref[0:1, :], ids_ref[1:2, :]
    chosen = jnp.where((id0 == expert) | (id1 == expert), 1.0, 0.0).astype(jnp.bfloat16)
    t_row = lax.broadcasted_iota(jnp.int32, (tok, tok), 0)
    t_col = lax.broadcasted_iota(jnp.int32, (tok, tok), 1)
    earlier = jnp.where(t_row < t_col, 1.0, 0.0).astype(jnp.bfloat16)
    before = jnp.dot(chosen, earlier, preferred_element_type=jnp.float32)

    def dest(ids):
        slot = jnp.sum(jnp.where(ids == expert, before, 0.0), axis=0, keepdims=True)
        return ids.astype(jnp.float32) * cap + slot

    where = lax.broadcasted_iota(jnp.int32, (8, tok), 0)
    places[hi] = jnp.where(
        where == 0, dest(id0), jnp.where(
            where == 1, dest(id1), jnp.where(where == 2, gw_ref[0:1, :], gw_ref[1:2, :])))

    @pl.when(core == 0)
    def _():
        for way in (1, 0):
            send_places(way)

    def send_line(way, k):
        @pl.when((core == 1) & (k == 0))
        def _():
            send_places(way)

        send_own(way, k)

    def row_index():
        r = lax.broadcasted_iota(jnp.int32, (rows, tok), 0)
        dl = r // cap % 2 * 2 + r // cap // 2
        return ((hi * SUB + (lo + dl) % SUB) * cap + r % cap).astype(jnp.float32)

    def choose(j, at):
        index = row_index()
        w = places[j]
        pick[at] = jnp.where((index == w[0:1, :]) | (index == w[1:2, :]), 1.0, 0.0).astype(
            jnp.bfloat16)

    def pack(j, k, at):
        got = jnp.dot(pick[at], lines[j, :, dcol(k)],
                      preferred_element_type=jnp.float32).astype(jnp.bfloat16)
        outgoing[far_rows(j), dcol(k)] = got[cap:, :]
        for dl in range(1, SUB):
            out_copy(j, dl, k).start()
        arrived[slot_rows(j, 0), dcol(k)] = got[:cap, :]

    ftile = min(ff, 256)

    def up(j, side):
        for which in (0, 1):
            @pl.when(side == which)
            def _():
                def landed(k, carry):
                    out_arrival(j, which, k).wait_recv()
                    return carry

                lax.fori_loop(0, KD, landed, 0)

        def tile(f, carry):
            cols = pl.ds(pl.multiple_of(f * ftile, ftile), ftile)
            x = arrived[side_rows(j, side), :]
            g = jnp.dot(x, wg[:, cols], preferred_element_type=jnp.float32)
            u = jnp.dot(x, wu[:, cols], preferred_element_type=jnp.float32)
            hidden[j * 2 + side, :, cols] = (g / (1.0 + jnp.exp(-g)) * u).astype(jnp.bfloat16)
            return carry

        lax.fori_loop(0, ff // ftile, tile, 0)

    def down(j, side, k):
        got = jnp.dot(hidden[j * 2 + side], wd[:, rcol(k)],
                      preferred_element_type=jnp.float32).astype(jnp.bfloat16)

        @pl.when(side == 0)
        def _():
            results[slot_rows(j, 2), rcol(k)] = got[cap:, :]
            back_copy(j, 2, k).start()
            returned[slot_rows(j, 0), rcol(k)] = got[:cap, :]

        @pl.when(side == 1)
        def _():
            results[side_rows(j, 1), rcol(k)] = got
            for dl in (1, 3):
                back_copy(j, dl, k).start()

    def weigh(j, at):
        index = row_index()
        w = places[j]
        weight = jnp.transpose(jnp.where(index == w[0:1, :], w[2:3, :], 0.0)
                               + jnp.where(index == w[1:2, :], w[3:4, :], 0.0))
        top = weight.astype(jnp.bfloat16)
        high[at] = top
        low[at] = (weight - top.astype(jnp.float32)).astype(jnp.bfloat16)

    def mix(j, k, at):
        block = returned[block_rows(j), rcol(k)]
        return (jnp.dot(high[at], block, preferred_element_type=jnp.float32)
                + jnp.dot(low[at], block, preferred_element_type=jnp.float32))

    def take(j, k):
        way = jnp.where(j < hi, 1, 0)

        @pl.when((k == 0) & (j != hi))
        def _():
            place_copy(j, way).wait_recv()

        @pl.when(k == 0)
        def _():
            choose(j, j)

        @pl.when(j != hi)
        def _():
            line_copy(j, k, way).wait_recv()

        pack(j, k, j)

    def pass_on(j, k):
        way = jnp.where(j < hi, 1, 0)

        @pl.when(k == 0)
        def _():
            place_copy(j, way).start()

        line_copy(j, k, way).start()

    def add(j, k):
        way = jnp.where(j > hi, 1, 0)

        @pl.when(k == 0)
        def _():
            weigh(j, j)

        back_arrival(j, k).wait_recv()
        value = mix(j, k, j)
        at = way * zs + j
        beyond = way * hi + (1 - way) * (zs - 1 - hi)

        @pl.when(beyond > 0)
        def _():
            chain_copy(way, j, k).wait_recv()
            chain[at, :, rcol(k)] = (
                value + chain[at, :, rcol(k)].astype(jnp.float32)).astype(jnp.bfloat16)

        @pl.when(beyond == 0)
        def _():
            chain[at, :, rcol(k)] = value.astype(jnp.bfloat16)

        chain_copy(way, j, k).start()

    def final(k):
        @pl.when(k == 0)
        def _():
            weigh(hi, hi)

        back_arrival(hi, k).wait_recv()
        value = mix(hi, k, hi)

        def arrived_from(way):
            chain_copy(way, hi, k).wait_recv()
            return chain[way * zs + hi, :, rcol(k)].astype(jnp.float32)

        def put(total):
            out_ref[:, rcol(k)] = total.astype(out_ref.dtype)

        @pl.when(hi == 0)
        def _():
            put(value + arrived_from(0))

        @pl.when(hi == zs - 1)
        def _():
            put(value + arrived_from(1))

        @pl.when((hi > 0) & (hi < zs - 1))
        def _():
            put(value + arrived_from(0) + arrived_from(1))

    def run(near, i, carry):
        spot, digit = lax.div(i, many), lax.rem(i, many)
        word = near[0]
        for at in range(1, len(near)):
            word = jnp.where(spot == at, near[at], word)
        for r in range(1, many):
            word = jnp.where(digit >= r, lax.div(word, 1 << bits), word)
        code = lax.rem(word, 1 << bits)
        kind = lax.div(code, zs * max(KD, KR))
        j = lax.rem(lax.div(code, max(KD, KR)), zs)
        k = lax.rem(code, max(KD, KR))

        acts = {
            "S": lambda: send_line(1, k),
            "Z": lambda: send_line(0, k),
            "G": lambda: pass_on(j, k),
            "T": lambda: take(j, k),
            "U": lambda: up(j, kind - KINDS.index("U")),
            "D": lambda: down(j, kind - KINDS.index("D"), k),
            "M": lambda: add(j, k),
            "F": lambda: final(k),
            "W": lambda: [c.wait() for c in w_copies],
            "N": lambda: pl.semaphore_signal(
                turn, inc=1, device_id=peer(hi, lo + 1), device_id_type=pl.DeviceIdType.MESH),
            "Q": lambda: pl.semaphore_wait(turn, 1),
        }

        def among(names):
            if len(names) == 1:
                acts[names[0]]()
                return
            cut = len(names) // 2
            low = kind < KINDS.index(names[cut])
            pl.when(low)(lambda: among(names[:cut]))
            pl.when(jnp.logical_not(low))(lambda: among(names[cut:]))

        pl.when(kind < KINDS.index("X"))(lambda: among(list(acts)))
        return carry

    def turns(a, carry):
        near = []
        for r in range(GROUP):
            word = words[r]
            for at in range(1, len(words) // GROUP):
                word = jnp.where(a == at, words[at * GROUP + r], word)
            near.append(word)
        return lax.fori_loop(0, GROUP * many, functools.partial(run, near), carry)

    lax.fori_loop(0, len(words) // GROUP, turns, 0)

    def finish(j, carry):
        at = far_rows(j)
        remote(outgoing.at[at, :], outgoing.at[at, :], dsend.at[j], drecv.at[0],
               peer(hi, (lo + 1) % SUB)).wait_send()
        remote(results.at[at, :], results.at[at, :], bsend.at[j], brecv.at[0],
               peer(hi, (lo + 1) % SUB)).wait_send()
        for way in (0, 1):
            to = peer(onward(way), lo)

            @pl.when((hi < zs - 1) & (j <= hi) if way else (hi > 0) & (j >= hi))
            def _():
                place_copy(j, way).wait_send()
                remote(lines.at[j], lines.at[j], lsend.at[way * zs + j], lrecv.at[0],
                       to).wait_send()

            @pl.when(j > hi if way else j < hi)
            def _():
                at = way * zs + j
                remote(chain.at[at], chain.at[at], csend.at[at], crecv.at[0], to).wait_send()

        return carry

    lax.fori_loop(0, zs, finish, 0)


def per_device(tokens, norm_gain, expert_ids, gate_weights, w_gate, w_up, w_down):
    n = lax.axis_size("ep")
    tok, width = tokens.shape
    top = expert_ids.shape[1]
    ff = w_gate.shape[2]
    cap = 2 * tok * top // n
    total = n * cap
    zs = n // SUB
    rows = SUB * cap
    table = tables(zs)
    bf16 = jnp.bfloat16
    dma = pltpu.SemaphoreType.DMA
    vmem = pl.BlockSpec(memory_space=pltpu.VMEM)
    hbm = pl.BlockSpec(memory_space=pl.ANY)
    return pl.pallas_call(
        functools.partial(kernel, n, cap, table),
        out_shape=pltpu.VMEM((tok, width), bf16),
        in_specs=[hbm] + [vmem] * 3 + [hbm] * 3,
        out_specs=vmem,
        scratch_shapes=[
            pltpu.VMEM((width, ff), bf16),
            pltpu.VMEM((width, ff), bf16),
            pltpu.VMEM((ff, width), bf16),
            pltpu.VMEM((zs, tok, width), bf16),
            pltpu.VMEM((zs, 8, tok), jnp.float32),
            pltpu.VMEM((total, width), bf16),
            pltpu.VMEM((total, width), bf16),
            pltpu.VMEM((total, width), bf16),
            pltpu.VMEM((total, width), bf16),
            pltpu.VMEM((2 * zs, rows // 2, ff), bf16),
            pltpu.VMEM((2 * zs, tok, width), bf16),
            pltpu.VMEM((zs, rows, tok), bf16),
            pltpu.VMEM((zs, tok, rows), bf16),
            pltpu.VMEM((zs, tok, rows), bf16),
            pltpu.VMEM((tok, width), bf16),
            dma((PIECES,)),
            dma((3,)),
            dma((2 * zs,)),
            dma((zs * KD,)),
            dma((2 * zs,)),
            dma((zs,)),
            dma((zs,)),
            dma((2 * zs * KD,)),
            dma((zs,)),
            dma((zs * KR,)),
            dma((2 * zs,)),
            dma((2 * zs * KR,)),
            pltpu.SemaphoreType.REGULAR,
        ],
        compiler_params=pltpu.CompilerParams(
            collective_id=0, has_side_effects=True, vmem_limit_bytes=58 * 1024 * 1024),
    )(tokens, norm_gain.reshape(1, width), expert_ids.T, gate_weights.T, w_gate, w_up, w_down)


def solution(mesh):
    return jax.shard_map(
        per_device,
        mesh=mesh,
        in_specs=(
            P(("grp", "ep"), None),
            P(),
            P(("grp", "ep"), None),
            P(("grp", "ep"), None),
            P("ep", None, None),
            P("ep", None, None),
            P("ep", None, None),
        ),
        out_specs=P(("grp", "ep"), None),
        check_vma=False,
    )
```

```python
import bisect
import functools
import heapq
import jax
import jax.numpy as jnp
from jax import lax
from jax.experimental import pallas as pl
from jax.experimental.pallas import tpu as pltpu
from jax.sharding import PartitionSpec as P

SUB = 4
KD = 8
KR = 8
PIECES = 4
GROUP = 8
KINDS = "SZGTUVDEMFWNQX"
COST = {"T": 1.6, "U": 2.05, "V": 2.05, "D": 1.96, "E": 1.96, "M": 1.84, "F": 1.7, "G": 0.15, "S": 0.1, "Z": 0.1}
RANK = {"S": 0, "Z": 0, "G": 0.5, "T": 1, "N": -1, "M": 2, "F": 3, "D": 4, "E": 4, "U": 5, "V": 5}
Z_BLOCK, Y_BLOCK, LAG, START, PACK, STEP, BACKLOG = 11.3, 5.6, 2.2, 2.9, 3.8, 0.09, 3.0
HANDOVER = 1
PRIO = {(0, 0, 'T', 2): 2.3,
 (0, 1, 'D', 0): 4.5,
 (0, 1, 'M', 2): 1.0,
 (0, 1, 'T', 2): 4.9,
 (1, 0, 'D', 0): 1.8,
 (1, 0, 'E', 1): 1.8,
 (1, 0, 'E', 2): 6.0,
 (1, 0, 'T', 2): 6.0,
 (1, 0, 'Z', 2): 2.6,
 (1, 1, 'D', 1): 3.4,
 (1, 1, 'D', 2): 4.7,
 (1, 1, 'D', 3): 3.5,
 (1, 1, 'E', 3): 0.2,
 (1, 1, 'S', 0): 2.3,
 (1, 1, 'S', 1): 2.0,
 (1, 1, 'S', 3): 4.5,
 (1, 1, 'T', 0): 3.6,
 (1, 1, 'V', 0): 2.0,
 (1, 1, 'V', 1): 2.2,
 (1, 1, 'V', 3): 1.8,
 (1, 1, 'Z', 0): 3.7,
 (1, 1, 'Z', 1): 4.0}
HOLD = {(0, 0, 'U', 0): 86,
 (0, 1, 'E', 0): 86,
 (0, 1, 'U', 0): 85,
 (1, 0, 'D', 1): 82,
 (1, 0, 'E', 0): 70,
 (1, 0, 'G', 2): 30,
 (1, 0, 'S', 0): 26,
 (1, 0, 'U', 0): 64,
 (1, 0, 'U', 3): 34,
 (1, 0, 'V', 1): 66,
 (1, 1, 'E', 0): 65,
 (1, 1, 'T', 1): 32,
 (1, 1, 'V', 1): 82,
 (1, 1, 'Z', 0): 56}


def plan(zs):
    half = zs // 2
    cores = [(h, c) for h in range(half) for c in (0, 1)]
    need, when, ready = {}, {}, {d: [] for d in cores}
    order = {d: [] for d in cores}
    pieces = {"T": KD, "D": KR, "E": KR, "M": KR, "F": KR}
    events, busy, links, turn = [], dict.fromkeys(cores, 0.0), {}, [0]

    def post(at, what, key):
        turn[0] += 1
        heapq.heappush(events, (at, turn[0], what, key))

    def way_of(h, name, b):
        if name == "S" or (name == "G" and b < h) or (name == "M" and b > h):
            return h, 1
        if name in "ZGM":
            return h, 0
        return (h, 2) if name in "DE" else None

    def release(d, name, b, k):
        key = d + ((name, k * 4 // KD) if name in "SZ" else (name, b))
        at = max(when[d, name, b, k], HOLD.get(key, 0.0))
        if name in "SZ" and k + d[1] == 0:
            key, at = (), START
        bisect.insort(ready[d], (PRIO.get(key, RANK[name]) + 0.01 * k, abs(b - d[0]), name, b, k,
                                 at, way_of(d[0], name, b)))

    def task(d, name, b, k, deps, at=0.0):
        need[d, name, b, k], when[d, name, b, k] = deps, at
        if deps == 0:
            release(d, name, b, k)

    for d in cores:
        h, c = d
        for b in range(zs):
            for k in range(KD):
                task(d, "T", b, k, int(b != h), PACK if b == h else 0.0)
                if b != h and (h < zs - 1 if b < h else h > 0):
                    task(d, "G", b, k, 1)
            for name, other in (("U", "D"), ("V", "E")):
                task(d, name, b, 0, KD)
                for k in range(KR):
                    task(d, other, b, k, 1)
            for k in range(KR):
                if b == h:
                    task(d, "F", b, k, 2 + (h > 0) + (h < zs - 1))
                else:
                    task(d, "M", b, k, 2 + (h > 0 if b > h else h < zs - 1))
        if c == 0:
            task(d, "N", h + 1, 0, 1)
        for k in range(KD):
            for name in "SZ" if h > 0 else "S":
                task(d, name, h, k, c + (k > 0), START)
        post(START, "core", d)
        post(PACK, "core", d)

    def supply(d, name, b, k, at):
        if d[0] >= half:
            d, b = (zs - 1 - d[0], d[1]), zs - 1 - b
        key = (d, name, b, k)
        need[key] -= 1
        when[key] = max(when[key], at)
        if need[key] == 0:
            release(*key)
        post(at, "core", d)

    def settle(key, t):
        lk = links[key]
        live = [q for q in lk["queues"] if q]
        for q in live:
            q[0][0] -= (t - lk["at"]) / len(live)
        lk["at"] = t
        for q in live:
            while q and q[0][0] <= 1e-6:
                for e in q.pop(0)[1]:
                    supply(*e, t + LAG)
        lk["stamp"] += 1
        live = [q for q in lk["queues"] if q]
        if live:
            post(t + min(q[0][0] for q in live) * len(live), "link", (key, lk["stamp"]))

    def wire(key, c, time, t, targets):
        lk = links.setdefault(key, {"at": 0.0, "queues": ([], []), "stamp": 0})
        if any(lk["queues"]):
            settle(key, t)
        lk["at"] = t
        lk["queues"][c].append([time, targets])
        settle(key, t)

    def backlog(key, c, t):
        lk = links.get(key)
        if lk is None:
            return 0.0
        return sum(x[0] for x in lk["queues"][c]) * sum(map(bool, lk["queues"]))

    def onward(h, c, way, b, k, name, time, t):
        g = h + 2 * way - 1
        wire((h, way), c, time, t, [((g, c), "F" if name == "M" and g == b else name, b, k)])

    def pick(d, t):
        later, full = None, {}
        for i, x in enumerate(ready[d]):
            at, gate = x[5:]
            if at <= t + 1e-9 and gate is not None:
                if gate not in full:
                    full[gate] = backlog(gate, d[1], t) - BACKLOG
                at = t + full[gate] if full[gate] > 1e-6 else at
            if at <= t + 1e-9:
                return ready[d].pop(i)[2:5]
            later = at if later is None else min(later, at)
        if later is not None:
            post(max(later, t + 0.1), "core", d)
        return None

    while events:
        t, _, what, key = heapq.heappop(events)
        if what == "link":
            if links[key[0]]["stamp"] == key[1]:
                settle(key[0], t)
            continue
        d = key
        if busy[d] > t + 1e-9:
            continue
        choice = pick(d, t)
        if choice is None:
            continue
        h, c = d
        name, b, k = choice
        order[d].append(choice)
        done = t + STEP + COST.get(name, 0.0) / pieces.get(name, 1)
        done += 0.3 if k == 0 and name in "TM" else 0.0
        if name in "SZ":
            onward(h, c, int(name == "S"), b, k, "T", Z_BLOCK / KD, t)
            if k + 1 < KD:
                supply(d, name, b, k + 1, done)
        elif name == "G":
            onward(h, c, int(b < h), b, k, "T", Z_BLOCK / KD, t)
        elif name == "T":
            if (d, "G", b, k) in need:
                supply(d, "G", b, k, done)
            if c == 0 and b == h + 1 and k == KD * HANDOVER // 8:
                supply(d, "N", b, 0, done)
            wire((h, 2), c, Y_BLOCK / KD, t, [(d, "U", b, 0), ((h, 1 - c), "V", b, 0)])
        elif name == "N":
            for r in range(KD):
                for s in "SZ" if h > 0 else "S":
                    supply((h, 1), s, h, r, done + 0.3)
        elif name in "UV":
            for r in range(KR):
                supply(d, "D" if name == "U" else "E", b, r, done)
        elif name in "DE":
            wire((h, 2), c, Y_BLOCK / KR / 2, t + STEP,
                 [((h, c if name == "D" else 1 - c), "F" if b == h else "M", b, k)])
        elif name == "M":
            onward(h, c, int(b > h), b, k, "M", Z_BLOCK / KR, t + STEP)
        busy[d] = done
        post(done, "core", d)
    assert sum(map(len, order.values())) == len(need)
    return order


def tables(zs):
    order = plan(zs)

    def code(name, b, k):
        return (KINDS.index(name) * zs + b) * max(KD, KR) + k

    def listed(h, c):
        todo = list(order[min(h, zs - 1 - h), c])
        if h >= zs // 2:
            todo = [({"S": "Z", "Z": "S"}.get(name, name), zs - 1 - b, k) for name, b, k in todo]
        if c == 0:
            todo = [x for x in todo if x[0] not in "SZ" or x[2] > 0]
        names = [x[0] for x in todo]
        first = min(names.index("U"), names.index("V"))
        todo.insert(first, ("W", 0, 0))
        if c == 1:
            turn = min(i for i, x in enumerate(todo) if x[0] in "SZ")
            todo.insert(turn, ("Q", 0, 0))
        return todo

    lists = [listed(h, c) for h in range(zs) for c in (0, 1)]
    size = max(map(len, lists))
    size += -size % 3
    return [[code(*x) for x in o] + [code("X", 0, 0)] * (size - len(o)) for o in lists]


def kernel(n, cap, table, tok_ref, gain_ref, ids_ref, gw_ref, wg_ref, wu_ref, wd_ref, out_ref,
           wg, wu, wd, lines, places, outgoing, arrived, results, returned, hidden, chain,
           pick, high, low, raw,
           tsem, wsem, lsend, lrecv, psend, precv, dsend, drecv, bsend, brecv, csend, crecv, turn):
    zs = n // SUB
    me = lax.axis_index("ep")
    hi, lo = me // SUB, me % SUB
    core = lo % 2
    tok, width = tok_ref.shape
    ff = wg.shape[1]
    rows = SUB * cap
    dcols, rcols = width // KD, width // KR

    def peer(plane, part):
        return {"ep": plane * SUB + part}

    pieces = [pl.ds(i * (tok // PIECES), tok // PIECES) for i in range(PIECES)]
    t_copies = [pltpu.make_async_copy(tok_ref.at[at, :], raw.at[at, :], tsem.at[i])
                for i, at in enumerate(pieces)]
    for c in t_copies:
        c.start()

    barrier = pltpu.get_barrier_semaphore()

    def greet(to):
        pl.semaphore_signal(barrier, inc=1, device_id=to, device_id_type=pl.DeviceIdType.MESH)

    for dl in range(1, SUB):
        greet(peer(hi, (lo + dl) % SUB))

    @pl.when(hi > 0)
    def _():
        greet(peer((hi + zs - 1) % zs, lo))

    @pl.when(hi < zs - 1)
    def _():
        greet(peer((hi + 1) % zs, lo))

    w_copies = [
        pltpu.make_async_copy(wg_ref.at[0], wg, wsem.at[0]),
        pltpu.make_async_copy(wu_ref.at[0], wu, wsem.at[1]),
        pltpu.make_async_copy(wd_ref.at[0], wd, wsem.at[2]),
    ]
    for c in w_copies:
        c.start()

    def remote(src, dst, send, recv, to):
        return pltpu.make_async_remote_copy(
            src_ref=src, dst_ref=dst, send_sem=send, recv_sem=recv,
            device_id=to, device_id_type=pl.DeviceIdType.MESH)

    def dcol(k):
        return pl.ds(pl.multiple_of(k * dcols, dcols), dcols)

    def rcol(k):
        return pl.ds(pl.multiple_of(k * rcols, rcols), rcols)

    def slot_rows(j, dl):
        return pl.ds(pl.multiple_of(j * rows + (dl // 2 + dl % 2 * 2) * cap, cap), cap)

    def side_rows(j, side):
        return pl.ds(pl.multiple_of(j * rows + side * 2 * cap, 2 * cap), 2 * cap)

    def block_rows(j):
        return pl.ds(pl.multiple_of(j * rows, rows), rows)

    def far_rows(j):
        return pl.ds(pl.multiple_of(j * rows + cap, cap), rows - cap)

    def onward(way):
        return (hi + 2 * way - 1 + zs) % zs

    def line_copy(block, k, way):
        part = lines.at[block, :, dcol(k)]
        return remote(part, part, lsend.at[way * zs + block], lrecv.at[block * KD + k],
                      peer(onward(way), lo))

    def place_copy(block, way):
        return remote(places.at[block], places.at[block], psend.at[way * zs + block],
                      precv.at[block], peer(onward(way), lo))

    def out_copy(j, dl, k):
        at = slot_rows(j, dl)
        return remote(outgoing.at[at, dcol(k)], arrived.at[at, dcol(k)],
                      dsend.at[j], drecv.at[(j * 2 + dl % 2) * KD + k], peer(hi, (lo + dl) % SUB))

    def out_arrival(j, side, k):
        at = arrived.at[side_rows(j, 1) if side else slot_rows(j, 2), dcol(k)]
        return remote(at, at, dsend.at[j], drecv.at[(j * 2 + side) * KD + k],
                      peer(hi, (lo + 1) % SUB))

    def back_copy(j, dl, k):
        at = slot_rows(j, dl)
        return remote(results.at[at, rcol(k)], returned.at[at, rcol(k)],
                      bsend.at[j], brecv.at[j * KR + k], peer(hi, (lo - dl + SUB) % SUB))

    def back_arrival(j, k):
        at = returned.at[far_rows(j), rcol(k)]
        return remote(at, at, bsend.at[j], brecv.at[j * KR + k], peer(hi, (lo + 1) % SUB))

    def chain_copy(way, j, k):
        part = chain.at[way * zs + j, :, rcol(k)]
        return remote(part, part, csend.at[way * zs + j], crecv.at[(way * zs + j) * KR + k],
                      peer(onward(way), lo))

    bits = (len(KINDS) * zs * max(KD, KR) - 1).bit_length()
    many = 30 // bits
    idle = KINDS.index("X") * zs * max(KD, KR)
    where_am_i = hi * 2 + core
    words = []
    for i in range(0, len(table[0]), many):
        packed = [sum(x << bits * r for r, x in enumerate(row[i:i + many])) for row in table]
        word = jnp.int32(packed[0])
        for at in range(1, 2 * zs):
            word = jnp.where(where_am_i == at, packed[at], word)
        words.append(word)
    words += [jnp.int32(sum(idle << bits * r for r in range(many)))] * (-len(words) % GROUP)

    step = 32

    def norm(i, carry):
        at = pl.ds(pl.multiple_of(i * step, step), step)
        v = raw[at, :].astype(jnp.float32)
        scale = lax.rsqrt(jnp.mean(v * v, -1, keepdims=True) + 1e-06)
        lines[hi, at, :] = (v * scale * gain_ref[...]).astype(jnp.bfloat16)
        return carry

    per = tok // PIECES // step
    for i, c in enumerate(t_copies):
        c.wait()
        lax.fori_loop(i * per, (i + 1) * per, norm, 0)

    ends = jnp.where(hi == 0, 1, 0) + jnp.where(hi == zs - 1, 1, 0)
    pl.semaphore_wait(barrier, SUB + 1 - ends)

    def forward(way, act):
        @pl.when(jnp.where(way == 1, zs - 1 - hi, hi) > 0)
        def _():
            act(way)

    def send_own(way, k):
        forward(way, lambda w: line_copy(hi, k, w).start())

    def send_places(way):
        forward(way, lambda w: place_copy(hi, w).start())

    @pl.when(core == 0)
    def _():
        for way in (1, 0):
            send_own(way, 0)

    expert = lax.broadcasted_iota(jnp.int32, (n, tok), 0)
    id0, id1 = ids_ref[0:1, :], ids_ref[1:2, :]
    chosen = jnp.where((id0 == expert) | (id1 == expert), 1.0, 0.0).astype(jnp.bfloat16)
    t_row = lax.broadcasted_iota(jnp.int32, (tok, tok), 0)
    t_col = lax.broadcasted_iota(jnp.int32, (tok, tok), 1)
    earlier = jnp.where(t_row < t_col, 1.0, 0.0).astype(jnp.bfloat16)
    before = jnp.dot(chosen, earlier, preferred_element_type=jnp.float32)

    def dest(ids):
        slot = jnp.sum(jnp.where(ids == expert, before, 0.0), axis=0, keepdims=True)
        return ids.astype(jnp.float32) * cap + slot

    where = lax.broadcasted_iota(jnp.int32, (8, tok), 0)
    places[hi] = jnp.where(
        where == 0, dest(id0), jnp.where(
            where == 1, dest(id1), jnp.where(where == 2, gw_ref[0:1, :], gw_ref[1:2, :])))

    @pl.when(core == 0)
    def _():
        for way in (1, 0):
            send_places(way)

    def send_line(way, k):
        @pl.when((core == 1) & (k == 0))
        def _():
            send_places(way)

        send_own(way, k)

    def row_index():
        r = lax.broadcasted_iota(jnp.int32, (rows, tok), 0)
        dl = r // cap % 2 * 2 + r // cap // 2
        return ((hi * SUB + (lo + dl) % SUB) * cap + r % cap).astype(jnp.float32)

    def choose(j, at):
        index = row_index()
        w = places[j]
        pick[at] = jnp.where((index == w[0:1, :]) | (index == w[1:2, :]), 1.0, 0.0).astype(
            jnp.bfloat16)

    def pack(j, k, at):
        got = jnp.dot(pick[at], lines[j, :, dcol(k)],
                      preferred_element_type=jnp.float32).astype(jnp.bfloat16)
        outgoing[far_rows(j), dcol(k)] = got[cap:, :]
        for dl in range(1, SUB):
            out_copy(j, dl, k).start()
        arrived[slot_rows(j, 0), dcol(k)] = got[:cap, :]

    ftile = min(ff, 256)

    def up(j, side):
        for which in (0, 1):
            @pl.when(side == which)
            def _():
                def landed(k, carry):
                    out_arrival(j, which, k).wait_recv()
                    return carry

                lax.fori_loop(0, KD, landed, 0)

        def tile(f, carry):
            cols = pl.ds(pl.multiple_of(f * ftile, ftile), ftile)
            x = arrived[side_rows(j, side), :]
            g = jnp.dot(x, wg[:, cols], preferred_element_type=jnp.float32)
            u = jnp.dot(x, wu[:, cols], preferred_element_type=jnp.float32)
            hidden[j * 2 + side, :, cols] = (g / (1.0 + jnp.exp(-g)) * u).astype(jnp.bfloat16)
            return carry

        lax.fori_loop(0, ff // ftile, tile, 0)

    def down(j, side, k):
        got = jnp.dot(hidden[j * 2 + side], wd[:, rcol(k)],
                      preferred_element_type=jnp.float32).astype(jnp.bfloat16)

        @pl.when(side == 0)
        def _():
            results[slot_rows(j, 2), rcol(k)] = got[cap:, :]
            back_copy(j, 2, k).start()
            returned[slot_rows(j, 0), rcol(k)] = got[:cap, :]

        @pl.when(side == 1)
        def _():
            results[side_rows(j, 1), rcol(k)] = got
            for dl in (1, 3):
                back_copy(j, dl, k).start()

    def weigh(j, at):
        index = row_index()
        w = places[j]
        weight = jnp.transpose(jnp.where(index == w[0:1, :], w[2:3, :], 0.0)
                               + jnp.where(index == w[1:2, :], w[3:4, :], 0.0))
        top = weight.astype(jnp.bfloat16)
        high[at] = top
        low[at] = (weight - top.astype(jnp.float32)).astype(jnp.bfloat16)

    def mix(j, k, at):
        block = returned[block_rows(j), rcol(k)]
        return (jnp.dot(high[at], block, preferred_element_type=jnp.float32)
                + jnp.dot(low[at], block, preferred_element_type=jnp.float32))

    def take(j, k):
        way = jnp.where(j < hi, 1, 0)

        @pl.when((k == 0) & (j != hi))
        def _():
            place_copy(j, way).wait_recv()

        @pl.when(k == 0)
        def _():
            choose(j, j)

        @pl.when(j != hi)
        def _():
            line_copy(j, k, way).wait_recv()

        pack(j, k, j)

    def pass_on(j, k):
        way = jnp.where(j < hi, 1, 0)

        @pl.when(k == 0)
        def _():
            place_copy(j, way).start()

        line_copy(j, k, way).start()

    def add(j, k):
        way = jnp.where(j > hi, 1, 0)

        @pl.when(k == 0)
        def _():
            weigh(j, j)

        back_arrival(j, k).wait_recv()
        value = mix(j, k, j)
        at = way * zs + j
        beyond = way * hi + (1 - way) * (zs - 1 - hi)

        @pl.when(beyond > 0)
        def _():
            chain_copy(way, j, k).wait_recv()
            chain[at, :, rcol(k)] = (
                value + chain[at, :, rcol(k)].astype(jnp.float32)).astype(jnp.bfloat16)

        @pl.when(beyond == 0)
        def _():
            chain[at, :, rcol(k)] = value.astype(jnp.bfloat16)

        chain_copy(way, j, k).start()

    def final(k):
        @pl.when(k == 0)
        def _():
            weigh(hi, hi)

        back_arrival(hi, k).wait_recv()
        value = mix(hi, k, hi)

        def arrived_from(way):
            chain_copy(way, hi, k).wait_recv()
            return chain[way * zs + hi, :, rcol(k)].astype(jnp.float32)

        def put(total):
            out_ref[:, rcol(k)] = total.astype(out_ref.dtype)

        @pl.when(hi == 0)
        def _():
            put(value + arrived_from(0))

        @pl.when(hi == zs - 1)
        def _():
            put(value + arrived_from(1))

        @pl.when((hi > 0) & (hi < zs - 1))
        def _():
            put(value + arrived_from(0) + arrived_from(1))

    def run(near, i, carry):
        spot, digit = lax.div(i, many), lax.rem(i, many)
        word = near[0]
        for at in range(1, len(near)):
            word = jnp.where(spot == at, near[at], word)
        for r in range(1, many):
            word = jnp.where(digit >= r, lax.div(word, 1 << bits), word)
        code = lax.rem(word, 1 << bits)
        kind = lax.div(code, zs * max(KD, KR))
        j = lax.rem(lax.div(code, max(KD, KR)), zs)
        k = lax.rem(code, max(KD, KR))

        acts = {
            "S": lambda: send_line(1, k),
            "Z": lambda: send_line(0, k),
            "G": lambda: pass_on(j, k),
            "T": lambda: take(j, k),
            "U": lambda: up(j, kind - KINDS.index("U")),
            "D": lambda: down(j, kind - KINDS.index("D"), k),
            "M": lambda: add(j, k),
            "F": lambda: final(k),
            "W": lambda: [c.wait() for c in w_copies],
            "N": lambda: pl.semaphore_signal(
                turn, inc=1, device_id=peer(hi, lo + 1), device_id_type=pl.DeviceIdType.MESH),
            "Q": lambda: pl.semaphore_wait(turn, 1),
        }

        def among(names):
            if len(names) == 1:
                acts[names[0]]()
                return
            cut = len(names) // 2
            low = kind < KINDS.index(names[cut])
            pl.when(low)(lambda: among(names[:cut]))
            pl.when(jnp.logical_not(low))(lambda: among(names[cut:]))

        pl.when(kind < KINDS.index("X"))(lambda: among(list(acts)))
        return carry

    def turns(a, carry):
        near = []
        for r in range(GROUP):
            word = words[r]
            for at in range(1, len(words) // GROUP):
                word = jnp.where(a == at, words[at * GROUP + r], word)
            near.append(word)
        return lax.fori_loop(0, GROUP * many, functools.partial(run, near), carry)

    lax.fori_loop(0, len(words) // GROUP, turns, 0)

    def finish(j, carry):
        at = far_rows(j)
        remote(outgoing.at[at, :], outgoing.at[at, :], dsend.at[j], drecv.at[0],
               peer(hi, (lo + 1) % SUB)).wait_send()
        remote(results.at[at, :], results.at[at, :], bsend.at[j], brecv.at[0],
               peer(hi, (lo + 1) % SUB)).wait_send()
        for way in (0, 1):
            to = peer(onward(way), lo)

            @pl.when((hi < zs - 1) & (j <= hi) if way else (hi > 0) & (j >= hi))
            def _():
                place_copy(j, way).wait_send()
                remote(lines.at[j], lines.at[j], lsend.at[way * zs + j], lrecv.at[0],
                       to).wait_send()

            @pl.when(j > hi if way else j < hi)
            def _():
                at = way * zs + j
                remote(chain.at[at], chain.at[at], csend.at[at], crecv.at[0], to).wait_send()

        return carry

    lax.fori_loop(0, zs, finish, 0)


def per_device(tokens, norm_gain, expert_ids, gate_weights, w_gate, w_up, w_down):
    n = lax.axis_size("ep")
    tok, width = tokens.shape
    top = expert_ids.shape[1]
    ff = w_gate.shape[2]
    cap = 2 * tok * top // n
    total = n * cap
    zs = n // SUB
    rows = SUB * cap
    table = tables(zs)
    bf16 = jnp.bfloat16
    dma = pltpu.SemaphoreType.DMA
    vmem = pl.BlockSpec(memory_space=pltpu.VMEM)
    hbm = pl.BlockSpec(memory_space=pl.ANY)
    return pl.pallas_call(
        functools.partial(kernel, n, cap, table),
        out_shape=pltpu.VMEM((tok, width), bf16),
        in_specs=[hbm] + [vmem] * 3 + [hbm] * 3,
        out_specs=vmem,
        scratch_shapes=[
            pltpu.VMEM((width, ff), bf16),
            pltpu.VMEM((width, ff), bf16),
            pltpu.VMEM((ff, width), bf16),
            pltpu.VMEM((zs, tok, width), bf16),
            pltpu.VMEM((zs, 8, tok), jnp.float32),
            pltpu.VMEM((total, width), bf16),
            pltpu.VMEM((total, width), bf16),
            pltpu.VMEM((total, width), bf16),
            pltpu.VMEM((total, width), bf16),
            pltpu.VMEM((2 * zs, rows // 2, ff), bf16),
            pltpu.VMEM((2 * zs, tok, width), bf16),
            pltpu.VMEM((zs, rows, tok), bf16),
            pltpu.VMEM((zs, tok, rows), bf16),
            pltpu.VMEM((zs, tok, rows), bf16),
            pltpu.VMEM((tok, width), bf16),
            dma((PIECES,)),
            dma((3,)),
            dma((2 * zs,)),
            dma((zs * KD,)),
            dma((2 * zs,)),
            dma((zs,)),
            dma((zs,)),
            dma((2 * zs * KD,)),
            dma((zs,)),
            dma((zs * KR,)),
            dma((2 * zs,)),
            dma((2 * zs * KR,)),
            pltpu.SemaphoreType.REGULAR,
        ],
        compiler_params=pltpu.CompilerParams(
            collective_id=0, has_side_effects=True, vmem_limit_bytes=58 * 1024 * 1024),
    )(tokens, norm_gain.reshape(1, width), expert_ids.T, gate_weights.T, w_gate, w_up, w_down)


def solution(mesh):
    return jax.shard_map(
        per_device,
        mesh=mesh,
        in_specs=(
            P(("grp", "ep"), None),
            P(),
            P(("grp", "ep"), None),
            P(("grp", "ep"), None),
            P("ep", None, None),
            P("ep", None, None),
            P("ep", None, None),
        ),
        out_specs=P(("grp", "ep"), None),
        check_vma=False,
    )
```

```python
import bisect
import functools
import heapq
import jax
import jax.numpy as jnp
from jax import lax
from jax.experimental import pallas as pl
from jax.experimental.pallas import tpu as pltpu
from jax.sharding import PartitionSpec as P

SUB = 4
KD = 8
KR = 8
PIECES = 4
GROUP = 8
KINDS = "SZGTUVDEMFWNQ"
COST = {"T": 1.6, "U": 2.05, "V": 2.05, "D": 1.96, "E": 1.96, "M": 1.84, "F": 1.7, "G": 0.15, "S": 0.1, "Z": 0.1}
RANK = {"S": 0, "Z": 0, "G": 0.5, "T": 1, "N": -1, "M": 2, "F": 3, "D": 4, "E": 4, "U": 5, "V": 5}
Z_BLOCK, Y_BLOCK, START, PACK, STEP, BACKLOG = 11.3, 5.6, 2.9, 3.8, 0.09, 3.0
LAG = (2.2, 2.2, 2.2)
HANDOVER = 4
PRIO = {(0, 0, 'E', 0): 0.8,
 (0, 0, 'M', 1): 5.6,
 (0, 1, 'D', 0): 4.8,
 (0, 1, 'T', 1): 5.1,
 (0, 1, 'T', 2): 4.6,
 (0, 1, 'V', 0): 0.3,
 (0, 1, 'V', 1): 1.0,
 (1, 0, 'E', 1): 4.9,
 (1, 0, 'G', 0): 2.1,
 (1, 0, 'M', 2): 5.8,
 (1, 0, 'M', 3): 0.2,
 (1, 0, 'S', 1): 4.2,
 (1, 0, 'T', 2): 0.7,
 (1, 0, 'U', 0): 6.0,
 (1, 0, 'V', 0): 2.9,
 (1, 1, 'E', 0): 0.5,
 (1, 1, 'E', 1): 6.0,
 (1, 1, 'E', 2): 0.4,
 (1, 1, 'E', 3): 2.6,
 (1, 1, 'G', 2): 1.1,
 (1, 1, 'G', 3): 2.6,
 (1, 1, 'S', 3): 2.3,
 (1, 1, 'T', 0): 2.6,
 (1, 1, 'T', 1): 5.9,
 (1, 1, 'T', 3): 4.9,
 (1, 1, 'Z', 0): 5.4}
HOLD = {(0, 0, 'D', 0): 82,
 (0, 0, 'E', 0): 95,
 (0, 0, 'T', 2): 42,
 (0, 0, 'U', 3): 38,
 (0, 1, 'E', 0): 93,
 (1, 0, 'D', 1): 91,
 (1, 0, 'G', 2): 29,
 (1, 0, 'S', 0): 27,
 (1, 0, 'T', 1): 36,
 (1, 0, 'U', 0): 69,
 (1, 0, 'V', 0): 69,
 (1, 1, 'E', 0): 64,
 (1, 1, 'E', 2): 64,
 (1, 1, 'T', 1): 65}


def plan(zs):
    half = zs // 2
    cores = [(h, c) for h in range(half) for c in (0, 1)]
    need, when, ready = {}, {}, {d: [] for d in cores}
    order = {d: [] for d in cores}
    pieces = {"T": KD, "D": KR, "E": KR, "M": KR, "F": KR}
    events, busy, links, turn = [], dict.fromkeys(cores, 0.0), {}, [0]

    def post(at, what, key):
        turn[0] += 1
        heapq.heappush(events, (at, turn[0], what, key))

    def way_of(h, name, b):
        if name == "S" or (name == "G" and b < h) or (name == "M" and b > h):
            return h, 1
        if name in "ZGM":
            return h, 0
        return (h, 2) if name in "DE" else None

    def release(d, name, b, k):
        key = d + ((name, k * 4 // KD) if name in "SZ" else (name, b))
        at = max(when[d, name, b, k], HOLD.get(key, 0.0))
        if name in "SZ" and k + d[1] == 0:
            key, at = (), START
        bisect.insort(ready[d], (PRIO.get(key, RANK[name]) + 0.01 * k, abs(b - d[0]), name, b, k,
                                 at, way_of(d[0], name, b)))

    def task(d, name, b, k, deps, at=0.0):
        need[d, name, b, k], when[d, name, b, k] = deps, at
        if deps == 0:
            release(d, name, b, k)

    for d in cores:
        h, c = d
        for b in range(zs):
            for k in range(KD):
                task(d, "T", b, k, int(b != h), PACK if b == h else 0.0)
                if b != h and (h < zs - 1 if b < h else h > 0):
                    task(d, "G", b, k, 1)
            for name, other in (("U", "D"), ("V", "E")):
                task(d, name, b, 0, KD)
                for k in range(KR):
                    task(d, other, b, k, 1)
            for k in range(KR):
                if b == h:
                    task(d, "F", b, k, 2 + (h > 0) + (h < zs - 1))
                else:
                    task(d, "M", b, k, 2 + (h > 0 if b > h else h < zs - 1))
        if c == 0:
            task(d, "N", h + 1, 0, 1)
        for k in range(KD):
            for name in "SZ" if h > 0 else "S":
                task(d, name, h, k, c + (k > 0), START)
        post(START, "core", d)
        post(PACK, "core", d)

    def supply(d, name, b, k, at):
        if d[0] >= half:
            d, b = (zs - 1 - d[0], d[1]), zs - 1 - b
        key = (d, name, b, k)
        need[key] -= 1
        when[key] = max(when[key], at)
        if need[key] == 0:
            release(*key)
        post(at, "core", d)

    def settle(key, t):
        lk = links[key]
        live = [q for q in lk["queues"] if q]
        for q in live:
            q[0][0] -= (t - lk["at"]) / len(live)
        lk["at"] = t
        for q in live:
            while q and q[0][0] <= 1e-6:
                for e in q.pop(0)[1]:
                    supply(*e, t + LAG[key[1]])
        lk["stamp"] += 1
        live = [q for q in lk["queues"] if q]
        if live:
            post(t + min(q[0][0] for q in live) * len(live), "link", (key, lk["stamp"]))

    def wire(key, c, time, t, targets):
        lk = links.setdefault(key, {"at": 0.0, "queues": ([], []), "stamp": 0})
        if any(lk["queues"]):
            settle(key, t)
        lk["at"] = t
        lk["queues"][c].append([time, targets])
        settle(key, t)

    def backlog(key, c, t):
        lk = links.get(key)
        if lk is None:
            return 0.0
        return sum(x[0] for x in lk["queues"][c]) * sum(map(bool, lk["queues"]))

    def onward(h, c, way, b, k, name, time, t):
        g = h + 2 * way - 1
        wire((h, way), c, time, t, [((g, c), "F" if name == "M" and g == b else name, b, k)])

    def pick(d, t):
        later, full = None, {}
        for i, x in enumerate(ready[d]):
            at, gate = x[5:]
            if at <= t + 1e-9 and gate is not None:
                if gate not in full:
                    full[gate] = backlog(gate, d[1], t) - BACKLOG
                at = t + full[gate] if full[gate] > 1e-6 else at
            if at <= t + 1e-9:
                return ready[d].pop(i)[2:5]
            later = at if later is None else min(later, at)
        if later is not None:
            post(max(later, t + 0.1), "core", d)
        return None

    while events:
        t, _, what, key = heapq.heappop(events)
        if what == "link":
            if links[key[0]]["stamp"] == key[1]:
                settle(key[0], t)
            continue
        d = key
        if busy[d] > t + 1e-9:
            continue
        choice = pick(d, t)
        if choice is None:
            continue
        h, c = d
        name, b, k = choice
        order[d].append(choice)
        done = t + STEP + COST.get(name, 0.0) / pieces.get(name, 1)
        done += 0.3 if k == 0 and name in "TM" else 0.0
        if name in "SZ":
            onward(h, c, int(name == "S"), b, k, "T", Z_BLOCK / KD, t)
            if k + 1 < KD:
                supply(d, name, b, k + 1, done)
        elif name == "G":
            onward(h, c, int(b < h), b, k, "T", Z_BLOCK / KD, t)
        elif name == "T":
            if (d, "G", b, k) in need:
                supply(d, "G", b, k, done)
            if c == 0 and b == h + 1 and k == KD * HANDOVER // 8:
                supply(d, "N", b, 0, done)
            wire((h, 2), c, Y_BLOCK / KD, t, [(d, "U", b, 0), ((h, 1 - c), "V", b, 0)])
        elif name == "N":
            for r in range(KD):
                for s in "SZ" if h > 0 else "S":
                    supply((h, 1), s, h, r, done + 0.3)
        elif name in "UV":
            for r in range(KR):
                supply(d, "D" if name == "U" else "E", b, r, done)
        elif name in "DE":
            wire((h, 2), c, Y_BLOCK / KR / 2, t + STEP,
                 [((h, c if name == "D" else 1 - c), "F" if b == h else "M", b, k)])
        elif name == "M":
            onward(h, c, int(b > h), b, k, "M", Z_BLOCK / KR, t + STEP)
        busy[d] = done
        post(done, "core", d)
    assert sum(map(len, order.values())) == len(need)
    return order


def tables(zs):
    order = plan(zs)

    def code(name, b, k):
        return (KINDS.index(name) * zs + b) * max(KD, KR) + k

    def listed(h, c):
        todo = list(order[min(h, zs - 1 - h), c])
        if h >= zs // 2:
            todo = [({"S": "Z", "Z": "S"}.get(name, name), zs - 1 - b, k) for name, b, k in todo]
        if c == 0:
            todo = [x for x in todo if x[0] not in "SZ" or x[2] > 0]
        names = [x[0] for x in todo]
        first = min(names.index("U"), names.index("V"))
        todo.insert(first, ("W", 0, 0))
        if c == 1:
            turn = min(i for i, x in enumerate(todo) if x[0] in "SZ")
            todo.insert(turn, ("Q", 0, 0))
        return todo

    lists = [listed(h, c) for h in range(zs) for c in (0, 1)]
    return [[code(*x) for x in o] for o in lists]


def kernel(n, cap, table, tok_ref, gain_ref, ids_ref, gw_ref, wg_ref, wu_ref, wd_ref, out_ref,
           wg, wu, wd, lines, places, outgoing, arrived, results, returned, hidden, chain,
           pick, high, low, raw,
           tsem, wsem, lsend, lrecv, psend, precv, dsend, drecv, bsend, brecv, csend, crecv, turn):
    zs = n // SUB
    me = lax.axis_index("ep")
    hi, lo = me // SUB, me % SUB
    core = (lo + 1) % 2
    tok, width = tok_ref.shape
    ff = wg.shape[1]
    rows = SUB * cap
    dcols, rcols = width // KD, width // KR

    def peer(plane, part):
        return {"ep": plane * SUB + part}

    pieces = [pl.ds(i * (tok // PIECES), tok // PIECES) for i in range(PIECES)]
    t_copies = [pltpu.make_async_copy(tok_ref.at[at, :], raw.at[at, :], tsem.at[i])
                for i, at in enumerate(pieces)]
    for c in t_copies:
        c.start()

    barrier = pltpu.get_barrier_semaphore()

    def greet(to):
        pl.semaphore_signal(barrier, inc=1, device_id=to, device_id_type=pl.DeviceIdType.MESH)

    for dl in range(1, SUB):
        greet(peer(hi, (lo + dl) % SUB))

    @pl.when(hi > 0)
    def _():
        greet(peer((hi + zs - 1) % zs, lo))

    @pl.when(hi < zs - 1)
    def _():
        greet(peer((hi + 1) % zs, lo))

    w_copies = [
        pltpu.make_async_copy(wg_ref.at[0], wg, wsem.at[0]),
        pltpu.make_async_copy(wu_ref.at[0], wu, wsem.at[1]),
        pltpu.make_async_copy(wd_ref.at[0], wd, wsem.at[2]),
    ]
    for c in w_copies:
        c.start()

    def remote(src, dst, send, recv, to):
        return pltpu.make_async_remote_copy(
            src_ref=src, dst_ref=dst, send_sem=send, recv_sem=recv,
            device_id=to, device_id_type=pl.DeviceIdType.MESH)

    def dcol(k):
        return pl.ds(pl.multiple_of(k * dcols, dcols), dcols)

    def rcol(k):
        return pl.ds(pl.multiple_of(k * rcols, rcols), rcols)

    def slot_rows(j, dl):
        return pl.ds(pl.multiple_of(j * rows + (dl // 2 + dl % 2 * 2) * cap, cap), cap)

    def side_rows(j, side):
        return pl.ds(pl.multiple_of(j * rows + side * 2 * cap, 2 * cap), 2 * cap)

    def block_rows(j):
        return pl.ds(pl.multiple_of(j * rows, rows), rows)

    def far_rows(j):
        return pl.ds(pl.multiple_of(j * rows + cap, cap), rows - cap)

    def onward(way):
        return (hi + 2 * way - 1 + zs) % zs

    def line_copy(block, k, way):
        part = lines.at[block, :, dcol(k)]
        return remote(part, part, lsend.at[way * zs + block], lrecv.at[block * KD + k],
                      peer(onward(way), lo))

    def place_copy(block, way):
        return remote(places.at[block], places.at[block], psend.at[way * zs + block],
                      precv.at[block], peer(onward(way), lo))

    def out_copy(j, dl, k):
        at = slot_rows(j, dl)
        return remote(outgoing.at[at, dcol(k)], arrived.at[at, dcol(k)],
                      dsend.at[j], drecv.at[(j * 2 + dl % 2) * KD + k], peer(hi, (lo + dl) % SUB))

    def out_arrival(j, side, k):
        at = arrived.at[side_rows(j, 1) if side else slot_rows(j, 2), dcol(k)]
        return remote(at, at, dsend.at[j], drecv.at[(j * 2 + side) * KD + k],
                      peer(hi, (lo + 1) % SUB))

    def back_copy(j, dl, k):
        at = slot_rows(j, dl)
        return remote(results.at[at, rcol(k)], returned.at[at, rcol(k)],
                      bsend.at[j], brecv.at[j * KR + k], peer(hi, (lo - dl + SUB) % SUB))

    def back_arrival(j, k):
        at = returned.at[far_rows(j), rcol(k)]
        return remote(at, at, bsend.at[j], brecv.at[j * KR + k], peer(hi, (lo + 1) % SUB))

    def chain_copy(way, j, k):
        part = chain.at[way * zs + j, :, rcol(k)]
        return remote(part, part, csend.at[way * zs + j], crecv.at[(way * zs + j) * KR + k],
                      peer(onward(way), lo))

    bits = (len(KINDS) * zs * max(KD, KR) - 1).bit_length()
    many = 30 // bits
    where_am_i = hi * 2 + core
    words = []
    for i in range(0, max(map(len, table)), many):
        packed = [sum(x << bits * r for r, x in enumerate(row[i:i + many])) for row in table]
        word = jnp.int32(packed[0])
        for at in range(1, 2 * zs):
            word = jnp.where(where_am_i == at, packed[at], word)
        words.append(word)
    words += [jnp.int32(0)] * (-len(words) % GROUP)
    count = jnp.int32(len(table[0]))
    for at in range(1, 2 * zs):
        count = jnp.where(where_am_i == at, len(table[at]), count)

    step = 32

    def norm(i, carry):
        at = pl.ds(pl.multiple_of(i * step, step), step)
        v = raw[at, :].astype(jnp.float32)
        scale = lax.rsqrt(jnp.mean(v * v, -1, keepdims=True) + 1e-06)
        lines[hi, at, :] = (v * scale * gain_ref[...]).astype(jnp.bfloat16)
        return carry

    per = tok // PIECES // step
    for i, c in enumerate(t_copies):
        c.wait()
        lax.fori_loop(i * per, (i + 1) * per, norm, 0)

    ends = jnp.where(hi == 0, 1, 0) + jnp.where(hi == zs - 1, 1, 0)
    pl.semaphore_wait(barrier, SUB + 1 - ends)

    def forward(way, act):
        @pl.when(jnp.where(way == 1, zs - 1 - hi, hi) > 0)
        def _():
            act(way)

    def send_own(way, k):
        forward(way, lambda w: line_copy(hi, k, w).start())

    def send_places(way):
        forward(way, lambda w: place_copy(hi, w).start())

    @pl.when(core == 0)
    def _():
        for way in (1, 0):
            send_own(way, 0)

    expert = lax.broadcasted_iota(jnp.int32, (n, tok), 0)
    id0, id1 = ids_ref[0:1, :], ids_ref[1:2, :]
    chosen = jnp.where((id0 == expert) | (id1 == expert), 1.0, 0.0).astype(jnp.bfloat16)
    t_row = lax.broadcasted_iota(jnp.int32, (tok, tok), 0)
    t_col = lax.broadcasted_iota(jnp.int32, (tok, tok), 1)
    earlier = jnp.where(t_row < t_col, 1.0, 0.0).astype(jnp.bfloat16)
    before = jnp.dot(chosen, earlier, preferred_element_type=jnp.float32)

    def dest(ids):
        slot = jnp.sum(jnp.where(ids == expert, before, 0.0), axis=0, keepdims=True)
        return ids.astype(jnp.float32) * cap + slot

    where = lax.broadcasted_iota(jnp.int32, (8, tok), 0)
    places[hi] = jnp.where(
        where == 0, dest(id0), jnp.where(
            where == 1, dest(id1), jnp.where(where == 2, gw_ref[0:1, :], gw_ref[1:2, :])))

    @pl.when(core == 0)
    def _():
        for way in (1, 0):
            send_places(way)

    def send_line(way, k):
        @pl.when((core == 1) & (k == 0))
        def _():
            send_places(way)

        send_own(way, k)

    def row_index():
        r = lax.broadcasted_iota(jnp.int32, (rows, tok), 0)
        dl = r // cap % 2 * 2 + r // cap // 2
        return ((hi * SUB + (lo + dl) % SUB) * cap + r % cap).astype(jnp.float32)

    def choose(j, at):
        index = row_index()
        w = places[j]
        pick[at] = jnp.where((index == w[0:1, :]) | (index == w[1:2, :]), 1.0, 0.0).astype(
            jnp.bfloat16)

    def pack(j, k, at):
        got = jnp.dot(pick[at], lines[j, :, dcol(k)],
                      preferred_element_type=jnp.float32).astype(jnp.bfloat16)
        outgoing[far_rows(j), dcol(k)] = got[cap:, :]
        for dl in range(1, SUB):
            out_copy(j, dl, k).start()
        arrived[slot_rows(j, 0), dcol(k)] = got[:cap, :]

    ftile = min(ff, 256)

    def up(j, side):
        for which in (0, 1):
            @pl.when(side == which)
            def _():
                def landed(k, carry):
                    out_arrival(j, which, k).wait_recv()
                    return carry

                lax.fori_loop(0, KD, landed, 0)

        def tile(f, carry):
            cols = pl.ds(pl.multiple_of(f * ftile, ftile), ftile)
            x = arrived[side_rows(j, side), :]
            g = jnp.dot(x, wg[:, cols], preferred_element_type=jnp.float32)
            u = jnp.dot(x, wu[:, cols], preferred_element_type=jnp.float32)
            hidden[j * 2 + side, :, cols] = (g / (1.0 + jnp.exp(-g)) * u).astype(jnp.bfloat16)
            return carry

        lax.fori_loop(0, ff // ftile, tile, 0)

    def down(j, side, k):
        got = jnp.dot(hidden[j * 2 + side], wd[:, rcol(k)],
                      preferred_element_type=jnp.float32).astype(jnp.bfloat16)

        @pl.when(side == 0)
        def _():
            results[slot_rows(j, 2), rcol(k)] = got[cap:, :]
            back_copy(j, 2, k).start()
            returned[slot_rows(j, 0), rcol(k)] = got[:cap, :]

        @pl.when(side == 1)
        def _():
            results[side_rows(j, 1), rcol(k)] = got
            for dl in (1, 3):
                back_copy(j, dl, k).start()

    def weigh(j, at):
        index = row_index()
        w = places[j]
        weight = jnp.transpose(jnp.where(index == w[0:1, :], w[2:3, :], 0.0)
                               + jnp.where(index == w[1:2, :], w[3:4, :], 0.0))
        top = weight.astype(jnp.bfloat16)
        high[at] = top
        low[at] = (weight - top.astype(jnp.float32)).astype(jnp.bfloat16)

    def mix(j, k, at):
        block = returned[block_rows(j), rcol(k)]
        return (jnp.dot(high[at], block, preferred_element_type=jnp.float32)
                + jnp.dot(low[at], block, preferred_element_type=jnp.float32))

    def take(j, k):
        way = jnp.where(j < hi, 1, 0)

        @pl.when((k == 0) & (j != hi))
        def _():
            place_copy(j, way).wait_recv()

        @pl.when(k == 0)
        def _():
            choose(j, j)

        @pl.when(j != hi)
        def _():
            line_copy(j, k, way).wait_recv()

        pack(j, k, j)

    def pass_on(j, k):
        way = jnp.where(j < hi, 1, 0)

        @pl.when(k == 0)
        def _():
            place_copy(j, way).start()

        line_copy(j, k, way).start()

    def add(j, k):
        way = jnp.where(j > hi, 1, 0)

        @pl.when(k == 0)
        def _():
            weigh(j, j)

        back_arrival(j, k).wait_recv()
        value = mix(j, k, j)
        at = way * zs + j
        beyond = way * hi + (1 - way) * (zs - 1 - hi)

        @pl.when(beyond > 0)
        def _():
            chain_copy(way, j, k).wait_recv()
            chain[at, :, rcol(k)] = (
                value + chain[at, :, rcol(k)].astype(jnp.float32)).astype(jnp.bfloat16)

        @pl.when(beyond == 0)
        def _():
            chain[at, :, rcol(k)] = value.astype(jnp.bfloat16)

        chain_copy(way, j, k).start()

    def final(k):
        @pl.when(k == 0)
        def _():
            weigh(hi, hi)

        back_arrival(hi, k).wait_recv()
        value = mix(hi, k, hi)

        def arrived_from(way):
            chain_copy(way, hi, k).wait_recv()
            return chain[way * zs + hi, :, rcol(k)].astype(jnp.float32)

        def put(total):
            out_ref[:, rcol(k)] = total.astype(out_ref.dtype)

        @pl.when(hi == 0)
        def _():
            put(value + arrived_from(0))

        @pl.when(hi == zs - 1)
        def _():
            put(value + arrived_from(1))

        @pl.when((hi > 0) & (hi < zs - 1))
        def _():
            put(value + arrived_from(0) + arrived_from(1))

    def run(near, i, carry):
        spot, digit = lax.div(i, many), lax.rem(i, many)
        word = near[0]
        for at in range(1, len(near)):
            word = jnp.where(spot == at, near[at], word)
        for r in range(1, many):
            word = jnp.where(digit >= r, lax.div(word, 1 << bits), word)
        code = lax.rem(word, 1 << bits)
        kind = lax.div(code, zs * max(KD, KR))
        j = lax.rem(lax.div(code, max(KD, KR)), zs)
        k = lax.rem(code, max(KD, KR))

        acts = {
            "S": lambda: send_line(1, k),
            "Z": lambda: send_line(0, k),
            "G": lambda: pass_on(j, k),
            "T": lambda: take(j, k),
            "U": lambda: up(j, kind - KINDS.index("U")),
            "D": lambda: down(j, kind - KINDS.index("D"), k),
            "M": lambda: add(j, k),
            "F": lambda: final(k),
            "W": lambda: [c.wait() for c in w_copies],
            "N": lambda: pl.semaphore_signal(
                turn, inc=1, device_id=peer(hi, lo - 1), device_id_type=pl.DeviceIdType.MESH),
            "Q": lambda: pl.semaphore_wait(turn, 1),
        }

        def among(names):
            if len(names) == 1:
                acts[names[0]]()
                return
            cut = len(names) // 2
            low = kind < KINDS.index(names[cut])
            pl.when(low)(lambda: among(names[:cut]))
            pl.when(jnp.logical_not(low))(lambda: among(names[cut:]))

        among(list(acts))
        return carry

    def turns(a, carry):
        near = []
        for r in range(GROUP):
            word = words[r]
            for at in range(1, len(words) // GROUP):
                word = jnp.where(a == at, words[at * GROUP + r], word)
            near.append(word)
        left = jnp.minimum(GROUP * many, count - a * (GROUP * many))
        return lax.fori_loop(0, left, functools.partial(run, near), carry)

    lax.fori_loop(0, lax.div(count + (GROUP * many - 1), GROUP * many), turns, 0)

    def finish(j, carry):
        at = far_rows(j)
        remote(outgoing.at[at, :], outgoing.at[at, :], dsend.at[j], drecv.at[0],
               peer(hi, (lo + 1) % SUB)).wait_send()
        remote(results.at[at, :], results.at[at, :], bsend.at[j], brecv.at[0],
               peer(hi, (lo + 1) % SUB)).wait_send()
        for way in (0, 1):
            to = peer(onward(way), lo)

            @pl.when((hi < zs - 1) & (j <= hi) if way else (hi > 0) & (j >= hi))
            def _():
                place_copy(j, way).wait_send()
                remote(lines.at[j], lines.at[j], lsend.at[way * zs + j], lrecv.at[0],
                       to).wait_send()

            @pl.when(j > hi if way else j < hi)
            def _():
                at = way * zs + j
                remote(chain.at[at], chain.at[at], csend.at[at], crecv.at[0], to).wait_send()

        return carry

    lax.fori_loop(0, zs, finish, 0)


def per_device(tokens, norm_gain, expert_ids, gate_weights, w_gate, w_up, w_down):
    n = lax.axis_size("ep")
    tok, width = tokens.shape
    top = expert_ids.shape[1]
    ff = w_gate.shape[2]
    cap = 2 * tok * top // n
    total = n * cap
    zs = n // SUB
    rows = SUB * cap
    table = tables(zs)
    bf16 = jnp.bfloat16
    dma = pltpu.SemaphoreType.DMA
    vmem = pl.BlockSpec(memory_space=pltpu.VMEM)
    hbm = pl.BlockSpec(memory_space=pl.ANY)
    return pl.pallas_call(
        functools.partial(kernel, n, cap, table),
        out_shape=pltpu.VMEM((tok, width), bf16),
        in_specs=[hbm] + [vmem] * 3 + [hbm] * 3,
        out_specs=vmem,
        scratch_shapes=[
            pltpu.VMEM((width, ff), bf16),
            pltpu.VMEM((width, ff), bf16),
            pltpu.VMEM((ff, width), bf16),
            pltpu.VMEM((zs, tok, width), bf16),
            pltpu.VMEM((zs, 8, tok), jnp.float32),
            pltpu.VMEM((total, width), bf16),
            pltpu.VMEM((total, width), bf16),
            pltpu.VMEM((total, width), bf16),
            pltpu.VMEM((total, width), bf16),
            pltpu.VMEM((2 * zs, rows // 2, ff), bf16),
            pltpu.VMEM((2 * zs, tok, width), bf16),
            pltpu.VMEM((zs, rows, tok), bf16),
            pltpu.VMEM((zs, tok, rows), bf16),
            pltpu.VMEM((zs, tok, rows), bf16),
            pltpu.VMEM((tok, width), bf16),
            dma((PIECES,)),
            dma((3,)),
            dma((2 * zs,)),
            dma((zs * KD,)),
            dma((2 * zs,)),
            dma((zs,)),
            dma((zs,)),
            dma((2 * zs * KD,)),
            dma((zs,)),
            dma((zs * KR,)),
            dma((2 * zs,)),
            dma((2 * zs * KR,)),
            pltpu.SemaphoreType.REGULAR,
        ],
        compiler_params=pltpu.CompilerParams(
            collective_id=0, has_side_effects=True, vmem_limit_bytes=58 * 1024 * 1024),
    )(tokens, norm_gain.reshape(1, width), expert_ids.T, gate_weights.T, w_gate, w_up, w_down)


def solution(mesh):
    return jax.shard_map(
        per_device,
        mesh=mesh,
        in_specs=(
            P(("grp", "ep"), None),
            P(),
            P(("grp", "ep"), None),
            P(("grp", "ep"), None),
            P("ep", None, None),
            P("ep", None, None),
            P("ep", None, None),
        ),
        out_specs=P(("grp", "ep"), None),
        check_vma=False,
    )
```

```python
import bisect
import functools
import heapq
import jax
import jax.numpy as jnp
from jax import lax
from jax.experimental import pallas as pl
from jax.experimental.pallas import tpu as pltpu
from jax.sharding import PartitionSpec as P

SUB = 4
KD = 8
KR = 8
PIECES = 4
GROUP = 8
KINDS = "SZGTUVDEMFWNQ"
COST = {"T": 1.6, "U": 2.05, "V": 2.05, "D": 1.96, "E": 1.96, "M": 1.84, "F": 1.7, "G": 0.15, "S": 0.1, "Z": 0.1}
RANK = {"S": 0, "Z": 0, "G": 0.5, "T": 1, "N": -1, "M": 2, "F": 3, "D": 4, "E": 4, "U": 5, "V": 5}
Z_BLOCK, Y_BLOCK, START, PACK, STEP, BACKLOG = 11.4, 5.75, 2.9, 3.8, 0.09, 3.0
LAG = (2.2, 2.2, 2.5)
HANDOVER = 4
PRIO = {(0, 0, 'S', 1): 6.0,
 (0, 0, 'T', 2): 5.3,
 (0, 0, 'V', 1): 0.1,
 (0, 1, 'E', 0): 5.5,
 (0, 1, 'T', 1): 5.4,
 (0, 1, 'T', 2): 5.3,
 (0, 1, 'V', 0): 3.4,
 (1, 0, 'D', 0): 2.0,
 (1, 0, 'D', 1): 0.2,
 (1, 0, 'D', 3): 2.4,
 (1, 0, 'E', 3): 0.2,
 (1, 0, 'M', 3): 4.0,
 (1, 0, 'S', 0): 2.6,
 (1, 0, 'T', 0): 4.7,
 (1, 0, 'T', 2): 3.6,
 (1, 0, 'U', 0): 2.4,
 (1, 0, 'U', 2): 1.5,
 (1, 0, 'V', 0): 2.4,
 (1, 0, 'Z', 2): 1.3,
 (1, 1, 'D', 0): 5.1,
 (1, 1, 'D', 1): 0.1,
 (1, 1, 'E', 0): 5.7,
 (1, 1, 'E', 3): 0.3,
 (1, 1, 'G', 0): 2.1,
 (1, 1, 'M', 2): 0.1,
 (1, 1, 'M', 3): 4.0,
 (1, 1, 'S', 1): 4.8,
 (1, 1, 'S', 3): 2.0,
 (1, 1, 'T', 2): 3.6,
 (1, 1, 'T', 3): 5.0,
 (1, 1, 'Z', 0): 5.5}
HOLD = {(0, 0, 'D', 0): 81,
 (0, 0, 'E', 0): 84,
 (0, 1, 'E', 0): 92,
 (1, 0, 'E', 2): 80,
 (1, 0, 'S', 0): 27,
 (1, 0, 'T', 1): 35,
 (1, 0, 'U', 0): 57,
 (1, 0, 'V', 0): 81,
 (1, 1, 'E', 2): 80,
 (1, 1, 'T', 1): 84,
 (1, 1, 'T', 2): 49,
 (1, 1, 'V', 1): 87,
 (1, 1, 'V', 3): 47,
 (1, 1, 'Z', 1): 64}


def plan(zs):
    half = zs // 2
    cores = [(h, c) for h in range(half) for c in (0, 1)]
    need, when, ready = {}, {}, {d: [] for d in cores}
    order = {d: [] for d in cores}
    pieces = {"T": KD, "D": KR, "E": KR, "M": KR, "F": KR}
    events, busy, links, turn = [], dict.fromkeys(cores, 0.0), {}, [0]

    def post(at, what, key):
        turn[0] += 1
        heapq.heappush(events, (at, turn[0], what, key))

    def way_of(h, name, b):
        if name == "S" or (name == "G" and b < h) or (name == "M" and b > h):
            return h, 1
        if name in "ZGM":
            return h, 0
        return (h, 2) if name in "DE" else None

    def release(d, name, b, k):
        key = d + ((name, k * 4 // KD) if name in "SZ" else (name, b))
        at = max(when[d, name, b, k], HOLD.get(key, 0.0))
        if name in "SZ" and k + d[1] == 0:
            key, at = (), START
        bisect.insort(ready[d], (PRIO.get(key, RANK[name]) + 0.01 * k, abs(b - d[0]), name, b, k,
                                 at, way_of(d[0], name, b)))

    def task(d, name, b, k, deps, at=0.0):
        need[d, name, b, k], when[d, name, b, k] = deps, at
        if deps == 0:
            release(d, name, b, k)

    for d in cores:
        h, c = d
        for b in range(zs):
            for k in range(KD):
                task(d, "T", b, k, int(b != h), PACK if b == h else 0.0)
                if b != h and (h < zs - 1 if b < h else h > 0):
                    task(d, "G", b, k, 1)
            for name, other in (("U", "D"), ("V", "E")):
                task(d, name, b, 0, KD)
                for k in range(KR):
                    task(d, other, b, k, 1)
            for k in range(KR):
                if b == h:
                    task(d, "F", b, k, 2 + (h > 0) + (h < zs - 1))
                else:
                    task(d, "M", b, k, 2 + (h > 0 if b > h else h < zs - 1))
        if c == 0:
            task(d, "N", h + 1, 0, 1)
        for k in range(KD):
            for name in "SZ" if h > 0 else "S":
                task(d, name, h, k, c + (k > 0), START)
        post(START, "core", d)
        post(PACK, "core", d)

    def supply(d, name, b, k, at):
        if d[0] >= half:
            d, b = (zs - 1 - d[0], d[1]), zs - 1 - b
        key = (d, name, b, k)
        need[key] -= 1
        when[key] = max(when[key], at)
        if need[key] == 0:
            release(*key)
        post(at, "core", d)

    def settle(key, t):
        lk = links[key]
        live = [q for q in lk["queues"] if q]
        for q in live:
            q[0][0] -= (t - lk["at"]) / len(live)
        lk["at"] = t
        for q in live:
            while q and q[0][0] <= 1e-6:
                for e in q.pop(0)[1]:
                    supply(*e, t + LAG[key[1]])
        lk["stamp"] += 1
        live = [q for q in lk["queues"] if q]
        if live:
            post(t + min(q[0][0] for q in live) * len(live), "link", (key, lk["stamp"]))

    def wire(key, c, time, t, targets):
        lk = links.setdefault(key, {"at": 0.0, "queues": ([], []), "stamp": 0})
        if any(lk["queues"]):
            settle(key, t)
        lk["at"] = t
        lk["queues"][c].append([time, targets])
        settle(key, t)

    def backlog(key, c, t):
        lk = links.get(key)
        if lk is None:
            return 0.0
        return sum(x[0] for x in lk["queues"][c]) * sum(map(bool, lk["queues"]))

    def onward(h, c, way, b, k, name, time, t):
        g = h + 2 * way - 1
        wire((h, way), c, time, t, [((g, c), "F" if name == "M" and g == b else name, b, k)])

    def pick(d, t):
        later, full = None, {}
        for i, x in enumerate(ready[d]):
            at, gate = x[5:]
            if at <= t + 1e-9 and gate is not None:
                if gate not in full:
                    full[gate] = backlog(gate, d[1], t) - BACKLOG
                at = t + full[gate] if full[gate] > 1e-6 else at
            if at <= t + 1e-9:
                return ready[d].pop(i)[2:5]
            later = at if later is None else min(later, at)
        if later is not None:
            post(max(later, t + 0.1), "core", d)
        return None

    while events:
        t, _, what, key = heapq.heappop(events)
        if what == "link":
            if links[key[0]]["stamp"] == key[1]:
                settle(key[0], t)
            continue
        d = key
        if busy[d] > t + 1e-9:
            continue
        choice = pick(d, t)
        if choice is None:
            continue
        h, c = d
        name, b, k = choice
        order[d].append(choice)
        done = t + STEP + COST.get(name, 0.0) / pieces.get(name, 1)
        done += 0.3 if k == 0 and name in "TM" else 0.0
        if name in "SZ":
            onward(h, c, int(name == "S"), b, k, "T", Z_BLOCK / KD, t)
            if k + 1 < KD:
                supply(d, name, b, k + 1, done)
        elif name == "G":
            onward(h, c, int(b < h), b, k, "T", Z_BLOCK / KD, t)
        elif name == "T":
            if (d, "G", b, k) in need:
                supply(d, "G", b, k, done)
            if c == 0 and b == h + 1 and k == KD * HANDOVER // 8:
                supply(d, "N", b, 0, done)
            wire((h, 2), c, Y_BLOCK / KD, t, [(d, "U", b, 0), ((h, 1 - c), "V", b, 0)])
        elif name == "N":
            for r in range(KD):
                for s in "SZ" if h > 0 else "S":
                    supply((h, 1), s, h, r, done + 0.3)
        elif name in "UV":
            for r in range(KR):
                supply(d, "D" if name == "U" else "E", b, r, done)
        elif name in "DE":
            wire((h, 2), c, Y_BLOCK / KR / 2, t + STEP,
                 [((h, c if name == "D" else 1 - c), "F" if b == h else "M", b, k)])
        elif name == "M":
            onward(h, c, int(b > h), b, k, "M", Z_BLOCK / KR, t + STEP)
        busy[d] = done
        post(done, "core", d)
    assert sum(map(len, order.values())) == len(need)
    return order


def tables(zs):
    order = plan(zs)

    def code(name, b, k):
        return (KINDS.index(name) * zs + b) * max(KD, KR) + k

    def listed(h, c):
        todo = list(order[min(h, zs - 1 - h), c])
        if h >= zs // 2:
            todo = [({"S": "Z", "Z": "S"}.get(name, name), zs - 1 - b, k) for name, b, k in todo]
        if c == 0:
            todo = [x for x in todo if x[0] not in "SZ" or x[2] > 0]
        names = [x[0] for x in todo]
        first = min(names.index("U"), names.index("V"))
        todo.insert(first, ("W", 0, 0))
        if c == 1:
            turn = min(i for i, x in enumerate(todo) if x[0] in "SZ")
            todo.insert(turn, ("Q", 0, 0))
        return todo

    lists = [listed(h, c) for h in range(zs) for c in (0, 1)]
    return [[code(*x) for x in o] for o in lists]


def kernel(n, cap, table, tok_ref, gain_ref, ids_ref, gw_ref, wg_ref, wu_ref, wd_ref, out_ref,
           wg, wu, wd, lines, places, outgoing, arrived, results, returned, hidden, chain,
           pick, high, low, raw,
           tsem, wsem, lsend, lrecv, psend, precv, dsend, drecv, bsend, brecv, csend, crecv, turn):
    zs = n // SUB
    me = lax.axis_index("ep")
    hi, lo = me // SUB, me % SUB
    core = (lo + 1) % 2
    tok, width = tok_ref.shape
    ff = wg.shape[1]
    rows = SUB * cap
    dcols, rcols = width // KD, width // KR

    def peer(plane, part):
        return {"ep": plane * SUB + part}

    pieces = [pl.ds(i * (tok // PIECES), tok // PIECES) for i in range(PIECES)]
    t_copies = [pltpu.make_async_copy(tok_ref.at[at, :], raw.at[at, :], tsem.at[i])
                for i, at in enumerate(pieces)]
    for c in t_copies:
        c.start()

    barrier = pltpu.get_barrier_semaphore()

    def greet(to):
        pl.semaphore_signal(barrier, inc=1, device_id=to, device_id_type=pl.DeviceIdType.MESH)

    for dl in range(1, SUB):
        greet(peer(hi, (lo + dl) % SUB))

    @pl.when(hi > 0)
    def _():
        greet(peer((hi + zs - 1) % zs, lo))

    @pl.when(hi < zs - 1)
    def _():
        greet(peer((hi + 1) % zs, lo))

    w_copies = [
        pltpu.make_async_copy(wg_ref.at[0], wg, wsem.at[0]),
        pltpu.make_async_copy(wu_ref.at[0], wu, wsem.at[1]),
        pltpu.make_async_copy(wd_ref.at[0], wd, wsem.at[2]),
    ]
    for c in w_copies:
        c.start()

    def remote(src, dst, send, recv, to):
        return pltpu.make_async_remote_copy(
            src_ref=src, dst_ref=dst, send_sem=send, recv_sem=recv,
            device_id=to, device_id_type=pl.DeviceIdType.MESH)

    def dcol(k):
        return pl.ds(pl.multiple_of(k * dcols, dcols), dcols)

    def rcol(k):
        return pl.ds(pl.multiple_of(k * rcols, rcols), rcols)

    def slot_rows(j, dl):
        return pl.ds(pl.multiple_of(j * rows + (dl // 2 + dl % 2 * 2) * cap, cap), cap)

    def side_rows(j, side):
        return pl.ds(pl.multiple_of(j * rows + side * 2 * cap, 2 * cap), 2 * cap)

    def block_rows(j):
        return pl.ds(pl.multiple_of(j * rows, rows), rows)

    def far_rows(j):
        return pl.ds(pl.multiple_of(j * rows + cap, cap), rows - cap)

    def onward(way):
        return (hi + 2 * way - 1 + zs) % zs

    def line_copy(block, k, way):
        part = lines.at[block, :, dcol(k)]
        return remote(part, part, lsend.at[way * zs + block], lrecv.at[block * KD + k],
                      peer(onward(way), lo))

    def place_copy(block, way):
        return remote(places.at[block], places.at[block], psend.at[way * zs + block],
                      precv.at[block], peer(onward(way), lo))

    def out_copy(j, dl, k):
        at = slot_rows(j, dl)
        return remote(outgoing.at[at, dcol(k)], arrived.at[at, dcol(k)],
                      dsend.at[j], drecv.at[(j * 2 + dl % 2) * KD + k], peer(hi, (lo + dl) % SUB))

    def out_arrival(j, side, k):
        at = arrived.at[side_rows(j, 1) if side else slot_rows(j, 2), dcol(k)]
        return remote(at, at, dsend.at[j], drecv.at[(j * 2 + side) * KD + k],
                      peer(hi, (lo + 1) % SUB))

    def back_copy(j, dl, k):
        at = slot_rows(j, dl)
        return remote(results.at[at, rcol(k)], returned.at[at, rcol(k)],
                      bsend.at[j], brecv.at[j * KR + k], peer(hi, (lo - dl + SUB) % SUB))

    def back_arrival(j, k):
        at = returned.at[far_rows(j), rcol(k)]
        return remote(at, at, bsend.at[j], brecv.at[j * KR + k], peer(hi, (lo + 1) % SUB))

    def chain_copy(way, j, k):
        part = chain.at[way * zs + j, :, rcol(k)]
        return remote(part, part, csend.at[way * zs + j], crecv.at[(way * zs + j) * KR + k],
                      peer(onward(way), lo))

    bits = (len(KINDS) * zs * max(KD, KR) - 1).bit_length()
    many = 30 // bits
    where_am_i = hi * 2 + core
    words = []
    for i in range(0, max(map(len, table)), many):
        packed = [sum(x << bits * r for r, x in enumerate(row[i:i + many])) for row in table]
        word = jnp.int32(packed[0])
        for at in range(1, 2 * zs):
            word = jnp.where(where_am_i == at, packed[at], word)
        words.append(word)
    words += [jnp.int32(0)] * (-len(words) % GROUP)
    count = jnp.int32(len(table[0]))
    for at in range(1, 2 * zs):
        count = jnp.where(where_am_i == at, len(table[at]), count)

    step = 32

    def norm(i, carry):
        at = pl.ds(pl.multiple_of(i * step, step), step)
        v = raw[at, :].astype(jnp.float32)
        scale = lax.rsqrt(jnp.mean(v * v, -1, keepdims=True) + 1e-06)
        lines[hi, at, :] = (v * scale * gain_ref[...]).astype(jnp.bfloat16)
        return carry

    per = tok // PIECES // step
    for i, c in enumerate(t_copies):
        c.wait()
        lax.fori_loop(i * per, (i + 1) * per, norm, 0)

    ends = jnp.where(hi == 0, 1, 0) + jnp.where(hi == zs - 1, 1, 0)
    pl.semaphore_wait(barrier, SUB + 1 - ends)

    def forward(way, act):
        @pl.when(jnp.where(way == 1, zs - 1 - hi, hi) > 0)
        def _():
            act(way)

    def send_own(way, k):
        forward(way, lambda w: line_copy(hi, k, w).start())

    def send_places(way):
        forward(way, lambda w: place_copy(hi, w).start())

    @pl.when(core == 0)
    def _():
        for way in (1, 0):
            send_own(way, 0)

    expert = lax.broadcasted_iota(jnp.int32, (n, tok), 0)
    id0, id1 = ids_ref[0:1, :], ids_ref[1:2, :]
    chosen = jnp.where((id0 == expert) | (id1 == expert), 1.0, 0.0).astype(jnp.bfloat16)
    t_row = lax.broadcasted_iota(jnp.int32, (tok, tok), 0)
    t_col = lax.broadcasted_iota(jnp.int32, (tok, tok), 1)
    earlier = jnp.where(t_row < t_col, 1.0, 0.0).astype(jnp.bfloat16)
    before = jnp.dot(chosen, earlier, preferred_element_type=jnp.float32)

    def dest(ids):
        slot = jnp.sum(jnp.where(ids == expert, before, 0.0), axis=0, keepdims=True)
        return ids.astype(jnp.float32) * cap + slot

    where = lax.broadcasted_iota(jnp.int32, (8, tok), 0)
    places[hi] = jnp.where(
        where == 0, dest(id0), jnp.where(
            where == 1, dest(id1), jnp.where(where == 2, gw_ref[0:1, :], gw_ref[1:2, :])))

    @pl.when(core == 0)
    def _():
        for way in (1, 0):
            send_places(way)

    def send_line(way, k):
        @pl.when((core == 1) & (k == 0))
        def _():
            send_places(way)

        send_own(way, k)

    def row_index():
        r = lax.broadcasted_iota(jnp.int32, (rows, tok), 0)
        dl = r // cap % 2 * 2 + r // cap // 2
        return ((hi * SUB + (lo + dl) % SUB) * cap + r % cap).astype(jnp.float32)

    def choose(j, at):
        index = row_index()
        w = places[j]
        pick[at] = jnp.where((index == w[0:1, :]) | (index == w[1:2, :]), 1.0, 0.0).astype(
            jnp.bfloat16)

    def pack(j, k, at):
        got = jnp.dot(pick[at], lines[j, :, dcol(k)],
                      preferred_element_type=jnp.float32).astype(jnp.bfloat16)
        outgoing[far_rows(j), dcol(k)] = got[cap:, :]
        for dl in range(1, SUB):
            out_copy(j, dl, k).start()
        arrived[slot_rows(j, 0), dcol(k)] = got[:cap, :]

    ftile = min(ff, 256)

    def up(j, side):
        for which in (0, 1):
            @pl.when(side == which)
            def _():
                def landed(k, carry):
                    out_arrival(j, which, k).wait_recv()
                    return carry

                lax.fori_loop(0, KD, landed, 0)

        def tile(f, carry):
            cols = pl.ds(pl.multiple_of(f * ftile, ftile), ftile)
            x = arrived[side_rows(j, side), :]
            g = jnp.dot(x, wg[:, cols], preferred_element_type=jnp.float32)
            u = jnp.dot(x, wu[:, cols], preferred_element_type=jnp.float32)
            hidden[j * 2 + side, :, cols] = (g / (1.0 + jnp.exp(-g)) * u).astype(jnp.bfloat16)
            return carry

        lax.fori_loop(0, ff // ftile, tile, 0)

    def down(j, side, k):
        got = jnp.dot(hidden[j * 2 + side], wd[:, rcol(k)],
                      preferred_element_type=jnp.float32).astype(jnp.bfloat16)

        @pl.when(side == 0)
        def _():
            results[slot_rows(j, 2), rcol(k)] = got[cap:, :]
            back_copy(j, 2, k).start()
            returned[slot_rows(j, 0), rcol(k)] = got[:cap, :]

        @pl.when(side == 1)
        def _():
            results[side_rows(j, 1), rcol(k)] = got
            for dl in (1, 3):
                back_copy(j, dl, k).start()

    def weigh(j, at):
        index = row_index()
        w = places[j]
        weight = jnp.transpose(jnp.where(index == w[0:1, :], w[2:3, :], 0.0)
                               + jnp.where(index == w[1:2, :], w[3:4, :], 0.0))
        top = weight.astype(jnp.bfloat16)
        high[at] = top
        low[at] = (weight - top.astype(jnp.float32)).astype(jnp.bfloat16)

    def mix(j, k, at):
        block = returned[block_rows(j), rcol(k)]
        return (jnp.dot(high[at], block, preferred_element_type=jnp.float32)
                + jnp.dot(low[at], block, preferred_element_type=jnp.float32))

    def take(j, k):
        way = jnp.where(j < hi, 1, 0)

        @pl.when((k == 0) & (j != hi))
        def _():
            place_copy(j, way).wait_recv()

        @pl.when(k == 0)
        def _():
            choose(j, j)

        @pl.when(j != hi)
        def _():
            line_copy(j, k, way).wait_recv()

        pack(j, k, j)

    def pass_on(j, k):
        way = jnp.where(j < hi, 1, 0)

        @pl.when(k == 0)
        def _():
            place_copy(j, way).start()

        line_copy(j, k, way).start()

    def add(j, k):
        way = jnp.where(j > hi, 1, 0)

        @pl.when(k == 0)
        def _():
            weigh(j, j)

        back_arrival(j, k).wait_recv()
        value = mix(j, k, j)
        at = way * zs + j
        beyond = way * hi + (1 - way) * (zs - 1 - hi)

        @pl.when(beyond > 0)
        def _():
            chain_copy(way, j, k).wait_recv()
            chain[at, :, rcol(k)] = (
                value + chain[at, :, rcol(k)].astype(jnp.float32)).astype(jnp.bfloat16)

        @pl.when(beyond == 0)
        def _():
            chain[at, :, rcol(k)] = value.astype(jnp.bfloat16)

        chain_copy(way, j, k).start()

    def final(k):
        @pl.when(k == 0)
        def _():
            weigh(hi, hi)

        back_arrival(hi, k).wait_recv()
        value = mix(hi, k, hi)

        def arrived_from(way):
            chain_copy(way, hi, k).wait_recv()
            return chain[way * zs + hi, :, rcol(k)].astype(jnp.float32)

        def put(total):
            out_ref[:, rcol(k)] = total.astype(out_ref.dtype)

        @pl.when(hi == 0)
        def _():
            put(value + arrived_from(0))

        @pl.when(hi == zs - 1)
        def _():
            put(value + arrived_from(1))

        @pl.when((hi > 0) & (hi < zs - 1))
        def _():
            put(value + arrived_from(0) + arrived_from(1))

    def run(near, i, carry):
        spot, digit = lax.div(i, many), lax.rem(i, many)
        word = near[0]
        for at in range(1, len(near)):
            word = jnp.where(spot == at, near[at], word)
        for r in range(1, many):
            word = jnp.where(digit >= r, lax.div(word, 1 << bits), word)
        code = lax.rem(word, 1 << bits)
        kind = lax.div(code, zs * max(KD, KR))
        j = lax.rem(lax.div(code, max(KD, KR)), zs)
        k = lax.rem(code, max(KD, KR))

        acts = {
            "S": lambda: send_line(1, k),
            "Z": lambda: send_line(0, k),
            "G": lambda: pass_on(j, k),
            "T": lambda: take(j, k),
            "U": lambda: up(j, kind - KINDS.index("U")),
            "D": lambda: down(j, kind - KINDS.index("D"), k),
            "M": lambda: add(j, k),
            "F": lambda: final(k),
            "W": lambda: [c.wait() for c in w_copies],
            "N": lambda: pl.semaphore_signal(
                turn, inc=1, device_id=peer(hi, lo - 1), device_id_type=pl.DeviceIdType.MESH),
            "Q": lambda: pl.semaphore_wait(turn, 1),
        }

        def among(names):
            if len(names) == 1:
                acts[names[0]]()
                return
            cut = len(names) // 2
            low = kind < KINDS.index(names[cut])
            pl.when(low)(lambda: among(names[:cut]))
            pl.when(jnp.logical_not(low))(lambda: among(names[cut:]))

        among(list(acts))
        return carry

    def turns(a, carry):
        near = []
        for r in range(GROUP):
            word = words[r]
            for at in range(1, len(words) // GROUP):
                word = jnp.where(a == at, words[at * GROUP + r], word)
            near.append(word)
        left = jnp.minimum(GROUP * many, count - a * (GROUP * many))
        return lax.fori_loop(0, left, functools.partial(run, near), carry)

    lax.fori_loop(0, lax.div(count + (GROUP * many - 1), GROUP * many), turns, 0)

    def finish(j, carry):
        at = far_rows(j)
        remote(outgoing.at[at, :], outgoing.at[at, :], dsend.at[j], drecv.at[0],
               peer(hi, (lo + 1) % SUB)).wait_send()
        remote(results.at[at, :], results.at[at, :], bsend.at[j], brecv.at[0],
               peer(hi, (lo + 1) % SUB)).wait_send()
        for way in (0, 1):
            to = peer(onward(way), lo)

            @pl.when((hi < zs - 1) & (j <= hi) if way else (hi > 0) & (j >= hi))
            def _():
                place_copy(j, way).wait_send()
                remote(lines.at[j], lines.at[j], lsend.at[way * zs + j], lrecv.at[0],
                       to).wait_send()

            @pl.when(j > hi if way else j < hi)
            def _():
                at = way * zs + j
                remote(chain.at[at], chain.at[at], csend.at[at], crecv.at[0], to).wait_send()

        return carry

    lax.fori_loop(0, zs, finish, 0)


def per_device(tokens, norm_gain, expert_ids, gate_weights, w_gate, w_up, w_down):
    n = lax.axis_size("ep")
    tok, width = tokens.shape
    top = expert_ids.shape[1]
    ff = w_gate.shape[2]
    cap = 2 * tok * top // n
    total = n * cap
    zs = n // SUB
    rows = SUB * cap
    table = tables(zs)
    bf16 = jnp.bfloat16
    dma = pltpu.SemaphoreType.DMA
    vmem = pl.BlockSpec(memory_space=pltpu.VMEM)
    hbm = pl.BlockSpec(memory_space=pl.ANY)
    return pl.pallas_call(
        functools.partial(kernel, n, cap, table),
        out_shape=pltpu.VMEM((tok, width), bf16),
        in_specs=[hbm] + [vmem] * 3 + [hbm] * 3,
        out_specs=vmem,
        scratch_shapes=[
            pltpu.VMEM((width, ff), bf16),
            pltpu.VMEM((width, ff), bf16),
            pltpu.VMEM((ff, width), bf16),
            pltpu.VMEM((zs, tok, width), bf16),
            pltpu.VMEM((zs, 8, tok), jnp.float32),
            pltpu.VMEM((total, width), bf16),
            pltpu.VMEM((total, width), bf16),
            pltpu.VMEM((total, width), bf16),
            pltpu.VMEM((total, width), bf16),
            pltpu.VMEM((2 * zs, rows // 2, ff), bf16),
            pltpu.VMEM((2 * zs, tok, width), bf16),
            pltpu.VMEM((zs, rows, tok), bf16),
            pltpu.VMEM((zs, tok, rows), bf16),
            pltpu.VMEM((zs, tok, rows), bf16),
            pltpu.VMEM((tok, width), bf16),
            dma((PIECES,)),
            dma((3,)),
            dma((2 * zs,)),
            dma((zs * KD,)),
            dma((2 * zs,)),
            dma((zs,)),
            dma((zs,)),
            dma((2 * zs * KD,)),
            dma((zs,)),
            dma((zs * KR,)),
            dma((2 * zs,)),
            dma((2 * zs * KR,)),
            pltpu.SemaphoreType.REGULAR,
        ],
        compiler_params=pltpu.CompilerParams(
            collective_id=0, has_side_effects=True, vmem_limit_bytes=58 * 1024 * 1024),
    )(tokens, norm_gain.reshape(1, width), expert_ids.T, gate_weights.T, w_gate, w_up, w_down)


def solution(mesh):
    return jax.shard_map(
        per_device,
        mesh=mesh,
        in_specs=(
            P(("grp", "ep"), None),
            P(),
            P(("grp", "ep"), None),
            P(("grp", "ep"), None),
            P("ep", None, None),
            P("ep", None, None),
            P("ep", None, None),
        ),
        out_specs=P(("grp", "ep"), None),
        check_vma=False,
    )
```

```python
import bisect
import functools
import heapq
import jax
import jax.numpy as jnp
from jax import lax
from jax.experimental import pallas as pl
from jax.experimental.pallas import tpu as pltpu
from jax.sharding import PartitionSpec as P

SUB = 4
KD = 8
KR = 8
PIECES = 4
GROUP = 8
KINDS = "SZGTUVDEMFWNQ"
COST = {"T": 1.6, "U": 2.05, "V": 2.05, "D": 1.96, "E": 1.96, "M": 1.84, "F": 1.7, "G": 0.15, "S": 0.1, "Z": 0.1}
RANK = {"S": 0, "Z": 0, "G": 0.5, "T": 1, "N": -1, "M": 2, "F": 3, "D": 4, "E": 4, "U": 5, "V": 5}
Z_BLOCK, Y_BLOCK, START, PACK, STEP, BACKLOG = 11.4, 5.75, 2.9, 3.8, 0.09, 3.0
LAG = (2.2, 2.2, 2.5)
HANDOVER = 4
PRIO = {(0, 0, 'S', 1): 6.0,
 (0, 0, 'T', 2): 5.3,
 (0, 0, 'V', 1): 0.1,
 (0, 1, 'E', 0): 5.5,
 (0, 1, 'T', 1): 5.4,
 (0, 1, 'T', 2): 5.3,
 (0, 1, 'V', 0): 3.4,
 (1, 0, 'D', 0): 2.0,
 (1, 0, 'D', 1): 0.2,
 (1, 0, 'D', 3): 2.4,
 (1, 0, 'E', 3): 0.2,
 (1, 0, 'M', 3): 4.0,
 (1, 0, 'S', 0): 2.6,
 (1, 0, 'T', 0): 4.7,
 (1, 0, 'T', 2): 3.6,
 (1, 0, 'U', 0): 2.4,
 (1, 0, 'U', 2): 1.5,
 (1, 0, 'V', 0): 2.4,
 (1, 0, 'Z', 2): 1.3,
 (1, 1, 'D', 0): 5.1,
 (1, 1, 'D', 1): 0.1,
 (1, 1, 'E', 0): 5.7,
 (1, 1, 'E', 3): 0.3,
 (1, 1, 'G', 0): 2.1,
 (1, 1, 'M', 2): 0.1,
 (1, 1, 'M', 3): 4.0,
 (1, 1, 'S', 1): 4.8,
 (1, 1, 'S', 3): 2.0,
 (1, 1, 'T', 2): 3.6,
 (1, 1, 'T', 3): 5.0,
 (1, 1, 'Z', 0): 5.5}
HOLD = {(0, 0, 'D', 0): 81,
 (0, 0, 'E', 0): 84,
 (0, 1, 'E', 0): 92,
 (1, 0, 'E', 2): 80,
 (1, 0, 'S', 0): 27,
 (1, 0, 'T', 1): 35,
 (1, 0, 'U', 0): 57,
 (1, 0, 'V', 0): 81,
 (1, 1, 'E', 2): 80,
 (1, 1, 'T', 1): 84,
 (1, 1, 'T', 2): 49,
 (1, 1, 'V', 1): 87,
 (1, 1, 'V', 3): 47,
 (1, 1, 'Z', 1): 64}


def plan(zs):
    half = zs // 2
    cores = [(h, c) for h in range(half) for c in (0, 1)]
    need, when, ready = {}, {}, {d: [] for d in cores}
    order = {d: [] for d in cores}
    pieces = {"T": KD, "D": KR, "E": KR, "M": KR, "F": KR}
    events, busy, links, turn = [], dict.fromkeys(cores, 0.0), {}, [0]

    def post(at, what, key):
        turn[0] += 1
        heapq.heappush(events, (at, turn[0], what, key))

    def way_of(h, name, b):
        if name == "S" or (name == "G" and b < h) or (name == "M" and b > h):
            return h, 1
        if name in "ZGM":
            return h, 0
        return (h, 2) if name in "DE" else None

    def release(d, name, b, k):
        key = d + ((name, k * 4 // KD) if name in "SZ" else (name, b))
        at = max(when[d, name, b, k], HOLD.get(key, 0.0))
        if name in "SZ" and k + d[1] == 0:
            key, at = (), START
        bisect.insort(ready[d], (PRIO.get(key, RANK[name]) + 0.01 * k, abs(b - d[0]), name, b, k,
                                 at, way_of(d[0], name, b)))

    def task(d, name, b, k, deps, at=0.0):
        need[d, name, b, k], when[d, name, b, k] = deps, at
        if deps == 0:
            release(d, name, b, k)

    for d in cores:
        h, c = d
        for b in range(zs):
            for k in range(KD):
                task(d, "T", b, k, int(b != h), PACK if b == h else 0.0)
                if b != h and (h < zs - 1 if b < h else h > 0):
                    task(d, "G", b, k, 1)
            for name, other in (("U", "D"), ("V", "E")):
                task(d, name, b, 0, KD)
                for k in range(KR):
                    task(d, other, b, k, 1)
            for k in range(KR):
                if b == h:
                    task(d, "F", b, k, 2 + (h > 0) + (h < zs - 1))
                else:
                    task(d, "M", b, k, 2 + (h > 0 if b > h else h < zs - 1))
        if c == 0:
            task(d, "N", h + 1, 0, 1)
        for k in range(KD):
            for name in "SZ" if h > 0 else "S":
                task(d, name, h, k, c + (k > 0), START)
        post(START, "core", d)
        post(PACK, "core", d)

    def supply(d, name, b, k, at):
        if d[0] >= half:
            d, b = (zs - 1 - d[0], d[1]), zs - 1 - b
        key = (d, name, b, k)
        need[key] -= 1
        when[key] = max(when[key], at)
        if need[key] == 0:
            release(*key)
        post(at, "core", d)

    def settle(key, t):
        lk = links[key]
        live = [q for q in lk["queues"] if q]
        for q in live:
            q[0][0] -= (t - lk["at"]) / len(live)
        lk["at"] = t
        for q in live:
            while q and q[0][0] <= 1e-6:
                for e in q.pop(0)[1]:
                    supply(*e, t + LAG[key[1]])
        lk["stamp"] += 1
        live = [q for q in lk["queues"] if q]
        if live:
            post(t + min(q[0][0] for q in live) * len(live), "link", (key, lk["stamp"]))

    def wire(key, c, time, t, targets):
        lk = links.setdefault(key, {"at": 0.0, "queues": ([], []), "stamp": 0})
        if any(lk["queues"]):
            settle(key, t)
        lk["at"] = t
        lk["queues"][c].append([time, targets])
        settle(key, t)

    def backlog(key, c, t):
        lk = links.get(key)
        if lk is None:
            return 0.0
        return sum(x[0] for x in lk["queues"][c]) * sum(map(bool, lk["queues"]))

    def onward(h, c, way, b, k, name, time, t):
        g = h + 2 * way - 1
        wire((h, way), c, time, t, [((g, c), "F" if name == "M" and g == b else name, b, k)])

    def pick(d, t):
        later, full = None, {}
        for i, x in enumerate(ready[d]):
            at, gate = x[5:]
            if at <= t + 1e-9 and gate is not None:
                if gate not in full:
                    full[gate] = backlog(gate, d[1], t) - BACKLOG
                at = t + full[gate] if full[gate] > 1e-6 else at
            if at <= t + 1e-9:
                return ready[d].pop(i)[2:5]
            later = at if later is None else min(later, at)
        if later is not None:
            post(max(later, t + 0.1), "core", d)
        return None

    while events:
        t, _, what, key = heapq.heappop(events)
        if what == "link":
            if links[key[0]]["stamp"] == key[1]:
                settle(key[0], t)
            continue
        d = key
        if busy[d] > t + 1e-9:
            continue
        choice = pick(d, t)
        if choice is None:
            continue
        h, c = d
        name, b, k = choice
        order[d].append(choice)
        done = t + STEP + COST.get(name, 0.0) / pieces.get(name, 1)
        done += 0.3 if k == 0 and name in "TM" else 0.0
        if name in "SZ":
            onward(h, c, int(name == "S"), b, k, "T", Z_BLOCK / KD, t)
            if k + 1 < KD:
                supply(d, name, b, k + 1, done)
        elif name == "G":
            onward(h, c, int(b < h), b, k, "T", Z_BLOCK / KD, t)
        elif name == "T":
            if (d, "G", b, k) in need:
                supply(d, "G", b, k, done)
            if c == 0 and b == h + 1 and k == KD * HANDOVER // 8:
                supply(d, "N", b, 0, done)
            wire((h, 2), c, Y_BLOCK / KD, t, [(d, "U", b, 0), ((h, 1 - c), "V", b, 0)])
        elif name == "N":
            for r in range(KD):
                for s in "SZ" if h > 0 else "S":
                    supply((h, 1), s, h, r, done + 0.3)
        elif name in "UV":
            for r in range(KR):
                supply(d, "D" if name == "U" else "E", b, r, done)
        elif name in "DE":
            wire((h, 2), c, Y_BLOCK / KR / 2, t + STEP,
                 [((h, c if name == "D" else 1 - c), "F" if b == h else "M", b, k)])
        elif name == "M":
            onward(h, c, int(b > h), b, k, "M", Z_BLOCK / KR, t + STEP)
        busy[d] = done
        post(done, "core", d)
    assert sum(map(len, order.values())) == len(need)
    return order


def tables(zs):
    order = plan(zs)

    def code(name, b, k):
        return (KINDS.index(name) * zs + b) * max(KD, KR) + k

    def listed(h, c):
        todo = list(order[min(h, zs - 1 - h), c])
        if h >= zs // 2:
            todo = [({"S": "Z", "Z": "S"}.get(name, name), zs - 1 - b, k) for name, b, k in todo]
        if c == 0:
            todo = [x for x in todo if x[0] not in "SZ" or x[2] > 0]
        names = [x[0] for x in todo]
        first = min(names.index("U"), names.index("V"))
        todo.insert(first, ("W", 0, 0))
        if c == 1:
            turn = min(i for i, x in enumerate(todo) if x[0] in "SZ")
            todo.insert(turn, ("Q", 0, 0))
        return todo

    lists = [listed(h, c) for h in range(zs) for c in (0, 1)]
    return [[code(*x) for x in o] for o in lists]


def kernel(n, cap, table, tok_ref, gain_ref, ids_ref, gw_ref, wg_ref, wu_ref, wd_ref, out_ref,
           wg, wu, wd, lines, places, outgoing, arrived, results, returned, hidden, chain,
           pick, high, low, raw,
           tsem, wsem, lsend, lrecv, psend, precv, dsend, drecv, bsend, brecv, csend, crecv, turn):
    zs = n // SUB
    me = lax.axis_index("ep")
    hi, lo = me // SUB, me % SUB
    core = (lo + 1) % 2
    tok, width = tok_ref.shape
    ff = wg.shape[1]
    rows = SUB * cap
    dcols, rcols = width // KD, width // KR

    def peer(plane, part):
        return {"ep": plane * SUB + part}

    pieces = [pl.ds(i * (tok // PIECES), tok // PIECES) for i in range(PIECES)]
    t_copies = [pltpu.make_async_copy(tok_ref.at[at, :], raw.at[at, :], tsem.at[i])
                for i, at in enumerate(pieces)]
    for c in t_copies:
        c.start()

    barrier = pltpu.get_barrier_semaphore()

    def greet(to):
        pl.semaphore_signal(barrier, inc=1, device_id=to, device_id_type=pl.DeviceIdType.MESH)

    for dl in range(1, SUB):
        greet(peer(hi, (lo + dl) % SUB))

    @pl.when(hi > 0)
    def _():
        greet(peer((hi + zs - 1) % zs, lo))

    @pl.when(hi < zs - 1)
    def _():
        greet(peer((hi + 1) % zs, lo))

    w_copies = [
        pltpu.make_async_copy(wg_ref.at[0], wg, wsem.at[0]),
        pltpu.make_async_copy(wu_ref.at[0], wu, wsem.at[1]),
        pltpu.make_async_copy(wd_ref.at[0], wd, wsem.at[2]),
    ]
    for c in w_copies:
        c.start()

    def remote(src, dst, send, recv, to):
        return pltpu.make_async_remote_copy(
            src_ref=src, dst_ref=dst, send_sem=send, recv_sem=recv,
            device_id=to, device_id_type=pl.DeviceIdType.MESH)

    def dcol(k):
        return pl.ds(pl.multiple_of(k * dcols, dcols), dcols)

    def rcol(k):
        return pl.ds(pl.multiple_of(k * rcols, rcols), rcols)

    def slot_rows(j, dl):
        return pl.ds(pl.multiple_of(j * rows + (dl // 2 + dl % 2 * 2) * cap, cap), cap)

    def side_rows(j, side):
        return pl.ds(pl.multiple_of(j * rows + side * 2 * cap, 2 * cap), 2 * cap)

    def block_rows(j):
        return pl.ds(pl.multiple_of(j * rows, rows), rows)

    def far_rows(j):
        return pl.ds(pl.multiple_of(j * rows + cap, cap), rows - cap)

    def onward(way):
        return (hi + 2 * way - 1 + zs) % zs

    def line_copy(block, k, way):
        part = lines.at[block, :, dcol(k)]
        return remote(part, part, lsend.at[way * zs + block], lrecv.at[block * KD + k],
                      peer(onward(way), lo))

    def place_copy(block, way):
        return remote(places.at[block], places.at[block], psend.at[way * zs + block],
                      precv.at[block], peer(onward(way), lo))

    def out_copy(j, dl, k):
        at = slot_rows(j, dl)
        return remote(outgoing.at[at, dcol(k)], arrived.at[at, dcol(k)],
                      dsend.at[j], drecv.at[(j * 2 + dl % 2) * KD + k], peer(hi, (lo + dl) % SUB))

    def out_arrival(j, side, k):
        at = arrived.at[side_rows(j, 1) if side else slot_rows(j, 2), dcol(k)]
        return remote(at, at, dsend.at[j], drecv.at[(j * 2 + side) * KD + k],
                      peer(hi, (lo + 1) % SUB))

    def back_copy(j, dl, k):
        at = slot_rows(j, dl)
        return remote(results.at[at, rcol(k)], returned.at[at, rcol(k)],
                      bsend.at[j], brecv.at[j * KR + k], peer(hi, (lo - dl + SUB) % SUB))

    def back_arrival(j, k):
        at = returned.at[far_rows(j), rcol(k)]
        return remote(at, at, bsend.at[j], brecv.at[j * KR + k], peer(hi, (lo + 1) % SUB))

    def chain_copy(way, j, k):
        part = chain.at[way * zs + j, :, rcol(k)]
        return remote(part, part, csend.at[way * zs + j], crecv.at[(way * zs + j) * KR + k],
                      peer(onward(way), lo))

    bits = (len(KINDS) * zs * max(KD, KR) - 1).bit_length()
    many = 30 // bits
    where_am_i = hi * 2 + core
    words = []
    for i in range(0, max(map(len, table)), many):
        packed = [sum(x << bits * r for r, x in enumerate(row[i:i + many])) for row in table]
        word = jnp.int32(packed[0])
        for at in range(1, 2 * zs):
            word = jnp.where(where_am_i == at, packed[at], word)
        words.append(word)
    words += [jnp.int32(0)] * (-len(words) % GROUP)
    count = jnp.int32(len(table[0]))
    for at in range(1, 2 * zs):
        count = jnp.where(where_am_i == at, len(table[at]), count)

    step = min(64, tok // PIECES)

    def norm(i, carry):
        at = pl.ds(pl.multiple_of(i * step, step), step)
        v = raw[at, :].astype(jnp.float32)
        scale = lax.rsqrt(jnp.mean(v * v, -1, keepdims=True) + 1e-06)
        lines[hi, at, :] = (v * scale * gain_ref[...]).astype(jnp.bfloat16)
        return carry

    per = tok // PIECES // step
    for i, c in enumerate(t_copies):
        c.wait()
        lax.fori_loop(i * per, (i + 1) * per, norm, 0)

    ends = jnp.where(hi == 0, 1, 0) + jnp.where(hi == zs - 1, 1, 0)
    pl.semaphore_wait(barrier, SUB + 1 - ends)

    def forward(way, act):
        @pl.when(jnp.where(way == 1, zs - 1 - hi, hi) > 0)
        def _():
            act(way)

    def send_own(way, k):
        forward(way, lambda w: line_copy(hi, k, w).start())

    def send_places(way):
        forward(way, lambda w: place_copy(hi, w).start())

    @pl.when(core == 0)
    def _():
        for way in (1, 0):
            send_own(way, 0)

    expert = lax.broadcasted_iota(jnp.int32, (n, tok), 0)
    id0, id1 = ids_ref[0:1, :], ids_ref[1:2, :]
    chosen = jnp.where((id0 == expert) | (id1 == expert), 1.0, 0.0).astype(jnp.bfloat16)
    t_row = lax.broadcasted_iota(jnp.int32, (tok, tok), 0)
    t_col = lax.broadcasted_iota(jnp.int32, (tok, tok), 1)
    earlier = jnp.where(t_row < t_col, 1.0, 0.0).astype(jnp.bfloat16)
    before = jnp.dot(chosen, earlier, preferred_element_type=jnp.float32)

    def dest(ids):
        slot = jnp.sum(jnp.where(ids == expert, before, 0.0), axis=0, keepdims=True)
        return ids.astype(jnp.float32) * cap + slot

    where = lax.broadcasted_iota(jnp.int32, (8, tok), 0)
    places[hi] = jnp.where(
        where == 0, dest(id0), jnp.where(
            where == 1, dest(id1), jnp.where(where == 2, gw_ref[0:1, :], gw_ref[1:2, :])))

    @pl.when(core == 0)
    def _():
        for way in (1, 0):
            send_places(way)

    def send_line(way, k):
        @pl.when((core == 1) & (k == 0))
        def _():
            send_places(way)

        send_own(way, k)

    def row_index():
        r = lax.broadcasted_iota(jnp.int32, (rows, tok), 0)
        dl = r // cap % 2 * 2 + r // cap // 2
        return ((hi * SUB + (lo + dl) % SUB) * cap + r % cap).astype(jnp.float32)

    def choose(j, at):
        index = row_index()
        w = places[j]
        pick[at] = jnp.where((index == w[0:1, :]) | (index == w[1:2, :]), 1.0, 0.0).astype(
            jnp.bfloat16)

    def pack(j, k, at):
        got = jnp.dot(pick[at], lines[j, :, dcol(k)],
                      preferred_element_type=jnp.float32).astype(jnp.bfloat16)
        outgoing[far_rows(j), dcol(k)] = got[cap:, :]
        for dl in range(1, SUB):
            out_copy(j, dl, k).start()
        arrived[slot_rows(j, 0), dcol(k)] = got[:cap, :]

    ftile = min(ff, 512)

    def up(j, side):
        for which in (0, 1):
            @pl.when(side == which)
            def _():
                def landed(k, carry):
                    out_arrival(j, which, k).wait_recv()
                    return carry

                lax.fori_loop(0, KD, landed, 0)

        def tile(f, carry):
            cols = pl.ds(pl.multiple_of(f * ftile, ftile), ftile)
            x = arrived[side_rows(j, side), :]
            g = jnp.dot(x, wg[:, cols], preferred_element_type=jnp.float32)
            u = jnp.dot(x, wu[:, cols], preferred_element_type=jnp.float32)
            hidden[j * 2 + side, :, cols] = (g / (1.0 + jnp.exp(-g)) * u).astype(jnp.bfloat16)
            return carry

        lax.fori_loop(0, ff // ftile, tile, 0)

    def down(j, side, k):
        got = jnp.dot(hidden[j * 2 + side], wd[:, rcol(k)],
                      preferred_element_type=jnp.float32).astype(jnp.bfloat16)

        @pl.when(side == 0)
        def _():
            results[slot_rows(j, 2), rcol(k)] = got[cap:, :]
            back_copy(j, 2, k).start()
            returned[slot_rows(j, 0), rcol(k)] = got[:cap, :]

        @pl.when(side == 1)
        def _():
            results[side_rows(j, 1), rcol(k)] = got
            for dl in (1, 3):
                back_copy(j, dl, k).start()

    def weigh(j, at):
        index = row_index()
        w = places[j]
        weight = jnp.transpose(jnp.where(index == w[0:1, :], w[2:3, :], 0.0)
                               + jnp.where(index == w[1:2, :], w[3:4, :], 0.0))
        top = weight.astype(jnp.bfloat16)
        high[at] = top
        low[at] = (weight - top.astype(jnp.float32)).astype(jnp.bfloat16)

    def mix(j, k, at):
        block = returned[block_rows(j), rcol(k)]
        return (jnp.dot(high[at], block, preferred_element_type=jnp.float32)
                + jnp.dot(low[at], block, preferred_element_type=jnp.float32))

    def take(j, k):
        way = jnp.where(j < hi, 1, 0)

        @pl.when((k == 0) & (j != hi))
        def _():
            place_copy(j, way).wait_recv()

        @pl.when(k == 0)
        def _():
            choose(j, j)

        @pl.when(j != hi)
        def _():
            line_copy(j, k, way).wait_recv()

        pack(j, k, j)

    def pass_on(j, k):
        way = jnp.where(j < hi, 1, 0)

        @pl.when(k == 0)
        def _():
            place_copy(j, way).start()

        line_copy(j, k, way).start()

    def add(j, k):
        way = jnp.where(j > hi, 1, 0)

        @pl.when(k == 0)
        def _():
            weigh(j, j)

        back_arrival(j, k).wait_recv()
        value = mix(j, k, j)
        at = way * zs + j
        beyond = way * hi + (1 - way) * (zs - 1 - hi)

        @pl.when(beyond > 0)
        def _():
            chain_copy(way, j, k).wait_recv()
            chain[at, :, rcol(k)] = (
                value + chain[at, :, rcol(k)].astype(jnp.float32)).astype(jnp.bfloat16)

        @pl.when(beyond == 0)
        def _():
            chain[at, :, rcol(k)] = value.astype(jnp.bfloat16)

        chain_copy(way, j, k).start()

    def final(k):
        @pl.when(k == 0)
        def _():
            weigh(hi, hi)

        back_arrival(hi, k).wait_recv()
        value = mix(hi, k, hi)

        def arrived_from(way):
            chain_copy(way, hi, k).wait_recv()
            return chain[way * zs + hi, :, rcol(k)].astype(jnp.float32)

        def put(total):
            out_ref[:, rcol(k)] = total.astype(out_ref.dtype)

        @pl.when(hi == 0)
        def _():
            put(value + arrived_from(0))

        @pl.when(hi == zs - 1)
        def _():
            put(value + arrived_from(1))

        @pl.when((hi > 0) & (hi < zs - 1))
        def _():
            put(value + arrived_from(0) + arrived_from(1))

    def run(near, i, carry):
        spot, digit = lax.div(i, many), lax.rem(i, many)
        word = near[0]
        for at in range(1, len(near)):
            word = jnp.where(spot == at, near[at], word)
        for r in range(1, many):
            word = jnp.where(digit >= r, lax.div(word, 1 << bits), word)
        code = lax.rem(word, 1 << bits)
        kind = lax.div(code, zs * max(KD, KR))
        j = lax.rem(lax.div(code, max(KD, KR)), zs)
        k = lax.rem(code, max(KD, KR))

        acts = {
            "S": lambda: send_line(1, k),
            "Z": lambda: send_line(0, k),
            "G": lambda: pass_on(j, k),
            "T": lambda: take(j, k),
            "U": lambda: up(j, kind - KINDS.index("U")),
            "D": lambda: down(j, kind - KINDS.index("D"), k),
            "M": lambda: add(j, k),
            "F": lambda: final(k),
            "W": lambda: [c.wait() for c in w_copies],
            "N": lambda: pl.semaphore_signal(
                turn, inc=1, device_id=peer(hi, lo - 1), device_id_type=pl.DeviceIdType.MESH),
            "Q": lambda: pl.semaphore_wait(turn, 1),
        }

        def among(names):
            if len(names) == 1:
                acts[names[0]]()
                return
            cut = len(names) // 2
            low = kind < KINDS.index(names[cut])
            pl.when(low)(lambda: among(names[:cut]))
            pl.when(jnp.logical_not(low))(lambda: among(names[cut:]))

        among(list(acts))
        return carry

    def turns(a, carry):
        near = []
        for r in range(GROUP):
            word = words[r]
            for at in range(1, len(words) // GROUP):
                word = jnp.where(a == at, words[at * GROUP + r], word)
            near.append(word)
        left = jnp.minimum(GROUP * many, count - a * (GROUP * many))
        return lax.fori_loop(0, left, functools.partial(run, near), carry)

    lax.fori_loop(0, lax.div(count + (GROUP * many - 1), GROUP * many), turns, 0)

    def finish(j, carry):
        at = far_rows(j)
        remote(outgoing.at[at, :], outgoing.at[at, :], dsend.at[j], drecv.at[0],
               peer(hi, (lo + 1) % SUB)).wait_send()
        remote(results.at[at, :], results.at[at, :], bsend.at[j], brecv.at[0],
               peer(hi, (lo + 1) % SUB)).wait_send()
        for way in (0, 1):
            to = peer(onward(way), lo)

            @pl.when((hi < zs - 1) & (j <= hi) if way else (hi > 0) & (j >= hi))
            def _():
                place_copy(j, way).wait_send()
                remote(lines.at[j], lines.at[j], lsend.at[way * zs + j], lrecv.at[0],
                       to).wait_send()

            @pl.when(j > hi if way else j < hi)
            def _():
                at = way * zs + j
                remote(chain.at[at], chain.at[at], csend.at[at], crecv.at[0], to).wait_send()

        return carry

    lax.fori_loop(0, zs, finish, 0)


def per_device(tokens, norm_gain, expert_ids, gate_weights, w_gate, w_up, w_down):
    n = lax.axis_size("ep")
    tok, width = tokens.shape
    top = expert_ids.shape[1]
    ff = w_gate.shape[2]
    cap = 2 * tok * top // n
    total = n * cap
    zs = n // SUB
    rows = SUB * cap
    table = tables(zs)
    bf16 = jnp.bfloat16
    dma = pltpu.SemaphoreType.DMA
    vmem = pl.BlockSpec(memory_space=pltpu.VMEM)
    hbm = pl.BlockSpec(memory_space=pl.ANY)
    return pl.pallas_call(
        functools.partial(kernel, n, cap, table),
        out_shape=pltpu.VMEM((tok, width), bf16),
        in_specs=[hbm] + [vmem] * 3 + [hbm] * 3,
        out_specs=vmem,
        scratch_shapes=[
            pltpu.VMEM((width, ff), bf16),
            pltpu.VMEM((width, ff), bf16),
            pltpu.VMEM((ff, width), bf16),
            pltpu.VMEM((zs, tok, width), bf16),
            pltpu.VMEM((zs, 8, tok), jnp.float32),
            pltpu.VMEM((total, width), bf16),
            pltpu.VMEM((total, width), bf16),
            pltpu.VMEM((total, width), bf16),
            pltpu.VMEM((total, width), bf16),
            pltpu.VMEM((2 * zs, rows // 2, ff), bf16),
            pltpu.VMEM((2 * zs, tok, width), bf16),
            pltpu.VMEM((zs, rows, tok), bf16),
            pltpu.VMEM((zs, tok, rows), bf16),
            pltpu.VMEM((zs, tok, rows), bf16),
            pltpu.VMEM((tok, width), bf16),
            dma((PIECES,)),
            dma((3,)),
            dma((2 * zs,)),
            dma((zs * KD,)),
            dma((2 * zs,)),
            dma((zs,)),
            dma((zs,)),
            dma((2 * zs * KD,)),
            dma((zs,)),
            dma((zs * KR,)),
            dma((2 * zs,)),
            dma((2 * zs * KR,)),
            pltpu.SemaphoreType.REGULAR,
        ],
        compiler_params=pltpu.CompilerParams(
            collective_id=0, has_side_effects=True, vmem_limit_bytes=58 * 1024 * 1024),
    )(tokens, norm_gain.reshape(1, width), expert_ids.T, gate_weights.T, w_gate, w_up, w_down)


def solution(mesh):
    return jax.shard_map(
        per_device,
        mesh=mesh,
        in_specs=(
            P(("grp", "ep"), None),
            P(),
            P(("grp", "ep"), None),
            P(("grp", "ep"), None),
            P("ep", None, None),
            P("ep", None, None),
            P("ep", None, None),
        ),
        out_specs=P(("grp", "ep"), None),
        check_vma=False,
    )
```

```python
import bisect
import functools
import heapq
import jax
import jax.numpy as jnp
from jax import lax
from jax.experimental import pallas as pl
from jax.experimental.pallas import tpu as pltpu
from jax.sharding import PartitionSpec as P

SUB = 4
KD = 8
KR = 8
PIECES = 2
GROUP = 4
KINDS = "SZGTUVDEMFWNQ"
COST = {"T": 1.6, "U": 2.05, "V": 2.05, "D": 1.96, "E": 1.96, "M": 1.84, "F": 1.7, "G": 0.15, "S": 0.1, "Z": 0.1}
RANK = {"S": 0, "Z": 0, "G": 0.5, "T": 1, "N": -1, "M": 2, "F": 3, "D": 4, "E": 4, "U": 5, "V": 5}
Z_BLOCK, Y_BLOCK, START, PACK, STEP, BACKLOG = 11.4, 5.75, 2.9, 3.8, 0.09, 3.0
LAG = (2.2, 2.2, 2.5)
HANDOVER = 4
PRIO = {(0, 0, 'S', 1): 6.0,
 (0, 0, 'T', 2): 5.3,
 (0, 0, 'V', 1): 0.1,
 (0, 1, 'E', 0): 5.5,
 (0, 1, 'T', 1): 5.4,
 (0, 1, 'T', 2): 5.3,
 (0, 1, 'V', 0): 3.4,
 (1, 0, 'D', 0): 2.0,
 (1, 0, 'D', 1): 0.2,
 (1, 0, 'D', 3): 2.4,
 (1, 0, 'E', 3): 0.2,
 (1, 0, 'M', 3): 4.0,
 (1, 0, 'S', 0): 2.6,
 (1, 0, 'T', 0): 4.7,
 (1, 0, 'T', 2): 3.6,
 (1, 0, 'U', 0): 2.4,
 (1, 0, 'U', 2): 1.5,
 (1, 0, 'V', 0): 2.4,
 (1, 0, 'Z', 2): 1.3,
 (1, 1, 'D', 0): 5.1,
 (1, 1, 'D', 1): 0.1,
 (1, 1, 'E', 0): 5.7,
 (1, 1, 'E', 3): 0.3,
 (1, 1, 'G', 0): 2.1,
 (1, 1, 'M', 2): 0.1,
 (1, 1, 'M', 3): 4.0,
 (1, 1, 'S', 1): 4.8,
 (1, 1, 'S', 3): 2.0,
 (1, 1, 'T', 2): 3.6,
 (1, 1, 'T', 3): 5.0,
 (1, 1, 'Z', 0): 5.5}
HOLD = {(0, 0, 'D', 0): 81,
 (0, 0, 'E', 0): 84,
 (0, 1, 'E', 0): 92,
 (1, 0, 'E', 2): 80,
 (1, 0, 'S', 0): 27,
 (1, 0, 'T', 1): 35,
 (1, 0, 'U', 0): 57,
 (1, 0, 'V', 0): 81,
 (1, 1, 'E', 2): 80,
 (1, 1, 'T', 1): 84,
 (1, 1, 'T', 2): 49,
 (1, 1, 'V', 1): 87,
 (1, 1, 'V', 3): 47,
 (1, 1, 'Z', 1): 64}


def plan(zs):
    half = zs // 2
    cores = [(h, c) for h in range(half) for c in (0, 1)]
    need, when, ready = {}, {}, {d: [] for d in cores}
    order = {d: [] for d in cores}
    pieces = {"T": KD, "D": KR, "E": KR, "M": KR, "F": KR}
    events, busy, links, turn = [], dict.fromkeys(cores, 0.0), {}, [0]

    def post(at, what, key):
        turn[0] += 1
        heapq.heappush(events, (at, turn[0], what, key))

    def way_of(h, name, b):
        if name == "S" or (name == "G" and b < h) or (name == "M" and b > h):
            return h, 1
        if name in "ZGM":
            return h, 0
        return (h, 2) if name in "DE" else None

    def release(d, name, b, k):
        key = d + ((name, k * 4 // KD) if name in "SZ" else (name, b))
        at = max(when[d, name, b, k], HOLD.get(key, 0.0))
        if name in "SZ" and k + d[1] == 0:
            key, at = (), START
        bisect.insort(ready[d], (PRIO.get(key, RANK[name]) + 0.01 * k, abs(b - d[0]), name, b, k,
                                 at, way_of(d[0], name, b)))

    def task(d, name, b, k, deps, at=0.0):
        need[d, name, b, k], when[d, name, b, k] = deps, at
        if deps == 0:
            release(d, name, b, k)

    for d in cores:
        h, c = d
        for b in range(zs):
            for k in range(KD):
                task(d, "T", b, k, int(b != h), PACK if b == h else 0.0)
                if b != h and (h < zs - 1 if b < h else h > 0):
                    task(d, "G", b, k, 1)
            for name, other in (("U", "D"), ("V", "E")):
                task(d, name, b, 0, KD)
                for k in range(KR):
                    task(d, other, b, k, 1)
            for k in range(KR):
                if b == h:
                    task(d, "F", b, k, 2 + (h > 0) + (h < zs - 1))
                else:
                    task(d, "M", b, k, 2 + (h > 0 if b > h else h < zs - 1))
        if c == 0:
            task(d, "N", h + 1, 0, 1)
        for k in range(KD):
            for name in "SZ" if h > 0 else "S":
                task(d, name, h, k, c + (k > 0), START)
        post(START, "core", d)
        post(PACK, "core", d)

    def supply(d, name, b, k, at):
        if d[0] >= half:
            d, b = (zs - 1 - d[0], d[1]), zs - 1 - b
        key = (d, name, b, k)
        need[key] -= 1
        when[key] = max(when[key], at)
        if need[key] == 0:
            release(*key)
        post(at, "core", d)

    def settle(key, t):
        lk = links[key]
        live = [q for q in lk["queues"] if q]
        for q in live:
            q[0][0] -= (t - lk["at"]) / len(live)
        lk["at"] = t
        for q in live:
            while q and q[0][0] <= 1e-6:
                for e in q.pop(0)[1]:
                    supply(*e, t + LAG[key[1]])
        lk["stamp"] += 1
        live = [q for q in lk["queues"] if q]
        if live:
            post(t + min(q[0][0] for q in live) * len(live), "link", (key, lk["stamp"]))

    def wire(key, c, time, t, targets):
        lk = links.setdefault(key, {"at": 0.0, "queues": ([], []), "stamp": 0})
        if any(lk["queues"]):
            settle(key, t)
        lk["at"] = t
        lk["queues"][c].append([time, targets])
        settle(key, t)

    def backlog(key, c, t):
        lk = links.get(key)
        if lk is None:
            return 0.0
        return sum(x[0] for x in lk["queues"][c]) * sum(map(bool, lk["queues"]))

    def onward(h, c, way, b, k, name, time, t):
        g = h + 2 * way - 1
        wire((h, way), c, time, t, [((g, c), "F" if name == "M" and g == b else name, b, k)])

    def pick(d, t):
        later, full = None, {}
        for i, x in enumerate(ready[d]):
            at, gate = x[5:]
            if at <= t + 1e-9 and gate is not None:
                if gate not in full:
                    full[gate] = backlog(gate, d[1], t) - BACKLOG
                at = t + full[gate] if full[gate] > 1e-6 else at
            if at <= t + 1e-9:
                return ready[d].pop(i)[2:5]
            later = at if later is None else min(later, at)
        if later is not None:
            post(max(later, t + 0.1), "core", d)
        return None

    while events:
        t, _, what, key = heapq.heappop(events)
        if what == "link":
            if links[key[0]]["stamp"] == key[1]:
                settle(key[0], t)
            continue
        d = key
        if busy[d] > t + 1e-9:
            continue
        choice = pick(d, t)
        if choice is None:
            continue
        h, c = d
        name, b, k = choice
        order[d].append(choice)
        done = t + STEP + COST.get(name, 0.0) / pieces.get(name, 1)
        done += 0.3 if k == 0 and name in "TM" else 0.0
        if name in "SZ":
            onward(h, c, int(name == "S"), b, k, "T", Z_BLOCK / KD, t)
            if k + 1 < KD:
                supply(d, name, b, k + 1, done)
        elif name == "G":
            onward(h, c, int(b < h), b, k, "T", Z_BLOCK / KD, t)
        elif name == "T":
            if (d, "G", b, k) in need:
                supply(d, "G", b, k, done)
            if c == 0 and b == h + 1 and k == KD * HANDOVER // 8:
                supply(d, "N", b, 0, done)
            wire((h, 2), c, Y_BLOCK / KD, t, [(d, "U", b, 0), ((h, 1 - c), "V", b, 0)])
        elif name == "N":
            for r in range(KD):
                for s in "SZ" if h > 0 else "S":
                    supply((h, 1), s, h, r, done + 0.3)
        elif name in "UV":
            for r in range(KR):
                supply(d, "D" if name == "U" else "E", b, r, done)
        elif name in "DE":
            wire((h, 2), c, Y_BLOCK / KR / 2, t + STEP,
                 [((h, c if name == "D" else 1 - c), "F" if b == h else "M", b, k)])
        elif name == "M":
            onward(h, c, int(b > h), b, k, "M", Z_BLOCK / KR, t + STEP)
        busy[d] = done
        post(done, "core", d)
    assert sum(map(len, order.values())) == len(need)
    return order


def tables(zs):
    order = plan(zs)

    def code(name, b, k):
        return (KINDS.index(name) * zs + b) * max(KD, KR) + k

    def listed(h, c):
        todo = list(order[min(h, zs - 1 - h), c])
        if h >= zs // 2:
            todo = [({"S": "Z", "Z": "S"}.get(name, name), zs - 1 - b, k) for name, b, k in todo]
        if c == 0:
            todo = [x for x in todo if x[0] not in "SZ" or x[2] > 0]
        names = [x[0] for x in todo]
        first = min(names.index("U"), names.index("V"))
        todo.insert(first, ("W", 0, 0))
        if c == 1:
            turn = min(i for i, x in enumerate(todo) if x[0] in "SZ")
            todo.insert(turn, ("Q", 0, 0))
        return todo

    lists = [listed(h, c) for h in range(zs) for c in (0, 1)]
    return [[code(*x) for x in o] for o in lists]


def kernel(n, cap, table, tok_ref, gain_ref, ids_ref, gw_ref, wg_ref, wu_ref, wd_ref, out_ref,
           wg, wu, wd, lines, places, outgoing, arrived, results, returned, hidden, chain,
           pick, high, low, raw,
           tsem, wsem, lsend, lrecv, psend, precv, dsend, drecv, bsend, brecv, csend, crecv, turn):
    zs = n // SUB
    me = lax.axis_index("ep")
    hi, lo = me // SUB, me % SUB
    core = (lo + 1) % 2
    tok, width = tok_ref.shape
    ff = wg.shape[1]
    rows = SUB * cap
    dcols, rcols = width // KD, width // KR

    def peer(plane, part):
        return {"ep": plane * SUB + part}

    pieces = [pl.ds(i * (tok // PIECES), tok // PIECES) for i in range(PIECES)]
    t_copies = [pltpu.make_async_copy(tok_ref.at[at, :], raw.at[at, :], tsem.at[i])
                for i, at in enumerate(pieces)]
    for c in t_copies:
        c.start()

    barrier = pltpu.get_barrier_semaphore()

    def greet(to):
        pl.semaphore_signal(barrier, inc=1, device_id=to, device_id_type=pl.DeviceIdType.MESH)

    for dl in range(1, SUB):
        greet(peer(hi, (lo + dl) % SUB))

    @pl.when(hi > 0)
    def _():
        greet(peer((hi + zs - 1) % zs, lo))

    @pl.when(hi < zs - 1)
    def _():
        greet(peer((hi + 1) % zs, lo))

    w_copies = [
        pltpu.make_async_copy(wg_ref.at[0], wg, wsem.at[0]),
        pltpu.make_async_copy(wu_ref.at[0], wu, wsem.at[1]),
        pltpu.make_async_copy(wd_ref.at[0], wd, wsem.at[2]),
    ]
    for c in w_copies:
        c.start()

    def remote(src, dst, send, recv, to):
        return pltpu.make_async_remote_copy(
            src_ref=src, dst_ref=dst, send_sem=send, recv_sem=recv,
            device_id=to, device_id_type=pl.DeviceIdType.MESH)

    def dcol(k):
        return pl.ds(pl.multiple_of(k * dcols, dcols), dcols)

    def rcol(k):
        return pl.ds(pl.multiple_of(k * rcols, rcols), rcols)

    def slot_rows(j, dl):
        return pl.ds(pl.multiple_of(j * rows + (dl // 2 + dl % 2 * 2) * cap, cap), cap)

    def side_rows(j, side):
        return pl.ds(pl.multiple_of(j * rows + side * 2 * cap, 2 * cap), 2 * cap)

    def block_rows(j):
        return pl.ds(pl.multiple_of(j * rows, rows), rows)

    def far_rows(j):
        return pl.ds(pl.multiple_of(j * rows + cap, cap), rows - cap)

    def onward(way):
        return (hi + 2 * way - 1 + zs) % zs

    def line_copy(block, k, way):
        part = lines.at[block, :, dcol(k)]
        return remote(part, part, lsend.at[way * zs + block], lrecv.at[block * KD + k],
                      peer(onward(way), lo))

    def place_copy(block, way):
        return remote(places.at[block], places.at[block], psend.at[way * zs + block],
                      precv.at[block], peer(onward(way), lo))

    def out_copy(j, dl, k):
        at = slot_rows(j, dl)
        return remote(outgoing.at[at, dcol(k)], arrived.at[at, dcol(k)],
                      dsend.at[j], drecv.at[(j * 2 + dl % 2) * KD + k], peer(hi, (lo + dl) % SUB))

    def out_arrival(j, side, k):
        at = arrived.at[side_rows(j, 1) if side else slot_rows(j, 2), dcol(k)]
        return remote(at, at, dsend.at[j], drecv.at[(j * 2 + side) * KD + k],
                      peer(hi, (lo + 1) % SUB))

    def back_copy(j, dl, k):
        at = slot_rows(j, dl)
        return remote(results.at[at, rcol(k)], returned.at[at, rcol(k)],
                      bsend.at[j], brecv.at[j * KR + k], peer(hi, (lo - dl + SUB) % SUB))

    def back_arrival(j, k):
        at = returned.at[far_rows(j), rcol(k)]
        return remote(at, at, bsend.at[j], brecv.at[j * KR + k], peer(hi, (lo + 1) % SUB))

    def chain_copy(way, j, k):
        part = chain.at[way * zs + j, :, rcol(k)]
        return remote(part, part, csend.at[way * zs + j], crecv.at[(way * zs + j) * KR + k],
                      peer(onward(way), lo))

    bits = (len(KINDS) * zs * max(KD, KR) - 1).bit_length()
    many = 30 // bits
    where_am_i = hi * 2 + core
    words = []
    for i in range(0, max(map(len, table)), many):
        packed = [sum(x << bits * r for r, x in enumerate(row[i:i + many])) for row in table]
        word = jnp.int32(packed[0])
        for at in range(1, 2 * zs):
            word = jnp.where(where_am_i == at, packed[at], word)
        words.append(word)
    words += [jnp.int32(0)] * (-len(words) % GROUP)
    count = jnp.int32(len(table[0]))
    for at in range(1, 2 * zs):
        count = jnp.where(where_am_i == at, len(table[at]), count)

    step = min(128, tok // PIECES)

    def norm(i, carry):
        at = pl.ds(pl.multiple_of(i * step, step), step)
        v = raw[at, :].astype(jnp.float32)
        scale = lax.rsqrt(jnp.mean(v * v, -1, keepdims=True) + 1e-06)
        lines[hi, at, :] = (v * scale * gain_ref[...]).astype(jnp.bfloat16)
        return carry

    per = tok // PIECES // step
    for i, c in enumerate(t_copies):
        c.wait()
        lax.fori_loop(i * per, (i + 1) * per, norm, 0)

    ends = jnp.where(hi == 0, 1, 0) + jnp.where(hi == zs - 1, 1, 0)
    pl.semaphore_wait(barrier, SUB + 1 - ends)

    def forward(way, act):
        @pl.when(jnp.where(way == 1, zs - 1 - hi, hi) > 0)
        def _():
            act(way)

    def send_own(way, k):
        forward(way, lambda w: line_copy(hi, k, w).start())

    def send_places(way):
        forward(way, lambda w: place_copy(hi, w).start())

    @pl.when(core == 0)
    def _():
        for way in (1, 0):
            send_own(way, 0)

    expert = lax.broadcasted_iota(jnp.int32, (n, tok), 0)
    id0, id1 = ids_ref[0:1, :], ids_ref[1:2, :]
    chosen = jnp.where((id0 == expert) | (id1 == expert), 1.0, 0.0).astype(jnp.bfloat16)
    t_row = lax.broadcasted_iota(jnp.int32, (tok, tok), 0)
    t_col = lax.broadcasted_iota(jnp.int32, (tok, tok), 1)
    earlier = jnp.where(t_row < t_col, 1.0, 0.0).astype(jnp.bfloat16)
    before = jnp.dot(chosen, earlier, preferred_element_type=jnp.float32)

    def dest(ids):
        slot = jnp.sum(jnp.where(ids == expert, before, 0.0), axis=0, keepdims=True)
        return ids.astype(jnp.float32) * cap + slot

    where = lax.broadcasted_iota(jnp.int32, (8, tok), 0)
    places[hi] = jnp.where(
        where == 0, dest(id0), jnp.where(
            where == 1, dest(id1), jnp.where(where == 2, gw_ref[0:1, :], gw_ref[1:2, :])))

    @pl.when(core == 0)
    def _():
        for way in (1, 0):
            send_places(way)

    def send_line(way, k):
        @pl.when((core == 1) & (k == 0))
        def _():
            send_places(way)

        send_own(way, k)

    def row_index():
        r = lax.broadcasted_iota(jnp.int32, (rows, tok), 0)
        dl = r // cap % 2 * 2 + r // cap // 2
        return ((hi * SUB + (lo + dl) % SUB) * cap + r % cap).astype(jnp.float32)

    def choose(j, at):
        index = row_index()
        w = places[j]
        pick[at] = jnp.where((index == w[0:1, :]) | (index == w[1:2, :]), 1.0, 0.0).astype(
            jnp.bfloat16)

    def pack(j, k, at):
        got = jnp.dot(pick[at], lines[j, :, dcol(k)],
                      preferred_element_type=jnp.float32).astype(jnp.bfloat16)
        outgoing[far_rows(j), dcol(k)] = got[cap:, :]
        for dl in range(1, SUB):
            out_copy(j, dl, k).start()
        arrived[slot_rows(j, 0), dcol(k)] = got[:cap, :]

    ftile = min(ff, 512)

    def up(j, side):
        for which in (0, 1):
            @pl.when(side == which)
            def _():
                def landed(k, carry):
                    out_arrival(j, which, k).wait_recv()
                    return carry

                lax.fori_loop(0, KD, landed, 0)

        def tile(f, carry):
            cols = pl.ds(pl.multiple_of(f * ftile, ftile), ftile)
            x = arrived[side_rows(j, side), :]
            g = jnp.dot(x, wg[:, cols], preferred_element_type=jnp.float32)
            u = jnp.dot(x, wu[:, cols], preferred_element_type=jnp.float32)
            hidden[j * 2 + side, :, cols] = (g / (1.0 + jnp.exp(-g)) * u).astype(jnp.bfloat16)
            return carry

        lax.fori_loop(0, ff // ftile, tile, 0)

    def down(j, side, k):
        got = jnp.dot(hidden[j * 2 + side], wd[:, rcol(k)],
                      preferred_element_type=jnp.float32).astype(jnp.bfloat16)

        @pl.when(side == 0)
        def _():
            results[slot_rows(j, 2), rcol(k)] = got[cap:, :]
            back_copy(j, 2, k).start()
            returned[slot_rows(j, 0), rcol(k)] = got[:cap, :]

        @pl.when(side == 1)
        def _():
            results[side_rows(j, 1), rcol(k)] = got
            for dl in (1, 3):
                back_copy(j, dl, k).start()

    def weigh(j, at):
        index = row_index()
        w = places[j]
        weight = jnp.transpose(jnp.where(index == w[0:1, :], w[2:3, :], 0.0)
                               + jnp.where(index == w[1:2, :], w[3:4, :], 0.0))
        top = weight.astype(jnp.bfloat16)
        high[at] = top
        low[at] = (weight - top.astype(jnp.float32)).astype(jnp.bfloat16)

    def mix(j, k, at):
        block = returned[block_rows(j), rcol(k)]
        return (jnp.dot(high[at], block, preferred_element_type=jnp.float32)
                + jnp.dot(low[at], block, preferred_element_type=jnp.float32))

    def take(j, k):
        way = jnp.where(j < hi, 1, 0)

        @pl.when((k == 0) & (j != hi))
        def _():
            place_copy(j, way).wait_recv()

        @pl.when(k == 0)
        def _():
            choose(j, j)

        @pl.when(j != hi)
        def _():
            line_copy(j, k, way).wait_recv()

        pack(j, k, j)

    def pass_on(j, k):
        way = jnp.where(j < hi, 1, 0)

        @pl.when(k == 0)
        def _():
            place_copy(j, way).start()

        line_copy(j, k, way).start()

    def add(j, k):
        way = jnp.where(j > hi, 1, 0)

        @pl.when(k == 0)
        def _():
            weigh(j, j)

        back_arrival(j, k).wait_recv()
        value = mix(j, k, j)
        at = way * zs + j
        beyond = way * hi + (1 - way) * (zs - 1 - hi)

        @pl.when(beyond > 0)
        def _():
            chain_copy(way, j, k).wait_recv()
            chain[at, :, rcol(k)] = (
                value + chain[at, :, rcol(k)].astype(jnp.float32)).astype(jnp.bfloat16)

        @pl.when(beyond == 0)
        def _():
            chain[at, :, rcol(k)] = value.astype(jnp.bfloat16)

        chain_copy(way, j, k).start()

    def final(k):
        @pl.when(k == 0)
        def _():
            weigh(hi, hi)

        back_arrival(hi, k).wait_recv()
        value = mix(hi, k, hi)

        def arrived_from(way):
            chain_copy(way, hi, k).wait_recv()
            return chain[way * zs + hi, :, rcol(k)].astype(jnp.float32)

        def put(total):
            out_ref[:, rcol(k)] = total.astype(out_ref.dtype)

        @pl.when(hi == 0)
        def _():
            put(value + arrived_from(0))

        @pl.when(hi == zs - 1)
        def _():
            put(value + arrived_from(1))

        @pl.when((hi > 0) & (hi < zs - 1))
        def _():
            put(value + arrived_from(0) + arrived_from(1))

    def run(near, i, carry):
        spot, digit = lax.div(i, many), lax.rem(i, many)
        word = near[0]
        for at in range(1, len(near)):
            word = jnp.where(spot == at, near[at], word)
        for r in range(1, many):
            word = jnp.where(digit >= r, lax.div(word, 1 << bits), word)
        code = lax.rem(word, 1 << bits)
        kind = lax.div(code, zs * max(KD, KR))
        j = lax.rem(lax.div(code, max(KD, KR)), zs)
        k = lax.rem(code, max(KD, KR))

        acts = {
            "S": lambda: send_line(1, k),
            "Z": lambda: send_line(0, k),
            "G": lambda: pass_on(j, k),
            "T": lambda: take(j, k),
            "U": lambda: up(j, kind - KINDS.index("U")),
            "D": lambda: down(j, kind - KINDS.index("D"), k),
            "M": lambda: add(j, k),
            "F": lambda: final(k),
            "W": lambda: [c.wait() for c in w_copies],
            "N": lambda: pl.semaphore_signal(
                turn, inc=1, device_id=peer(hi, lo - 1), device_id_type=pl.DeviceIdType.MESH),
            "Q": lambda: pl.semaphore_wait(turn, 1),
        }

        def among(names):
            if len(names) == 1:
                acts[names[0]]()
                return
            cut = len(names) // 2
            low = kind < KINDS.index(names[cut])
            pl.when(low)(lambda: among(names[:cut]))
            pl.when(jnp.logical_not(low))(lambda: among(names[cut:]))

        among(list(acts))
        return carry

    def turns(a, carry):
        near = []
        for r in range(GROUP):
            word = words[r]
            for at in range(1, len(words) // GROUP):
                word = jnp.where(a == at, words[at * GROUP + r], word)
            near.append(word)
        left = jnp.minimum(GROUP * many, count - a * (GROUP * many))
        return lax.fori_loop(0, left, functools.partial(run, near), carry)

    lax.fori_loop(0, lax.div(count + (GROUP * many - 1), GROUP * many), turns, 0)

    def finish(j, carry):
        at = far_rows(j)
        remote(outgoing.at[at, :], outgoing.at[at, :], dsend.at[j], drecv.at[0],
               peer(hi, (lo + 1) % SUB)).wait_send()
        remote(results.at[at, :], results.at[at, :], bsend.at[j], brecv.at[0],
               peer(hi, (lo + 1) % SUB)).wait_send()
        for way in (0, 1):
            to = peer(onward(way), lo)

            @pl.when((hi < zs - 1) & (j <= hi) if way else (hi > 0) & (j >= hi))
            def _():
                place_copy(j, way).wait_send()
                remote(lines.at[j], lines.at[j], lsend.at[way * zs + j], lrecv.at[0],
                       to).wait_send()

            @pl.when(j > hi if way else j < hi)
            def _():
                at = way * zs + j
                remote(chain.at[at], chain.at[at], csend.at[at], crecv.at[0], to).wait_send()

        return carry

    lax.fori_loop(0, zs, finish, 0)


def per_device(tokens, norm_gain, expert_ids, gate_weights, w_gate, w_up, w_down):
    n = lax.axis_size("ep")
    tok, width = tokens.shape
    top = expert_ids.shape[1]
    ff = w_gate.shape[2]
    cap = 2 * tok * top // n
    total = n * cap
    zs = n // SUB
    rows = SUB * cap
    table = tables(zs)
    bf16 = jnp.bfloat16
    dma = pltpu.SemaphoreType.DMA
    vmem = pl.BlockSpec(memory_space=pltpu.VMEM)
    hbm = pl.BlockSpec(memory_space=pl.ANY)
    return pl.pallas_call(
        functools.partial(kernel, n, cap, table),
        out_shape=pltpu.VMEM((tok, width), bf16),
        in_specs=[hbm] + [vmem] * 3 + [hbm] * 3,
        out_specs=vmem,
        scratch_shapes=[
            pltpu.VMEM((width, ff), bf16),
            pltpu.VMEM((width, ff), bf16),
            pltpu.VMEM((ff, width), bf16),
            pltpu.VMEM((zs, tok, width), bf16),
            pltpu.VMEM((zs, 8, tok), jnp.float32),
            pltpu.VMEM((total, width), bf16),
            pltpu.VMEM((total, width), bf16),
            pltpu.VMEM((total, width), bf16),
            pltpu.VMEM((total, width), bf16),
            pltpu.VMEM((2 * zs, rows // 2, ff), bf16),
            pltpu.VMEM((2 * zs, tok, width), bf16),
            pltpu.VMEM((zs, rows, tok), bf16),
            pltpu.VMEM((zs, tok, rows), bf16),
            pltpu.VMEM((zs, tok, rows), bf16),
            pltpu.VMEM((tok, width), bf16),
            dma((PIECES,)),
            dma((3,)),
            dma((2 * zs,)),
            dma((zs * KD,)),
            dma((2 * zs,)),
            dma((zs,)),
            dma((zs,)),
            dma((2 * zs * KD,)),
            dma((zs,)),
            dma((zs * KR,)),
            dma((2 * zs,)),
            dma((2 * zs * KR,)),
            pltpu.SemaphoreType.REGULAR,
        ],
        compiler_params=pltpu.CompilerParams(
            collective_id=0, has_side_effects=True, vmem_limit_bytes=58 * 1024 * 1024),
    )(tokens, norm_gain.reshape(1, width), expert_ids.T, gate_weights.T, w_gate, w_up, w_down)


def solution(mesh):
    return jax.shard_map(
        per_device,
        mesh=mesh,
        in_specs=(
            P(("grp", "ep"), None),
            P(),
            P(("grp", "ep"), None),
            P(("grp", "ep"), None),
            P("ep", None, None),
            P("ep", None, None),
            P("ep", None, None),
        ),
        out_specs=P(("grp", "ep"), None),
        check_vma=False,
    )
```
